512 devices in a mesh: ep: 128 (over z, x, core), tp: 4 (over y).
Axes of the slice: x: 4, y: 4, z: 16, core: 2. Of those that a mesh axis runs over, the one named last changes fastest.
Arguments:
- hidden_in: bfloat16 [2048, 1024], P('ep', 'tp'), may hold values from -40 to 40
- norm_gain_attn: float32 [1024], replicated, may hold values from 0.1 to 1.9
- query_weight: bfloat16 [1024, 512], P(None, 'tp'), may hold values from -0.1875 to 0.1875
- key_weight: bfloat16 [1024, 512], P(None, 'tp'), may hold values from -0.1875 to 0.1875
- value_weight: bfloat16 [1024, 512], P(None, 'tp'), may hold values from -0.1875 to 0.1875
- query_gain: float32 [128], replicated, may hold values from 1 to 1.6
- key_gain: float32 [128], replicated, may hold values from 1 to 1.6
- lambda_head: float32 [4], P('tp'), may hold values from 0.3 to 0.8
- sub_gain: float32 [128], replicated, may hold values from 0.1 to 1.9
- out_weight: bfloat16 [512, 1024], P('tp'), may hold values from -0.25 to 0.25
- cache_key: bfloat16 [2048, 256, 512], P('ep', None, 'tp'), may hold values from -8 to 8
- cache_value: bfloat16 [2048, 256, 512], P('ep', None, 'tp'), may hold values from -6 to 6
- lengths: int32 [2048], P('ep'), may hold values from 1 to 256
- norm_gain_mix: float32 [1024], P('tp'), may hold values from 0.1 to 1.9
- route_ids: int32 [2048, 6], P('ep'), may hold values from 0 to 127, all different within a row; in each aligned block of 16 rows (0 to 15, 16 to 31, ...) at most 2 rows name the same one
- route_logits: float32 [2048, 6], P('ep'), may hold values from -4 to 4
- expert_gate: bfloat16 [128, 1024, 1024], P('ep', None, 'tp'), may hold values from -0.5 to 0.5
- expert_up: bfloat16 [128, 1024, 1024], P('ep', None, 'tp'), may hold values from -0.5 to 0.5
- expert_down: bfloat16 [128, 1024, 1024], P('ep', 'tp'), may hold values from -0.046875 to 0.046875
- dense_gate: bfloat16 [1024, 2048], P('tp', 'ep'), may hold values from -0.1875 to 0.1875
- dense_up: bfloat16 [1024, 2048], P('tp', 'ep'), may hold values from -0.1875 to 0.1875
- dense_down: bfloat16 [2048, 1024], P('ep', 'tp'), may hold values from -0.125 to 0.125
- branch_gate: float32 [1024], P('tp'), may hold values from -0.1875 to 0.1875
Outputs:
- layer_out: bfloat16 [2048, 1024], P('ep', 'tp')
- key_rows: bfloat16 [2048, 512], P('ep', 'tp')
- value_rows: bfloat16 [2048, 512], P('ep', 'tp')
The draws below stay inside these ranges and needn't reach their ends.
Inputs may be any that keep to these rules, and one draw needn't show every extreme that they name: `route_ids`: each row names 6 different experts. Among the rows of one index of ep (aligned blocks of 16 rows) no expert is named by more than 2 rows, and in some blocks one expert is named by exactly 2.
All inputs are finite; a program needn't handle non-finite values.
Results may differ from the reference program's by a relative error of at most 0.0075.
Values may be sent and summed in bfloat16 or wider, within the bound.
No kernel may reach another device: no remote copies, remote signals or barrier semaphores. Data moves between devices by JAX's collectives and lax.ppermute only.
A program may use at most 64 MiB of HBM per device.

```python
import math
from functools import partial
import jax
import jax.numpy as jnp
import numpy as np
from jax import lax

D = 1024
HEADS = 4
QK = 64
VAL = 128
FF = 1024
DENSE = 2048
TOPK = 6
SEQ_GRP = 16
CACHE = 256
EXPERTS = 128
TOKENS = 2048
CAP = 2
N_EP = 128


def draw_hidden_in(key, part):
    row_key, entry_key = jax.random.split(jax.random.fold_in(key, 11))
    position = jnp.arange(D, dtype=jnp.float32) / D
    column_scale = 0.5 * 3.0 ** position
    entries = jnp.clip(jax.random.normal(entry_key, (TOKENS, D), jnp.float32), -4.0, 4.0)
    row_scale = jnp.exp(jax.random.uniform(row_key, (TOKENS, 1), jnp.float32, -0.7, 1.2))
    return (entries * row_scale * column_scale[None, :]).astype(jnp.bfloat16)


def plant(values, rng, smallest, high):
    spot = [jax.random.randint(jax.random.fold_in(rng, axis), (), 0, length) for axis, length in enumerate(values.shape)]
    widest = values.shape.index(max(values.shape))
    beside = spot[:widest] + [(spot[widest] + 1) % values.shape[widest]] + spot[widest + 1:]
    return values.at[tuple(spot)].set(smallest).at[tuple(beside)].set(high)


def levels(rng, extent, shards, smallest, top_value):
    def one(axis_at, parts):
        draws = jax.random.uniform(jax.random.fold_in(jax.random.fold_in(rng, 6), axis_at), (parts,), jnp.float32, smallest / len(shards), top_value / len(shards))
        return jnp.repeat(jnp.exp(draws), extent[axis_at] // parts).reshape((-1,) + (1,) * (len(extent) - axis_at - 1))

    level = one(*shards[0])
    for cut in shards[1:]:
        level = level * one(*cut)
    return level


def assign_block(own_key, own, number, rows, amount, top, most, slope):
    ranking = jax.random.permutation(own_key, amount)
    packed, common = portions_of(amount, rows * top, most, slope, True), portions_of(amount, rows * top, most, slope, False)
    places = jnp.arange(amount)

    def named(sizes, offset_by):
        used = int((sizes > 0).sum())
        fixed = max(1, used // 4)
        shifted = fixed + (places - fixed + offset_by * (used - fixed)) % max(1, amount - fixed)
        return jnp.zeros((amount,), jnp.int32).at[ranking[jnp.where(places < fixed, places, shifted)]].set(jnp.asarray(sizes, jnp.int32))

    sizes = jnp.where(number % 4 == 0, named(packed, number // 4), named(common, number - number // 4 - 1))
    mixed = jax.random.permutation(jax.random.fold_in(own, 3), amount)
    donor, sink = mixed[0:amount // 2 * 2:2], mixed[1:amount // 2 * 2:2]
    margin = jnp.minimum(sizes[donor] - 1, most - sizes[sink]) // 2
    margin = jnp.where((donor == ranking[0]) | (sink == ranking[0]) | (sizes[sink] == 0), 0, jnp.maximum(margin, 0))
    shifted = jax.random.randint(jax.random.fold_in(own, 4), (amount // 2,), 0, 1 << 20) % (margin + 1)
    sizes = sizes.at[donor].add(-shifted).at[sink].add(shifted)
    items = jnp.searchsorted(jnp.cumsum(sizes), jnp.arange(rows * top), side="right").astype(jnp.int32)
    table = items.reshape(top, rows).T
    table = table[jax.random.permutation(jax.random.fold_in(own, 1), rows)]
    offset_by = jax.random.randint(jax.random.fold_in(own, 2), (rows, 1), 0, top)
    return jnp.take_along_axis(table, (jnp.arange(top)[None, :] + offset_by) % top, axis=1)


def portions_of(amount, total, limit, slope, full):
    portions = [(1 << 20) // math.isqrt(rank ** slope) + 1 for rank in range(1, amount + 1)]
    largest = limit if full else min(limit, max(-(-total // amount), total * portions[0] // sum(portions)))
    least = 1 if total - largest >= amount - 1 else 0
    holding, rest = [largest] + [least] * (amount - 1), total - largest - least * (amount - 1)
    while rest > 0:
        candidates = [i for i in range(1, amount) if holding[i] < largest] or [i for i in range(1, amount) if holding[i] < limit]
        pool, left = sum([portions[i] for i in candidates]), rest
        for i in candidates:
            addition = min(limit - holding[i], max(1, left * portions[i] // pool), rest)
            holding[i] = holding[i] + addition
            rest = rest - addition
    return np.array(holding)


def normal_values(stream_key, dims, spread, reach, cuts=(), kind=jnp.bfloat16):
    gain = levels(stream_key, dims, cuts, -0.22, 0.18) if cuts else 1.0
    drawn = jax.random.normal(stream_key, dims, jnp.float32) * spread * gain
    return jnp.minimum(jnp.maximum(drawn, -reach), reach).astype(kind)


def setup_inputs(seed: int = 0) -> dict:
    key_of = jax.random.split(jax.random.key(seed), 24)
    hidden_in = draw_hidden_in(jax.random.fold_in(key_of[23], 71), 0)
    norm_gain_attn = jnp.clip(1.0 + 0.18 * jax.random.normal(key_of[1], (D,), jnp.float32), 0.1, 1.9)
    query_weight = normal_values(key_of[2], (D, HEADS * 2 * QK), D ** -0.5, 0.1875, ((1, 4),))
    key_weight = normal_values(key_of[3], (D, HEADS * 2 * QK), D ** -0.5, 0.1875, ((1, 4),))
    value_weight = normal_values(key_of[4], (D, HEADS * VAL), D ** -0.5, 0.1875, ((1, 4),))
    query_gain = jnp.clip(jax.random.uniform(key_of[5], (2 * QK,), jnp.float32, 1.0, 1.6), 1.0, 1.6)
    key_gain = jnp.clip(jax.random.uniform(key_of[6], (2 * QK,), jnp.float32, 1.0, 1.6), 1.0, 1.6)
    lambda_head = jnp.clip(0.3 + 0.5 * jax.random.uniform(key_of[7], (HEADS,), jnp.float32) ** levels(key_of[7], (HEADS,), ((0, 4),), -0.2, 0.2), 0.3, 0.8)
    sub_gain = jnp.clip(1.0 + 0.18 * jax.random.normal(key_of[8], (VAL,), jnp.float32), 0.1, 1.9)
    out_weight = normal_values(key_of[9], (HEADS * VAL, D), (HEADS * VAL) ** -0.5, 0.25, ((0, 4),))
    cache_key = normal_values(key_of[10], (TOKENS, CACHE, HEADS * 2 * QK), 1.25, 8.0, ((0, 128), (2, 4)))
    cache_value = normal_values(key_of[11], (TOKENS, CACHE, HEADS * VAL), 1.0, 6.0, ((0, 128), (2, 4)))
    lengths = plant(jax.random.randint(key_of[12], (TOKENS,), 1, CACHE + 1), jax.random.fold_in(key_of[12], 1), 1, CACHE).astype(jnp.int32)
    norm_gain_mix = jnp.clip(1.0 + 0.18 * jax.random.normal(key_of[13], (D,), jnp.float32), 0.1, 1.9)
    route_ids_keys = jax.random.split(jax.random.fold_in(key_of[14], 1), TOKENS // SEQ_GRP)
    route_ids_turns = jax.random.permutation(jax.random.fold_in(key_of[14], 3), TOKENS // SEQ_GRP)
    route_ids = jax.vmap(lambda own, number: assign_block(jax.random.fold_in(key_of[14], 2), own, number, SEQ_GRP, EXPERTS, TOPK, CAP, 1))(route_ids_keys, route_ids_turns).reshape((TOKENS, TOPK))
    route_logits = normal_values(key_of[15], (TOKENS, TOPK), 1.0, 4.0, ((0, 128),), jnp.float32)
    expert_gate = normal_values(key_of[16], (EXPERTS, D, FF), (D // 9) ** -0.5, 0.5, ((0, 128), (2, 4)))
    expert_up = normal_values(key_of[17], (EXPERTS, D, FF), (D // 9) ** -0.5, 0.5, ((0, 128), (2, 4)))
    expert_down = normal_values(key_of[18], (EXPERTS, FF, D), (16 * FF) ** -0.5, 0.046875, ((0, 128), (1, 4)))
    dense_gate = normal_values(key_of[19], (D, DENSE), D ** -0.5, 0.1875, ((0, 4), (1, 128)))
    dense_up = normal_values(key_of[20], (D, DENSE), D ** -0.5, 0.1875, ((0, 4), (1, 128)))
    dense_down = normal_values(key_of[21], (DENSE, D), DENSE ** -0.5, 0.125, ((0, 128), (1, 4)))
    branch_gate = normal_values(key_of[22], (D,), D ** -0.5, 0.1875, ((0, 4),), jnp.float32)
    return {"hidden_in": hidden_in, "norm_gain_attn": norm_gain_attn, "query_weight": query_weight, "key_weight": key_weight, "value_weight": value_weight, "query_gain": query_gain, "key_gain": key_gain, "lambda_head": lambda_head, "sub_gain": sub_gain, "out_weight": out_weight, "cache_key": cache_key, "cache_value": cache_value, "lengths": lengths, "norm_gain_mix": norm_gain_mix, "route_ids": route_ids, "route_logits": route_logits, "expert_gate": expert_gate, "expert_up": expert_up, "expert_down": expert_down, "dense_gate": dense_gate, "dense_up": dense_up, "dense_down": dense_down, "branch_gate": branch_gate}


EPSILON = 1e-06
CLAMP_LIMIT = 7.0
SWISH_ALPHA = 1.702
OUT_SCALE = 0.2 + 0.6 * math.exp(-0.6)

def rms_scale(values, scale_gain):
    mean_square = lax.optimization_barrier(jnp.mean(values * values, axis=-1, keepdims=True))
    return values * lax.rsqrt(mean_square + EPSILON) * scale_gain

def clamped_unit(gate_pre, up_pre):
    gate_cut = jnp.minimum(gate_pre, CLAMP_LIMIT)
    up_cut = jnp.clip(up_pre, -CLAMP_LIMIT, CLAMP_LIMIT)
    return (up_cut + 1.0) * gate_cut * jax.nn.sigmoid(SWISH_ALPHA * gate_cut)

def attend_block(block, lambda_head, sub_gain):
    query_rows, key_new, value_new, key_cache, value_cache, length_rows = block
    seq_count = query_rows.shape[0]
    scale_factor = QK ** (-0.5)
    query_float = query_rows.astype(jnp.float32)
    key_past = key_cache.astype(jnp.float32).reshape(seq_count, CACHE, HEADS, 2, QK)
    past_score = jnp.einsum('shmd,sjhmd->shmj', query_float, key_past) * scale_factor
    own_score = lax.optimization_barrier(jnp.sum(query_float * key_new.astype(jnp.float32), axis=-1)) * scale_factor
    valid_mask = lax.iota(jnp.int32, CACHE)[None, :] < length_rows[:, None]
    past_exp = jnp.where(valid_mask[:, None, None, :], jnp.exp(past_score), 0.0)
    own_exp = jnp.exp(own_score)
    denominator = lax.optimization_barrier(jnp.sum(past_exp, axis=-1)) + own_exp
    past_prob = past_exp / denominator[..., None]
    own_prob = own_exp / denominator
    weight_past = (past_prob[:, :, 0] - lambda_head[None, :, None] * past_prob[:, :, 1]).astype(jnp.bfloat16)
    weight_own = (own_prob[:, :, 0] - lambda_head[None, :] * own_prob[:, :, 1]).astype(jnp.bfloat16)
    value_past = value_cache.astype(jnp.float32).reshape(seq_count, CACHE, HEADS, VAL)
    head_mix = jnp.einsum('shj,sjhe->she', weight_past.astype(jnp.float32), value_past)
    head_mix = head_mix + weight_own.astype(jnp.float32)[..., None] * value_new.astype(jnp.float32)
    head_out = (rms_scale(head_mix, sub_gain) * OUT_SCALE).astype(jnp.bfloat16)
    return head_out.reshape(seq_count, HEADS * VAL)

def expert_routes(mix_rows, route_ids, expert_gate, expert_up, expert_down):
    flat_ids = route_ids.reshape(-1).astype(jnp.int32)
    route_total = flat_ids.shape[0]
    most_rows = N_EP * CAP

    def one_expert(carried, index):
        order = jnp.argsort(jnp.where(flat_ids == index, 0, 1).astype(jnp.int32), stable=True)[:most_rows]
        order = order.astype(jnp.int32)
        chosen = flat_ids[order] == index
        token_rows = mix_rows[order // TOPK]
        gate_pre = jnp.dot(token_rows, expert_gate[index], preferred_element_type=jnp.float32)
        up_pre = jnp.dot(token_rows, expert_up[index], preferred_element_type=jnp.float32)
        activation = clamped_unit(gate_pre, up_pre).astype(jnp.bfloat16)
        result = jnp.dot(activation, expert_down[index], preferred_element_type=jnp.float32).astype(jnp.bfloat16)
        result = lax.optimization_barrier(result).astype(jnp.float32)
        result = jnp.where(chosen[:, None], result, 0.0)
        return (carried.at[order].add(result), None)
    start_rows = jnp.zeros((route_total, D), jnp.float32)
    routed_rows, _ = lax.scan(one_expert, start_rows, jnp.arange(EXPERTS, dtype=jnp.int32))
    return routed_rows

def reference(hidden_in, norm_gain_attn, query_weight, key_weight, value_weight, query_gain, key_gain, lambda_head, sub_gain, out_weight, cache_key, cache_value, lengths, norm_gain_mix, route_ids, route_logits, expert_gate, expert_up, expert_down, dense_gate, dense_up, dense_down, branch_gate):
    normed = rms_scale(hidden_in.astype(jnp.float32), norm_gain_attn).astype(jnp.bfloat16)
    query_pre = jnp.dot(normed, query_weight, preferred_element_type=jnp.float32).reshape(TOKENS, HEADS, 2, QK)
    query_rows = rms_scale(query_pre, query_gain.reshape(2, QK)).astype(jnp.bfloat16)
    key_pre = jnp.dot(normed, key_weight, preferred_element_type=jnp.float32).reshape(TOKENS, HEADS, 2, QK)
    key_rows = rms_scale(key_pre, key_gain.reshape(2, QK)).astype(jnp.bfloat16)
    value_rows = jnp.dot(normed, value_weight, preferred_element_type=jnp.float32).astype(jnp.bfloat16)
    blocks = (query_rows.reshape(N_EP, SEQ_GRP, HEADS, 2, QK), key_rows.reshape(N_EP, SEQ_GRP, HEADS, 2, QK), value_rows.reshape(N_EP, SEQ_GRP, HEADS, VAL), cache_key.reshape(N_EP, SEQ_GRP, CACHE, HEADS * 2 * QK), cache_value.reshape(N_EP, SEQ_GRP, CACHE, HEADS * VAL), lengths.reshape(N_EP, SEQ_GRP))
    head_out = lax.map(partial(attend_block, lambda_head=lambda_head, sub_gain=sub_gain), blocks)
    head_out = head_out.reshape(TOKENS, HEADS * VAL)
    attn_out = jnp.dot(head_out, out_weight, preferred_element_type=jnp.float32)
    residual = hidden_in.astype(jnp.float32) + attn_out
    inverse = lax.rsqrt(lax.optimization_barrier(jnp.mean(residual * residual, axis=1, keepdims=True)) + EPSILON)
    mix_float = residual * inverse * norm_gain_mix
    mix_rows = mix_float.astype(jnp.bfloat16)
    branch_weight = jax.nn.sigmoid(lax.optimization_barrier(jnp.sum(mix_float * branch_gate, axis=1, keepdims=True)))
    route_weight = jax.nn.softmax(route_logits, axis=1)
    routed_rows = expert_routes(mix_rows, route_ids, expert_gate, expert_up, expert_down)
    routed = lax.optimization_barrier(jnp.sum(routed_rows.reshape(TOKENS, TOPK, D) * route_weight[:, :, None], axis=1))
    dense_gate_pre = jnp.dot(mix_rows, dense_gate, preferred_element_type=jnp.float32)
    dense_up_pre = jnp.dot(mix_rows, dense_up, preferred_element_type=jnp.float32)
    dense_act = (jax.nn.silu(dense_gate_pre) * dense_up_pre).astype(jnp.bfloat16)
    dense_result = jnp.dot(dense_act, dense_down, preferred_element_type=jnp.float32)
    layer_out = (residual + routed + branch_weight * dense_result).astype(jnp.bfloat16)
    return (layer_out, key_rows.reshape(TOKENS, HEADS * 2 * QK), value_rows)
```

```python
import math

import jax
import jax.numpy as jnp
from jax import lax
from jax.sharding import Mesh
from jax.sharding import PartitionSpec as P

EP = ("ep_0", "ep_1", "ep_2")
PLANE = ("ep_1", "ep_2")
BLOCK = ("ep_1", "ep_2", "tp")
CAP = 2


EPSILON = 1e-06
CLAMP_LIMIT = 7.0
SWISH_ALPHA = 1.702
OUT_SCALE = 0.2 + 0.6 * math.exp(-0.6)


def from_everyone(x, axis):
    copies = jnp.broadcast_to(x, (lax.axis_size(axis), *x.shape))
    return lax.all_to_all(copies, axis, split_axis=0, concat_axis=0, tiled=True)


def rms_scale(values, scale_gain):
    mean_square = jnp.mean(values * values, axis=-1, keepdims=True)
    return values * lax.rsqrt(mean_square + EPSILON) * scale_gain


def clamped_unit(gate_pre, up_pre):
    gate_cut = jnp.minimum(gate_pre, CLAMP_LIMIT)
    up_cut = jnp.clip(up_pre, -CLAMP_LIMIT, CLAMP_LIMIT)
    return (up_cut + 1.0) * gate_cut * jax.nn.sigmoid(SWISH_ALPHA * gate_cut)


def attend(
    normed,
    query_weight,
    key_weight,
    value_weight,
    query_gain,
    key_gain,
    lambda_head,
    sub_gain,
    cache_key,
    cache_value,
    lengths,
):
    seq_count = normed.shape[0]
    head_count = lambda_head.shape[0]
    qk_size = query_gain.shape[0] // 2
    val_size = value_weight.shape[1] // head_count
    cache_len = cache_key.shape[1]
    scale_factor = qk_size ** (-0.5)
    query_pre = jnp.dot(normed, query_weight, preferred_element_type=jnp.float32)
    query_rows = rms_scale(
        query_pre.reshape(seq_count, head_count, 2, qk_size), query_gain.reshape(2, qk_size)
    ).astype(jnp.bfloat16)
    key_pre = jnp.dot(normed, key_weight, preferred_element_type=jnp.float32)
    key_rows = rms_scale(
        key_pre.reshape(seq_count, head_count, 2, qk_size), key_gain.reshape(2, qk_size)
    ).astype(jnp.bfloat16)
    value_rows = jnp.dot(normed, value_weight, preferred_element_type=jnp.float32).astype(
        jnp.bfloat16
    )
    key_past = cache_key.reshape(seq_count, cache_len, head_count, 2, qk_size)
    past_score = (
        jnp.einsum("shmd,sjhmd->shmj", query_rows, key_past, preferred_element_type=jnp.float32)
        * scale_factor
    )
    own_score = (
        jnp.einsum("shmd,shmd->shm", query_rows, key_rows, preferred_element_type=jnp.float32)
        * scale_factor
    )
    valid_mask = lax.iota(jnp.int32, cache_len)[None, :] < lengths[:, None]
    past_exp = jnp.where(valid_mask[:, None, None, :], jnp.exp(past_score), 0.0)
    own_exp = jnp.exp(own_score)
    denominator = jnp.sum(past_exp, axis=-1) + own_exp
    past_prob = past_exp / denominator[..., None]
    own_prob = own_exp / denominator
    weight_past = (past_prob[:, :, 0] - lambda_head[None, :, None] * past_prob[:, :, 1]).astype(
        jnp.bfloat16
    )
    weight_own = (own_prob[:, :, 0] - lambda_head[None, :] * own_prob[:, :, 1]).astype(jnp.bfloat16)
    value_past = cache_value.reshape(seq_count, cache_len, head_count, val_size)
    head_mix = jnp.einsum(
        "shj,sjhe->she", weight_past, value_past, preferred_element_type=jnp.float32
    )
    own_value = value_rows.reshape(seq_count, head_count, val_size).astype(jnp.float32)
    head_mix = head_mix + weight_own.astype(jnp.float32)[..., None] * own_value
    head_out = (rms_scale(head_mix, sub_gain) * OUT_SCALE).astype(jnp.bfloat16)
    return (
        head_out.reshape(seq_count, head_count * val_size),
        key_rows.reshape(seq_count, -1),
        value_rows,
    )


def routing_tables(route_ids, route_weight):
    line = lax.axis_size("ep_0")
    plane = lax.axis_size("ep_1") * lax.axis_size("ep_2")
    seq_count, top_count = route_ids.shape
    packed = jnp.concatenate([route_ids.astype(jnp.float32).T, route_weight.T], axis=0)
    seen = from_everyone(packed, "ep_0")
    seen = seen.transpose(1, 0, 2).reshape(2 * top_count, line * seq_count)
    first = (lax.axis_index("ep_0") * plane).astype(jnp.float32)
    wanted = first + lax.broadcasted_iota(jnp.float32, (plane, 1), 0)
    named = [(seen[k][None, :] == wanted).astype(jnp.float32) for k in range(top_count)]
    match = sum(named)
    weight = sum(n * seen[top_count + k][None, :] for k, n in enumerate(named))
    total = line * seq_count
    row = lax.broadcasted_iota(jnp.int32, (total, total), 0)
    col = lax.broadcasted_iota(jnp.int32, (total, total), 1)
    earlier = ((row // seq_count == col // seq_count) & (row < col)).astype(jnp.bfloat16)
    rank = jnp.dot(match.astype(jnp.bfloat16), earlier, preferred_element_type=jnp.float32)
    slot = jnp.where(match > 0, rank, -1.0)
    shape = (plane, line, CAP, total)
    at_z = lax.broadcasted_iota(jnp.int32, shape, 1)
    at_slot = lax.broadcasted_iota(jnp.int32, shape, 2)
    of_z = lax.broadcasted_iota(jnp.int32, shape, 3) // seq_count
    hit = (at_z == of_z) & (slot[:, None, None, :] == at_slot.astype(jnp.float32))
    select = hit.astype(jnp.bfloat16).reshape(plane * line * CAP, total)
    scaled = jnp.where(hit, weight[:, None, None, :], 0.0).reshape(plane * line * CAP, total)
    upper = scaled.astype(jnp.bfloat16)
    lower = (scaled - upper.astype(jnp.float32)).astype(jnp.bfloat16)
    return select, upper, lower


def plane_weights(dense_gate, dense_up, dense_down):
    mine = jnp.concatenate([dense_gate.T, dense_up.T, dense_down], axis=0)
    units = dense_down.shape[0]
    seen = from_everyone(mine[None], PLANE).reshape(-1, *mine.shape)
    width = mine.shape[1]
    gate = seen[:, :units].reshape(-1, width)
    up = seen[:, units : 2 * units].reshape(-1, width)
    down = seen[:, 2 * units :].reshape(-1, width)
    return gate, up, down


def own_columns(x, axis):
    count = lax.axis_size(axis)
    width = x.shape[1] // count
    mine = lax.axis_index(axis)
    return sum(
        jnp.where(mine == k, x[:, k * width : (k + 1) * width], 0.0) for k in range(count)
    )


def body(
    hidden_in,
    norm_gain_attn,
    query_weight,
    key_weight,
    value_weight,
    query_gain,
    key_gain,
    lambda_head,
    sub_gain,
    out_weight,
    cache_key,
    cache_value,
    lengths,
    norm_gain_mix,
    route_ids,
    route_logits,
    expert_gate,
    expert_up,
    expert_down,
    dense_gate,
    dense_up,
    dense_down,
    branch_gate,
):
    seq_count = route_ids.shape[0]
    width = hidden_in.shape[1]
    line = lax.axis_size("ep_0")
    plane = lax.axis_size("ep_1") * lax.axis_size("ep_2")
    tp = lax.axis_size("tp")
    pieces = from_everyone(hidden_in, "tp")
    full_rows = jnp.concatenate([pieces[k] for k in range(tp)], axis=1).astype(jnp.float32)
    width_total = full_rows.shape[1]
    select, upper, lower = routing_tables(route_ids, jax.nn.softmax(route_logits, axis=1))
    gate_rows, up_rows, down_rows = plane_weights(dense_gate, dense_up, dense_down)
    normed = rms_scale(full_rows, norm_gain_attn).astype(jnp.bfloat16)
    head_out, key_rows, value_rows = attend(
        normed,
        query_weight,
        key_weight,
        value_weight,
        query_gain,
        key_gain,
        lambda_head,
        sub_gain,
        cache_key,
        cache_value,
        lengths,
    )
    head_terms = jnp.dot(head_out, out_weight, preferred_element_type=jnp.float32)
    residual_full = full_rows + from_everyone(head_terms, "tp").sum(axis=0)
    square_sum = jnp.sum(residual_full * residual_full, axis=1, keepdims=True)
    inverse = lax.rsqrt(square_sum / width_total + EPSILON)
    residual = own_columns(residual_full, "tp")
    mix_rows = (residual * inverse * norm_gain_mix[None, :]).astype(jnp.bfloat16)
    rows = from_everyone(mix_rows, "ep_0").reshape(line * seq_count, width)
    placed = jnp.dot(select, rows, preferred_element_type=jnp.float32).astype(jnp.bfloat16)
    placed = placed.reshape(plane, 1, line * CAP, width)
    placed = jnp.broadcast_to(placed, (plane, tp, line * CAP, width))
    arrived = lax.all_to_all(
        placed.reshape(plane * tp, line * CAP, width), BLOCK, 0, 0, tiled=True
    ).reshape(plane, tp, line * CAP, width)
    item_rows = jnp.concatenate(
        [arrived[:, k].reshape(plane * line * CAP, width) for k in range(tp)], axis=1
    )
    gate_pre = jnp.dot(item_rows, expert_gate[0], preferred_element_type=jnp.float32)
    up_pre = jnp.dot(item_rows, expert_up[0], preferred_element_type=jnp.float32)
    activation = clamped_unit(gate_pre, up_pre).astype(jnp.bfloat16)
    sent = jnp.stack(
        [
            jnp.dot(
                activation,
                expert_down[0][:, k * width : (k + 1) * width],
                preferred_element_type=jnp.float32,
            )
            .astype(jnp.bfloat16)
            .reshape(plane, line * CAP, width)
            for k in range(tp)
        ],
        axis=1,
    )
    returned = lax.all_to_all(
        sent.reshape(plane * tp, line * CAP, width), BLOCK, 0, 0, tiled=True
    ).reshape(plane, tp, line * CAP, width)
    route_out = jnp.sum(returned.astype(jnp.float32), axis=1).astype(jnp.bfloat16)
    route_out = route_out.reshape(plane * line * CAP, width)
    turned = (((0,), (0,)), ((), ()))
    routed = lax.dot_general(
        upper, route_out, turned, preferred_element_type=jnp.float32
    ) + lax.dot_general(lower, route_out, turned, preferred_element_type=jnp.float32)
    across = (((1,), (1,)), ((), ()))
    gate_part = lax.dot_general(rows, gate_rows, across, preferred_element_type=jnp.float32)
    up_part = lax.dot_general(rows, up_rows, across, preferred_element_type=jnp.float32)
    logit_part = jnp.sum(rows.astype(jnp.float32) * branch_gate[None, :], axis=1)
    units = gate_part.shape[1]
    logit_rows = jnp.broadcast_to(
        logit_part.reshape(-1, 2 * units), (8, (line * seq_count) // (2 * units), 2 * units)
    ).reshape(-1, 2 * units)
    together = jnp.concatenate(
        [jnp.concatenate([gate_part, up_part], axis=1), logit_rows], axis=0
    )
    summed = from_everyone(together, "tp").sum(axis=0)
    count = line * seq_count
    dense_act = (jax.nn.silu(summed[:count, :units]) * summed[:count, units:]).astype(jnp.bfloat16)
    logits = summed[count : count + count // (2 * units)].reshape(-1, 1)
    dense = jnp.dot(dense_act, down_rows, preferred_element_type=jnp.float32)
    back = (routed + jax.nn.sigmoid(logits) * dense).astype(jnp.bfloat16)
    home = lax.all_to_all(
        back.reshape(line, seq_count, width), "ep_0", 0, 0, tiled=True
    )
    layer_out = (residual + jnp.sum(home.astype(jnp.float32), axis=0)).astype(jnp.bfloat16)
    return (layer_out, key_rows, value_rows)


def solution(mesh):
    split = Mesh(mesh.devices.reshape(16, 4, 2, mesh.shape["tp"]), ("ep_0", "ep_1", "ep_2", "tp"))
    in_specs = (
        P(EP, "tp"),
        P(),
        P(None, "tp"),
        P(None, "tp"),
        P(None, "tp"),
        P(),
        P(),
        P("tp"),
        P(),
        P("tp", None),
        P(EP, None, "tp"),
        P(EP, None, "tp"),
        P(EP),
        P("tp"),
        P(EP, None),
        P(EP, None),
        P(EP, None, "tp"),
        P(EP, None, "tp"),
        P(EP, "tp", None),
        P("tp", EP),
        P("tp", EP),
        P(EP, "tp"),
        P("tp"),
    )
    out_specs = (P(EP, "tp"), P(EP, "tp"), P(EP, "tp"))
    return jax.shard_map(body, mesh=split, in_specs=in_specs, out_specs=out_specs, check_vma=False)
```

```python
import math

import jax
import jax.numpy as jnp
from jax import lax
from jax.experimental import pallas as pl
from jax.experimental.pallas import tpu as pltpu
from jax.sharding import Mesh
from jax.sharding import PartitionSpec as P

EP = ("ep_0", "ep_1", "ep_2")
PLANE = ("ep_1", "ep_2")
BLOCK = ("ep_1", "ep_2", "tp")
CAP = 2


EPSILON = 1e-06
CLAMP_LIMIT = 7.0
SWISH_ALPHA = 1.702
OUT_SCALE = 0.2 + 0.6 * math.exp(-0.6)


def from_everyone(x, axis):
    copies = jnp.broadcast_to(x, (lax.axis_size(axis), *x.shape))
    return lax.all_to_all(copies, axis, split_axis=0, concat_axis=0, tiled=True)


def rms_scale(values, scale_gain):
    mean_square = jnp.mean(values * values, axis=-1, keepdims=True)
    return values * lax.rsqrt(mean_square + EPSILON) * scale_gain


def clamped_unit(gate_pre, up_pre):
    gate_cut = jnp.minimum(gate_pre, CLAMP_LIMIT)
    up_cut = jnp.clip(up_pre, -CLAMP_LIMIT, CLAMP_LIMIT)
    return (up_cut + 1.0) * gate_cut * jax.nn.sigmoid(SWISH_ALPHA * gate_cut)


def attend(
    normed,
    query_weight,
    key_weight,
    value_weight,
    query_gain,
    key_gain,
    lambda_head,
    sub_gain,
    cache_key,
    cache_value,
    lengths,
):
    seq_count = normed.shape[0]
    head_count = lambda_head.shape[0]
    qk_size = query_gain.shape[0] // 2
    val_size = value_weight.shape[1] // head_count
    cache_len = cache_key.shape[1]
    scale_factor = qk_size ** (-0.5)
    query_pre = jnp.dot(normed, query_weight, preferred_element_type=jnp.float32)
    query_rows = rms_scale(
        query_pre.reshape(seq_count, head_count, 2, qk_size), query_gain.reshape(2, qk_size)
    ).astype(jnp.bfloat16)
    key_pre = jnp.dot(normed, key_weight, preferred_element_type=jnp.float32)
    key_rows = rms_scale(
        key_pre.reshape(seq_count, head_count, 2, qk_size), key_gain.reshape(2, qk_size)
    ).astype(jnp.bfloat16)
    value_rows = jnp.dot(normed, value_weight, preferred_element_type=jnp.float32).astype(
        jnp.bfloat16
    )
    key_past = cache_key.reshape(seq_count, cache_len, head_count, 2, qk_size)
    past_score = (
        jnp.einsum("shmd,sjhmd->shmj", query_rows, key_past, preferred_element_type=jnp.float32)
        * scale_factor
    )
    own_score = (
        jnp.einsum("shmd,shmd->shm", query_rows, key_rows, preferred_element_type=jnp.float32)
        * scale_factor
    )
    valid_mask = lax.iota(jnp.int32, cache_len)[None, :] < lengths[:, None]
    past_exp = jnp.where(valid_mask[:, None, None, :], jnp.exp(past_score), 0.0)
    own_exp = jnp.exp(own_score)
    denominator = jnp.sum(past_exp, axis=-1) + own_exp
    past_prob = past_exp / denominator[..., None]
    own_prob = own_exp / denominator
    weight_past = (past_prob[:, :, 0] - lambda_head[None, :, None] * past_prob[:, :, 1]).astype(
        jnp.bfloat16
    )
    weight_own = (own_prob[:, :, 0] - lambda_head[None, :] * own_prob[:, :, 1]).astype(jnp.bfloat16)
    value_past = cache_value.reshape(seq_count, cache_len, head_count, val_size)
    head_mix = jnp.einsum(
        "shj,sjhe->she", weight_past, value_past, preferred_element_type=jnp.float32
    )
    own_value = value_rows.reshape(seq_count, head_count, val_size).astype(jnp.float32)
    head_mix = head_mix + weight_own.astype(jnp.float32)[..., None] * own_value
    head_out = (rms_scale(head_mix, sub_gain) * OUT_SCALE).astype(jnp.bfloat16)
    return (
        head_out.reshape(seq_count, head_count * val_size),
        key_rows.reshape(seq_count, -1),
        value_rows,
    )


LANES = 128
TURNED = (((0,), (0,)), ((), ()))
ACROSS = (((1,), (1,)), ((), ()))
SCALARS = pl.BlockSpec(memory_space=pltpu.SMEM)
WHOLE = pl.BlockSpec(memory_space=pltpu.VMEM)


def mm(a, b):
    return jnp.dot(a, b, preferred_element_type=jnp.float32)


def routes_kernel(ids_ref, turned_ref, logits_ref, out_ref):
    ids = ids_ref[...]
    turned = turned_ref[...]
    count, top = ids.shape
    logits = logits_ref[...]
    grown = jnp.exp(logits - jnp.max(logits, axis=1, keepdims=True))
    weight = grown / jnp.sum(grown, axis=1, keepdims=True)
    upper = weight.astype(jnp.bfloat16).astype(jnp.float32)
    lower = weight - upper
    row = lax.broadcasted_iota(jnp.int32, (count, count), 0)
    col = lax.broadcasted_iota(jnp.int32, (count, count), 1)
    lane = lax.broadcasted_iota(jnp.int32, (count, LANES), 1)
    packed = jnp.zeros((count, LANES), jnp.float32)
    for k in range(top):
        mine = ids[:, k : k + 1]
        same = jnp.zeros((count, count), jnp.float32)
        for other in range(top):
            same = same + jnp.where(mine == turned[other : other + 1, :], 1.0, 0.0)
        rank = jnp.sum(jnp.where(col < row, same, 0.0), axis=1, keepdims=True)
        code = mine.astype(jnp.float32) * CAP + rank
        packed = jnp.where(lane == k, code, packed)
        packed = jnp.where(lane == top + k, upper[:, k : k + 1], packed)
        packed = jnp.where(lane == 2 * top + k, lower[:, k : k + 1], packed)
    out_ref[...] = packed


def mix_kernel(tp_ref, parts_ref, full_ref, lean_ref, gain_ref, routes_ref, res_ref, out_ref, *, top):
    residual = full_ref[...]
    tp = parts_ref.shape[0]
    for k in range(tp):
        residual = residual + parts_ref[k]
    total = residual.shape[1]
    width = total // tp
    inverse = lax.rsqrt(jnp.sum(residual * residual, axis=1, keepdims=True) / total + EPSILON)
    logit = jnp.sum(residual * lean_ref[...], axis=1, keepdims=True) * inverse
    branch = jax.nn.sigmoid(logit)
    upper = branch.astype(jnp.bfloat16).astype(jnp.float32)
    own = jnp.zeros((residual.shape[0], width), jnp.float32)
    for k in range(tp):
        own = own + jnp.where(tp_ref[0] == k, residual[:, k * width : (k + 1) * width], 0.0)
    res_ref[...] = own
    mix = (own * inverse * gain_ref[...]).astype(jnp.bfloat16)
    routes = routes_ref[...]
    lane = lax.broadcasted_iota(jnp.int32, routes.shape, 1)
    routes = jnp.where(lane == 3 * top, upper, routes)
    routes = jnp.where(lane == 3 * top + 1, branch - upper, routes)
    notes = routes.astype(jnp.bfloat16)
    for k in range(out_ref.shape[0]):
        out_ref[k, :, :width] = mix
        out_ref[k, :, width:] = notes


def slot_hits(notes, first, line, plane, top):
    total = notes.shape[0]
    slots = plane * line * CAP
    row = lax.broadcasted_iota(jnp.int32, (total, slots), 0)
    col = lax.broadcasted_iota(jnp.int32, (total, slots), 1)
    code = (first + col // (line * CAP)) * CAP + col % CAP
    here = row // (total // line) == (col // CAP) % line
    code = jnp.where(here, code, -1).astype(jnp.float32)
    return [notes[:, k : k + 1] == code for k in range(top)]


def outward_kernel(first_ref, seen_ref, out_ref, *, top):
    line, seq, wide = seen_ref.shape
    width = wide - LANES
    plane, tp, items, _ = out_ref.shape
    slots = line * CAP
    notes = seen_ref[:, :, width:].reshape(line * seq, LANES).astype(jnp.float32)
    rows = seen_ref[:, :, :width].reshape(line * seq, width)
    hits = slot_hits(notes, first_ref[0], line, plane, top)
    select = sum(jnp.where(h, 1.0, 0.0) for h in hits).astype(jnp.bfloat16)
    placed = lax.dot_general(select, rows, TURNED, preferred_element_type=jnp.float32)
    placed = placed.astype(jnp.bfloat16).reshape(plane, slots, width)
    for k in range(tp):
        out_ref[:, k, :slots, :] = placed
    dealt = rows.astype(jnp.float32).reshape(plane, tp, items - slots, width)
    out_ref[:, :, slots:, :] = dealt.astype(jnp.bfloat16)


def weights_kernel(first_ref, seen_ref, upper_ref, lower_ref, *, top, plane):
    line, seq, wide = seen_ref.shape
    width = wide - LANES
    notes = seen_ref[:, :, width:].reshape(line * seq, LANES).astype(jnp.float32)
    hits = slot_hits(notes, first_ref[0], line, plane, top)
    upper_ref[...] = sum(
        jnp.where(h, notes[:, top + k : top + k + 1], 0.0) for k, h in enumerate(hits)
    ).astype(jnp.bfloat16)
    lower_ref[...] = sum(
        jnp.where(h, notes[:, 2 * top + k : 2 * top + k + 1], 0.0) for k, h in enumerate(hits)
    ).astype(jnp.bfloat16)


def expert_kernel(seen_ref, gate_ref, up_ref, down_ref, dense_ref, out_ref, *, slots):
    plane, tp, items, width = seen_ref.shape
    gate_pre = up_pre = 0.0
    for k in range(tp):
        rows = seen_ref[:, k, :slots, :].reshape(plane * slots, width)
        gate_pre = gate_pre + mm(rows, gate_ref[0, k * width : (k + 1) * width, :])
        up_pre = up_pre + mm(rows, up_ref[0, k * width : (k + 1) * width, :])
    act = clamped_unit(gate_pre, up_pre).astype(jnp.bfloat16)
    for k in range(tp):
        part = mm(act, down_ref[0, :, k * width : (k + 1) * width]).astype(jnp.bfloat16)
        out_ref[:, k, :slots, :] = part.reshape(plane, slots, width)
    units = dense_ref.shape[2] // 3
    dealt = items - slots
    gate_pre = up_pre = 0.0
    for k in range(tp):
        rows = seen_ref[:, k, slots:, :].astype(jnp.float32).reshape(plane * dealt, width)
        rows = rows.astype(jnp.bfloat16)
        gate = dense_ref[:, k, :units, :].reshape(plane * units, width)
        up = dense_ref[:, k, units : 2 * units, :].reshape(plane * units, width)
        gate_pre = gate_pre + lax.dot_general(
            rows, gate, ACROSS, preferred_element_type=jnp.float32
        )
        up_pre = up_pre + lax.dot_general(rows, up, ACROSS, preferred_element_type=jnp.float32)
    act = (gate_pre / (1.0 + jnp.exp(-gate_pre)) * up_pre).astype(jnp.bfloat16)
    for k in range(tp):
        down = dense_ref[:, k, 2 * units :, :].reshape(plane * units, width)
        part = mm(act, down).reshape(plane, dealt, width)
        out_ref[:, k, slots:, :] = part.astype(jnp.bfloat16)


def inward_kernel(seen_ref, line_ref, upper_ref, lower_ref, out_ref, *, top):
    line, seq, width = out_ref.shape
    plane, tp, items, _ = seen_ref.shape
    slots = line * CAP
    whole = jnp.zeros((plane, slots, width), jnp.float32)
    for k in range(tp):
        whole = whole + seen_ref[:, k, :slots, :].astype(jnp.float32)
    whole = whole.astype(jnp.bfloat16).reshape(plane * slots, width)
    routed = mm(upper_ref[...], whole) + mm(lower_ref[...], whole)
    dense = seen_ref[:, :, slots:, :].astype(jnp.float32).reshape(line * seq, width)
    notes = line_ref[:, :, width:].reshape(line * seq, LANES).astype(jnp.float32)
    branch = notes[:, 3 * top : 3 * top + 1] + notes[:, 3 * top + 1 : 3 * top + 2]
    back = (routed + branch * dense).astype(jnp.bfloat16)
    out_ref[...] = back.reshape(line, seq, width)


def shaped(shape, dtype):
    return jax.ShapeDtypeStruct(shape, dtype)


def body(
    hidden_in,
    norm_gain_attn,
    query_weight,
    key_weight,
    value_weight,
    query_gain,
    key_gain,
    lambda_head,
    sub_gain,
    out_weight,
    cache_key,
    cache_value,
    lengths,
    norm_gain_mix,
    route_ids,
    route_logits,
    expert_gate,
    expert_up,
    expert_down,
    dense_gate,
    dense_up,
    dense_down,
    branch_gate,
):
    seq, top = route_ids.shape
    width = hidden_in.shape[1]
    units = dense_down.shape[0]
    line = lax.axis_size("ep_0")
    plane = lax.axis_size("ep_1") * lax.axis_size("ep_2")
    tp = lax.axis_size("tp")
    slots = line * CAP
    dealt = line * seq // (plane * tp)
    lean = norm_gain_mix * branch_gate
    lean_high = lean.astype(jnp.bfloat16)
    lean_low = (lean - lean_high.astype(jnp.float32)).astype(jnp.bfloat16)
    extra = jnp.zeros((8, width), jnp.bfloat16).at[0].set(lean_high).at[1].set(lean_low)
    mine = jnp.concatenate([hidden_in, dense_gate.T, dense_up.T, dense_down, extra], axis=0)
    pieces = from_everyone(mine, "tp")
    full_rows = jnp.concatenate([pieces[k, :seq] for k in range(tp)], axis=1).astype(jnp.float32)
    past = seq + 3 * units
    lean_full = jnp.concatenate(
        [
            pieces[k, past : past + 1].astype(jnp.float32)
            + pieces[k, past + 1 : past + 2].astype(jnp.float32)
            for k in range(tp)
        ],
        axis=1,
    )
    width_total = full_rows.shape[1]
    dense_weights = from_everyone(pieces[:, seq:past], PLANE).reshape(plane, tp, 3 * units, width)
    routes = pl.pallas_call(
        routes_kernel, out_shape=shaped((seq, LANES), jnp.float32), name="routes"
    )(route_ids, route_ids.T, route_logits)
    normed = rms_scale(full_rows, norm_gain_attn).astype(jnp.bfloat16)
    head_out, key_rows, value_rows = attend(
        normed,
        query_weight,
        key_weight,
        value_weight,
        query_gain,
        key_gain,
        lambda_head,
        sub_gain,
        cache_key,
        cache_value,
        lengths,
    )
    head_terms = jnp.dot(head_out, out_weight, preferred_element_type=jnp.float32)
    head_terms, dense_weights = lax.optimization_barrier((head_terms, dense_weights))
    parts = from_everyone(head_terms, "tp")
    residual, message = pl.pallas_call(
        lambda *refs: mix_kernel(*refs, top=top),
        out_shape=(
            shaped((seq, width), jnp.float32),
            shaped((line, seq, width + LANES), jnp.bfloat16),
        ),
        in_specs=[SCALARS] + [WHOLE] * 5,
        name="mix",
    )(
        lax.axis_index("tp").reshape(1),
        parts,
        full_rows,
        lean_full,
        norm_gain_mix[None, :],
        routes,
    )
    seen = lax.all_to_all(message, "ep_0", 0, 0, tiled=True)
    first = (lax.axis_index("ep_0") * plane).reshape(1)
    outward = pl.pallas_call(
        lambda *refs: outward_kernel(*refs, top=top),
        out_shape=shaped((plane, tp, slots + dealt, width), jnp.bfloat16),
        in_specs=[SCALARS, WHOLE],
        name="outward",
    )(first, seen)
    arrived = lax.all_to_all(
        outward.reshape(plane * tp, slots + dealt, width), BLOCK, 0, 0, tiled=True
    ).reshape(plane, tp, slots + dealt, width)
    upper, lower = pl.pallas_call(
        lambda *refs: weights_kernel(*refs, top=top, plane=plane),
        out_shape=(
            shaped((line * seq, plane * slots), jnp.bfloat16),
            shaped((line * seq, plane * slots), jnp.bfloat16),
        ),
        in_specs=[SCALARS, WHOLE],
        name="weights",
    )(first, seen)
    sent = pl.pallas_call(
        lambda *refs: expert_kernel(*refs, slots=slots),
        out_shape=shaped((plane, tp, slots + dealt, width), jnp.bfloat16),
        name="experts",
    )(arrived, expert_gate, expert_up, expert_down, dense_weights)
    returned = lax.all_to_all(
        sent.reshape(plane * tp, slots + dealt, width), BLOCK, 0, 0, tiled=True
    ).reshape(plane, tp, slots + dealt, width)
    back = pl.pallas_call(
        lambda *refs: inward_kernel(*refs, top=top),
        out_shape=shaped((line, seq, width), jnp.bfloat16),
        name="inward",
    )(returned, seen, upper, lower)
    home = lax.all_to_all(back, "ep_0", 0, 0, tiled=True)
    layer_out = (residual + jnp.sum(home.astype(jnp.float32), axis=0)).astype(jnp.bfloat16)
    return (layer_out, key_rows, value_rows)


def solution(mesh):
    split = Mesh(mesh.devices.reshape(16, 4, 2, mesh.shape["tp"]), ("ep_0", "ep_1", "ep_2", "tp"))
    in_specs = (
        P(EP, "tp"),
        P(),
        P(None, "tp"),
        P(None, "tp"),
        P(None, "tp"),
        P(),
        P(),
        P("tp"),
        P(),
        P("tp", None),
        P(EP, None, "tp"),
        P(EP, None, "tp"),
        P(EP),
        P("tp"),
        P(EP, None),
        P(EP, None),
        P(EP, None, "tp"),
        P(EP, None, "tp"),
        P(EP, "tp", None),
        P("tp", EP),
        P("tp", EP),
        P(EP, "tp"),
        P("tp"),
    )
    out_specs = (P(EP, "tp"), P(EP, "tp"), P(EP, "tp"))
    return jax.shard_map(body, mesh=split, in_specs=in_specs, out_specs=out_specs, check_vma=False)
```

```python
import math

import jax
import jax.numpy as jnp
from jax import lax
from jax.experimental import pallas as pl
from jax.experimental.pallas import tpu as pltpu

from jax.sharding import Mesh
from jax.sharding import PartitionSpec as P


EP = ("ep_0", "ep_1", "ep_2")
BLOCK = ("ep_1", "ep_2", "tp")
CAP = 2


EPSILON = 1e-06
CLAMP_LIMIT = 7.0
SWISH_ALPHA = 1.702
OUT_SCALE = 0.2 + 0.6 * math.exp(-0.6)


def from_everyone(x, axis):
    copies = jnp.broadcast_to(x, (lax.axis_size(axis), *x.shape))
    return lax.all_to_all(copies, axis, split_axis=0, concat_axis=0, tiled=True)


def rms_scale(values, scale_gain):
    mean_square = jnp.mean(values * values, axis=-1, keepdims=True)
    return values * lax.rsqrt(mean_square + EPSILON) * scale_gain


def clamped_unit(gate_pre, up_pre):
    gate_cut = jnp.minimum(gate_pre, CLAMP_LIMIT)
    up_cut = jnp.clip(up_pre, -CLAMP_LIMIT, CLAMP_LIMIT)
    return (up_cut + 1.0) * gate_cut * jax.nn.sigmoid(SWISH_ALPHA * gate_cut)


def attend(
    normed,
    query_weight,
    key_weight,
    value_weight,
    query_gain,
    key_gain,
    lambda_head,
    sub_gain,
    cache_key,
    cache_value,
    lengths,
):
    seq_count = normed.shape[0]
    head_count = lambda_head.shape[0]
    qk_size = query_gain.shape[0] // 2
    val_size = value_weight.shape[1] // head_count
    cache_len = cache_key.shape[1]
    scale_factor = qk_size ** (-0.5)
    query_pre = jnp.dot(normed, query_weight, preferred_element_type=jnp.float32)
    query_rows = rms_scale(
        query_pre.reshape(seq_count, head_count, 2, qk_size), query_gain.reshape(2, qk_size)
    ).astype(jnp.bfloat16)
    key_pre = jnp.dot(normed, key_weight, preferred_element_type=jnp.float32)
    key_rows = rms_scale(
        key_pre.reshape(seq_count, head_count, 2, qk_size), key_gain.reshape(2, qk_size)
    ).astype(jnp.bfloat16)
    value_rows = jnp.dot(normed, value_weight, preferred_element_type=jnp.float32).astype(
        jnp.bfloat16
    )
    key_past = cache_key.reshape(seq_count, cache_len, head_count, 2, qk_size)
    past_score = (
        jnp.einsum("shmd,sjhmd->shmj", query_rows, key_past, preferred_element_type=jnp.float32)
        * scale_factor
    )
    own_score = (
        jnp.einsum("shmd,shmd->shm", query_rows, key_rows, preferred_element_type=jnp.float32)
        * scale_factor
    )
    valid_mask = lax.iota(jnp.int32, cache_len)[None, :] < lengths[:, None]
    past_exp = jnp.where(valid_mask[:, None, None, :], jnp.exp(past_score), 0.0)
    own_exp = jnp.exp(own_score)
    denominator = jnp.sum(past_exp, axis=-1) + own_exp
    past_prob = past_exp / denominator[..., None]
    own_prob = own_exp / denominator
    weight_past = (past_prob[:, :, 0] - lambda_head[None, :, None] * past_prob[:, :, 1]).astype(
        jnp.bfloat16
    )
    weight_own = (own_prob[:, :, 0] - lambda_head[None, :] * own_prob[:, :, 1]).astype(jnp.bfloat16)
    value_past = cache_value.reshape(seq_count, cache_len, head_count, val_size)
    head_mix = jnp.einsum(
        "shj,sjhe->she", weight_past, value_past, preferred_element_type=jnp.float32
    )
    own_value = value_rows.reshape(seq_count, head_count, val_size).astype(jnp.float32)
    head_mix = head_mix + weight_own.astype(jnp.float32)[..., None] * own_value
    head_out = (rms_scale(head_mix, sub_gain) * OUT_SCALE).astype(jnp.bfloat16)
    return (
        head_out.reshape(seq_count, head_count * val_size),
        key_rows.reshape(seq_count, -1),
        value_rows,
    )


LANES = 128
TURNED = (((0,), (0,)), ((), ()))
ACROSS = (((1,), (1,)), ((), ()))
SCALARS = pl.BlockSpec(memory_space=pltpu.SMEM)
LIMIT = pltpu.CompilerParams(vmem_limit_bytes=12 * 2**20)
WHOLE = pl.BlockSpec(memory_space=pltpu.VMEM)


def mm(a, b):
    return jnp.dot(a, b, preferred_element_type=jnp.float32)


def far(x):
    return pltpu.with_memory_space_constraint(x, pltpu.HBM)


def near(x):
    return pltpu.with_memory_space_constraint(x, pltpu.VMEM)


def opening_kernel(hidden_ref, gate_ref, up_ref, down_ref, gain_ref, branch_ref, out_ref):
    lean = gain_ref[...] * branch_ref[...]
    high = lean.astype(jnp.bfloat16).astype(jnp.float32)
    row = lax.broadcasted_iota(jnp.int32, (8, lean.shape[1]), 0)
    extra = jnp.where(row == 0, high, jnp.where(row == 1, lean - high, 0.0))
    extra = extra.astype(jnp.bfloat16)
    seq, units = hidden_ref.shape[0], down_ref.shape[0]
    past = seq + 3 * units
    for k in range(out_ref.shape[0]):
        out_ref[k, :seq, :] = hidden_ref[...]
        out_ref[k, seq : seq + units, :] = gate_ref[...]
        out_ref[k, seq + units : seq + 2 * units, :] = up_ref[...]
        out_ref[k, seq + 2 * units : past, :] = down_ref[...]
        out_ref[k, past:, :] = extra


def routes_kernel(ids_ref, turned_ref, logits_ref, out_ref):
    ids = ids_ref[...]
    turned = turned_ref[...]
    count, top = ids.shape
    logits = logits_ref[...]
    grown = jnp.exp(logits - jnp.max(logits, axis=1, keepdims=True))
    weight = grown / jnp.sum(grown, axis=1, keepdims=True)
    upper = weight.astype(jnp.bfloat16).astype(jnp.float32)
    lower = weight - upper
    row = lax.broadcasted_iota(jnp.int32, (count, count), 0)
    col = lax.broadcasted_iota(jnp.int32, (count, count), 1)
    lane = lax.broadcasted_iota(jnp.int32, (count, LANES), 1)
    packed = jnp.zeros((count, LANES), jnp.float32)
    for k in range(top):
        mine = ids[:, k : k + 1]
        same = jnp.zeros((count, count), jnp.float32)
        for other in range(top):
            same = same + jnp.where(mine == turned[other : other + 1, :], 1.0, 0.0)
        rank = jnp.sum(jnp.where(col < row, same, 0.0), axis=1, keepdims=True)
        code = mine.astype(jnp.float32) * CAP + rank
        packed = jnp.where(lane == k, code, packed)
        packed = jnp.where(lane == top + k, upper[:, k : k + 1], packed)
        packed = jnp.where(lane == 2 * top + k, lower[:, k : k + 1], packed)
    out_ref[...] = packed


def mix_kernel(tp_ref, parts_ref, pieces_ref, gain_ref, routes_ref, res_ref, out_ref, *, top):
    tp, seq, _ = parts_ref.shape
    past = pieces_ref.shape[1] - 8
    residual = jnp.concatenate([pieces_ref[k, :seq, :] for k in range(tp)], axis=1)
    residual = residual.astype(jnp.float32)
    for k in range(tp):
        residual = residual + parts_ref[k]
    ends = [pieces_ref[k, past:, :].astype(jnp.float32) for k in range(tp)]
    lean = jnp.concatenate([end[0:1] + end[1:2] for end in ends], axis=1)
    total = residual.shape[1]
    width = total // tp
    inverse = lax.rsqrt(jnp.sum(residual * residual, axis=1, keepdims=True) / total + EPSILON)
    logit = jnp.sum(residual * lean, axis=1, keepdims=True) * inverse
    branch = jax.nn.sigmoid(logit)
    upper = branch.astype(jnp.bfloat16).astype(jnp.float32)
    own = jnp.zeros((residual.shape[0], width), jnp.float32)
    for k in range(tp):
        own = own + jnp.where(tp_ref[0] == k, residual[:, k * width : (k + 1) * width], 0.0)
    res_ref[...] = own
    mix = (own * inverse * gain_ref[...]).astype(jnp.bfloat16)
    routes = routes_ref[...]
    lane = lax.broadcasted_iota(jnp.int32, routes.shape, 1)
    routes = jnp.where(lane == 3 * top, upper, routes)
    routes = jnp.where(lane == 3 * top + 1, branch - upper, routes)
    notes = routes.astype(jnp.bfloat16)
    for k in range(out_ref.shape[0]):
        out_ref[k, :, :width] = mix
        out_ref[k, :, width:] = notes


def slot_hits(notes, first, line, plane, top):
    total = notes.shape[0]
    slots = plane * line * CAP
    row = lax.broadcasted_iota(jnp.int32, (total, slots), 0)
    col = lax.broadcasted_iota(jnp.int32, (total, slots), 1)
    code = (first + col // (line * CAP)) * CAP + col % CAP
    here = row // (total // line) == (col // CAP) % line
    code = jnp.where(here, code, -1).astype(jnp.float32)
    return [notes[:, k : k + 1] == code for k in range(top)]


def outward_kernel(first_ref, seen_ref, out_ref, *, top):
    line, seq, wide = seen_ref.shape
    width = wide - LANES
    plane, tp, items, _ = out_ref.shape
    slots = line * CAP
    notes = seen_ref[:, :, width:].reshape(line * seq, LANES).astype(jnp.float32)
    rows = seen_ref[:, :, :width].reshape(line * seq, width)
    hits = slot_hits(notes, first_ref[0], line, plane, top)
    select = sum(jnp.where(h, 1.0, 0.0) for h in hits).astype(jnp.bfloat16)
    placed = lax.dot_general(select, rows, TURNED, preferred_element_type=jnp.float32)
    placed = placed.astype(jnp.bfloat16).reshape(plane, slots, width)
    for k in range(tp):
        out_ref[:, k, :slots, :] = placed
    dealt = rows.astype(jnp.float32).reshape(plane, tp, items - slots, width)
    out_ref[:, :, slots:, :] = dealt.astype(jnp.bfloat16)


def weights_kernel(first_ref, seen_ref, upper_ref, lower_ref, *, top, plane):
    line, seq, wide = seen_ref.shape
    width = wide - LANES
    notes = seen_ref[:, :, width:].reshape(line * seq, LANES).astype(jnp.float32)
    hits = slot_hits(notes, first_ref[0], line, plane, top)
    upper_ref[...] = sum(
        jnp.where(h, notes[:, top + k : top + k + 1], 0.0) for k, h in enumerate(hits)
    ).astype(jnp.bfloat16)
    lower_ref[...] = sum(
        jnp.where(h, notes[:, 2 * top + k : 2 * top + k + 1], 0.0) for k, h in enumerate(hits)
    ).astype(jnp.bfloat16)


def expert_kernel(
    seen_ref, gate_ref, up_ref, down_hbm, own_hbm, other_hbm, out_ref, down_ref, dense_ref, sems, *, slots
):
    fetches = [
        pltpu.make_async_copy(own_hbm, dense_ref.at[0], sems.at[0]),
        pltpu.make_async_copy(other_hbm, dense_ref.at[1], sems.at[1]),
        pltpu.make_async_copy(down_hbm, down_ref, sems.at[2]),
    ]
    for fetch in fetches:
        fetch.start()
    plane, tp, items, width = seen_ref.shape
    gate_pre = up_pre = 0.0
    for k in range(tp):
        rows = seen_ref[:, k, :slots, :].reshape(plane * slots, width)
        gate_pre = gate_pre + mm(rows, gate_ref[0, k * width : (k + 1) * width, :])
        up_pre = up_pre + mm(rows, up_ref[0, k * width : (k + 1) * width, :])
    act = clamped_unit(gate_pre, up_pre).astype(jnp.bfloat16)
    _, columns, _, rows_each, _ = dense_ref.shape
    units = rows_each // 3
    every = 2 * columns * units
    dealt = items - slots
    fetches[0].wait()
    fetches[1].wait()
    gate_pre = up_pre = 0.0
    for k in range(tp):
        rows = seen_ref[:, k, slots:, :].astype(jnp.float32).reshape(plane * dealt, width)
        rows = rows.astype(jnp.bfloat16)
        gate = dense_ref[:, :, k, :units, :].reshape(every, width)
        up = dense_ref[:, :, k, units : 2 * units, :].reshape(every, width)
        gate_pre = gate_pre + lax.dot_general(
            rows, gate, ACROSS, preferred_element_type=jnp.float32
        )
        up_pre = up_pre + lax.dot_general(rows, up, ACROSS, preferred_element_type=jnp.float32)
    dense_act = (gate_pre / (1.0 + jnp.exp(-gate_pre)) * up_pre).astype(jnp.bfloat16)
    for k in range(tp):
        down = dense_ref[:, :, k, 2 * units :, :].reshape(every, width)
        part = mm(dense_act, down).reshape(plane, dealt, width)
        out_ref[:, k, slots:, :] = part.astype(jnp.bfloat16)
    fetches[2].wait()
    for k in range(tp):
        part = mm(act, down_ref[0, :, k * width : (k + 1) * width]).astype(jnp.bfloat16)
        out_ref[:, k, :slots, :] = part.reshape(plane, slots, width)


def inward_kernel(seen_ref, line_ref, upper_ref, lower_ref, out_ref, *, top):
    line, seq, width = out_ref.shape
    plane, tp, _, _ = seen_ref.shape
    slots = line * CAP
    whole = jnp.zeros((plane, slots, width), jnp.float32)
    for k in range(tp):
        whole = whole + seen_ref[:, k, :slots, :].astype(jnp.float32)
    whole = whole.astype(jnp.bfloat16).reshape(plane * slots, width)
    routed = mm(upper_ref[...], whole) + mm(lower_ref[...], whole)
    dense = seen_ref[:, :, slots:, :].astype(jnp.float32).reshape(line * seq, width)
    notes = line_ref[:, :, width:].reshape(line * seq, LANES).astype(jnp.float32)
    branch = notes[:, 3 * top : 3 * top + 1] + notes[:, 3 * top + 1 : 3 * top + 2]
    back = (routed + branch * dense).astype(jnp.bfloat16)
    out_ref[...] = back.reshape(line, seq, width)


def shaped(shape, dtype):
    return jax.ShapeDtypeStruct(shape, dtype)


def body(
    hidden_in,
    norm_gain_attn,
    query_weight,
    key_weight,
    value_weight,
    query_gain,
    key_gain,
    lambda_head,
    sub_gain,
    out_weight,
    cache_key,
    cache_value,
    lengths,
    norm_gain_mix,
    route_ids,
    route_logits,
    expert_gate,
    expert_up,
    expert_down,
    dense_gate,
    dense_up,
    dense_down,
    branch_gate,
):
    seq, top = route_ids.shape
    width = hidden_in.shape[1]
    units = dense_down.shape[0]
    line = lax.axis_size("ep_0")
    plane = lax.axis_size("ep_1") * lax.axis_size("ep_2")
    tp = lax.axis_size("tp")
    slots = line * CAP
    dealt = line * seq // (plane * tp)
    past = seq + 3 * units
    mine = pl.pallas_call(
        opening_kernel, out_shape=shaped((tp, past + 8, width), jnp.bfloat16), name="opening", compiler_params=LIMIT
    )(
        *map(
            far,
            (
                hidden_in,
                dense_gate.T,
                dense_up.T,
                dense_down,
                norm_gain_mix[None, :],
                branch_gate[None, :],
            ),
        )
    )
    pieces = lax.all_to_all(mine, "tp", 0, 0, tiled=True)
    full_rows = jnp.concatenate([pieces[k, :seq] for k in range(tp)], axis=1).astype(jnp.float32)
    routes = pl.pallas_call(
        routes_kernel, out_shape=shaped((seq, LANES), jnp.float32), name="routes", compiler_params=LIMIT
    )(route_ids, route_ids.T, route_logits)
    normed = rms_scale(full_rows, norm_gain_attn).astype(jnp.bfloat16)
    head_out, key_rows, value_rows = attend(
        normed,
        query_weight,
        key_weight,
        value_weight,
        query_gain,
        key_gain,
        lambda_head,
        sub_gain,
        cache_key,
        cache_value,
        lengths,
    )
    head_terms = jnp.dot(head_out, out_weight, preferred_element_type=jnp.float32)
    parts = from_everyone(head_terms, "tp")
    residual, message = pl.pallas_call(
        lambda *refs: mix_kernel(*refs, top=top),
        out_shape=(
            shaped((seq, width), jnp.float32),
            shaped((line, seq, width + LANES), jnp.bfloat16),
        ),
        in_specs=[SCALARS] + [WHOLE] * 4,
        name="mix",
        compiler_params=LIMIT,
    )(
        lax.axis_index("tp").reshape(1),
        near(parts),
        near(pieces),
        norm_gain_mix[None, :],
        near(routes),
    )
    seen = lax.all_to_all(message, "ep_0", 0, 0, tiled=True)
    columns = lax.axis_size("ep_1")
    held = [pieces[:, seq:past]]
    for shift in range(1, columns):
        held.append(
            lax.ppermute(held[0], "ep_1", [(i, (i + shift) % columns) for i in range(columns)])
        )
    own_dense, seen = lax.optimization_barrier((jnp.stack(held), seen))
    seen = near(seen)
    other_dense = lax.ppermute(own_dense, "ep_2", [(0, 1), (1, 0)])
    first = (lax.axis_index("ep_0") * plane).reshape(1)
    outward = pl.pallas_call(
        lambda *refs: outward_kernel(*refs, top=top),
        out_shape=shaped((plane, tp, slots + dealt, width), jnp.bfloat16),
        in_specs=[SCALARS, WHOLE],
        name="outward",
        compiler_params=LIMIT,
    )(first, seen)
    arrived = lax.all_to_all(
        outward.reshape(plane * tp, slots + dealt, width), BLOCK, 0, 0, tiled=True
    ).reshape(plane, tp, slots + dealt, width)
    upper, lower = pl.pallas_call(
        lambda *refs: weights_kernel(*refs, top=top, plane=plane),
        out_shape=(
            shaped((line * seq, plane * slots), jnp.bfloat16),
            shaped((line * seq, plane * slots), jnp.bfloat16),
        ),
        in_specs=[SCALARS, WHOLE],
        name="weights",
        compiler_params=LIMIT,
    )(first, seen)
    sent = pl.pallas_call(
        lambda *refs: expert_kernel(*refs, slots=slots),
        out_shape=shaped((plane, tp, slots + dealt, width), jnp.bfloat16),
        in_specs=[WHOLE] * 3 + [pl.BlockSpec(memory_space=pl.ANY)] * 3,
        scratch_shapes=[
            pltpu.VMEM(expert_down.shape, expert_down.dtype),
            pltpu.VMEM((2, *own_dense.shape), own_dense.dtype),
            pltpu.SemaphoreType.DMA((3,)),
        ],
        name="experts",
        compiler_params=LIMIT,
    )(
        near(arrived),
        near(expert_gate),
        near(expert_up),
        far(expert_down),
        far(own_dense),
        far(other_dense),
    )
    returned = lax.all_to_all(
        sent.reshape(plane * tp, slots + dealt, width), BLOCK, 0, 0, tiled=True
    ).reshape(plane, tp, slots + dealt, width)
    back = pl.pallas_call(
        lambda *refs: inward_kernel(*refs, top=top),
        out_shape=shaped((line, seq, width), jnp.bfloat16),
        name="inward",
        compiler_params=LIMIT,
    )(near(returned), seen, near(upper), near(lower))
    home = lax.all_to_all(back, "ep_0", 0, 0, tiled=True)
    layer_out = (residual + jnp.sum(home.astype(jnp.float32), axis=0)).astype(jnp.bfloat16)
    return (layer_out, key_rows, value_rows)


def solution(mesh):
    split = Mesh(mesh.devices.reshape(16, 4, 2, mesh.shape["tp"]), ("ep_0", "ep_1", "ep_2", "tp"))
    in_specs = (
        P(EP, "tp"),
        P(),
        P(None, "tp"),
        P(None, "tp"),
        P(None, "tp"),
        P(),
        P(),
        P("tp"),
        P(),
        P("tp", None),
        P(EP, None, "tp"),
        P(EP, None, "tp"),
        P(EP),
        P("tp"),
        P(EP, None),
        P(EP, None),
        P(EP, None, "tp"),
        P(EP, None, "tp"),
        P(EP, "tp", None),
        P("tp", EP),
        P("tp", EP),
        P(EP, "tp"),
        P("tp"),
    )
    out_specs = (P(EP, "tp"), P(EP, "tp"), P(EP, "tp"))
    return jax.shard_map(body, mesh=split, in_specs=in_specs, out_specs=out_specs, check_vma=False)
```

```python
import math

import jax
import jax.numpy as jnp
from jax import lax
from jax.experimental import pallas as pl
from jax.experimental.pallas import tpu as pltpu

from jax.sharding import Mesh
from jax.sharding import PartitionSpec as P


EP = ("ep_0", "ep_1", "ep_2")
BLOCK = ("ep_1", "ep_2", "tp")
CAP = 2


EPSILON = 1e-06
CLAMP_LIMIT = 7.0
SWISH_ALPHA = 1.702
OUT_SCALE = 0.2 + 0.6 * math.exp(-0.6)


def from_everyone(x, axis):
    copies = jnp.broadcast_to(x, (lax.axis_size(axis), *x.shape))
    return lax.all_to_all(copies, axis, split_axis=0, concat_axis=0, tiled=True)


def rms_scale(values, scale_gain):
    mean_square = jnp.mean(values * values, axis=-1, keepdims=True)
    return values * lax.rsqrt(mean_square + EPSILON) * scale_gain


def clamped_unit(gate_pre, up_pre):
    gate_cut = jnp.minimum(gate_pre, CLAMP_LIMIT)
    up_cut = jnp.clip(up_pre, -CLAMP_LIMIT, CLAMP_LIMIT)
    return (up_cut + 1.0) * gate_cut * jax.nn.sigmoid(SWISH_ALPHA * gate_cut)


def attend(
    normed,
    query_weight,
    key_weight,
    value_weight,
    query_gain,
    key_gain,
    lambda_head,
    sub_gain,
    cache_key,
    cache_value,
    lengths,
):
    seq_count = normed.shape[0]
    head_count = lambda_head.shape[0]
    qk_size = query_gain.shape[0] // 2
    val_size = value_weight.shape[1] // head_count
    cache_len = cache_key.shape[1]
    scale_factor = qk_size ** (-0.5)
    query_pre = jnp.dot(normed, query_weight, preferred_element_type=jnp.float32)
    query_rows = rms_scale(
        query_pre.reshape(seq_count, head_count, 2, qk_size), query_gain.reshape(2, qk_size)
    ).astype(jnp.bfloat16)
    key_pre = jnp.dot(normed, key_weight, preferred_element_type=jnp.float32)
    key_rows = rms_scale(
        key_pre.reshape(seq_count, head_count, 2, qk_size), key_gain.reshape(2, qk_size)
    ).astype(jnp.bfloat16)
    value_rows = jnp.dot(normed, value_weight, preferred_element_type=jnp.float32).astype(
        jnp.bfloat16
    )
    key_past = cache_key.reshape(seq_count, cache_len, head_count, 2, qk_size)
    past_score = (
        jnp.einsum("shmd,sjhmd->shmj", query_rows, key_past, preferred_element_type=jnp.float32)
        * scale_factor
    )
    own_score = (
        jnp.einsum("shmd,shmd->shm", query_rows, key_rows, preferred_element_type=jnp.float32)
        * scale_factor
    )
    valid_mask = lax.iota(jnp.int32, cache_len)[None, :] < lengths[:, None]
    past_exp = jnp.where(valid_mask[:, None, None, :], jnp.exp(past_score), 0.0)
    own_exp = jnp.exp(own_score)
    denominator = jnp.sum(past_exp, axis=-1) + own_exp
    past_prob = past_exp / denominator[..., None]
    own_prob = own_exp / denominator
    weight_past = (past_prob[:, :, 0] - lambda_head[None, :, None] * past_prob[:, :, 1]).astype(
        jnp.bfloat16
    )
    weight_own = (own_prob[:, :, 0] - lambda_head[None, :] * own_prob[:, :, 1]).astype(jnp.bfloat16)
    value_past = cache_value.reshape(seq_count, cache_len, head_count, val_size)
    head_mix = jnp.einsum(
        "shj,sjhe->she", weight_past, value_past, preferred_element_type=jnp.float32
    )
    own_value = value_rows.reshape(seq_count, head_count, val_size).astype(jnp.float32)
    head_mix = head_mix + weight_own.astype(jnp.float32)[..., None] * own_value
    head_out = (rms_scale(head_mix, sub_gain) * OUT_SCALE).astype(jnp.bfloat16)
    return (
        head_out.reshape(seq_count, head_count * val_size),
        key_rows.reshape(seq_count, -1),
        value_rows,
    )


LANES = 128
TURNED = (((0,), (0,)), ((), ()))
ACROSS = (((1,), (1,)), ((), ()))
SCALARS = pl.BlockSpec(memory_space=pltpu.SMEM)
LIMIT = pltpu.CompilerParams(vmem_limit_bytes=12 * 2**20)
WHOLE = pl.BlockSpec(memory_space=pltpu.VMEM)


def mm(a, b):
    return jnp.dot(a, b, preferred_element_type=jnp.float32)


def far(x):
    return pltpu.with_memory_space_constraint(x, pltpu.HBM)


def near(x):
    return pltpu.with_memory_space_constraint(x, pltpu.VMEM)


def opening_kernel(hidden_ref, gate_ref, up_ref, down_ref, gain_ref, branch_ref, out_ref):
    lean = gain_ref[...] * branch_ref[...]
    high = lean.astype(jnp.bfloat16).astype(jnp.float32)
    row = lax.broadcasted_iota(jnp.int32, (8, lean.shape[1]), 0)
    extra = jnp.where(row == 0, high, jnp.where(row == 1, lean - high, 0.0))
    extra = extra.astype(jnp.bfloat16)
    seq, units = hidden_ref.shape[0], down_ref.shape[0]
    past = seq + 3 * units
    for k in range(out_ref.shape[0]):
        out_ref[k, :seq, :] = hidden_ref[...]
        out_ref[k, seq : seq + units, :] = gate_ref[...]
        out_ref[k, seq + units : seq + 2 * units, :] = up_ref[...]
        out_ref[k, seq + 2 * units : past, :] = down_ref[...]
        out_ref[k, past:, :] = extra


def routes_kernel(ids_ref, turned_ref, logits_ref, out_ref):
    ids = ids_ref[...]
    turned = turned_ref[...]
    count, top = ids.shape
    logits = logits_ref[...]
    grown = jnp.exp(logits - jnp.max(logits, axis=1, keepdims=True))
    weight = grown / jnp.sum(grown, axis=1, keepdims=True)
    upper = weight.astype(jnp.bfloat16).astype(jnp.float32)
    lower = weight - upper
    row = lax.broadcasted_iota(jnp.int32, (count, count), 0)
    col = lax.broadcasted_iota(jnp.int32, (count, count), 1)
    lane = lax.broadcasted_iota(jnp.int32, (count, LANES), 1)
    packed = jnp.zeros((count, LANES), jnp.float32)
    for k in range(top):
        mine = ids[:, k : k + 1]
        same = jnp.zeros((count, count), jnp.float32)
        for other in range(top):
            same = same + jnp.where(mine == turned[other : other + 1, :], 1.0, 0.0)
        rank = jnp.sum(jnp.where(col < row, same, 0.0), axis=1, keepdims=True)
        code = mine.astype(jnp.float32) * CAP + rank
        packed = jnp.where(lane == k, code, packed)
        packed = jnp.where(lane == top + k, upper[:, k : k + 1], packed)
        packed = jnp.where(lane == 2 * top + k, lower[:, k : k + 1], packed)
    out_ref[...] = packed


def mix_kernel(tp_ref, parts_ref, pieces_ref, gain_ref, routes_ref, res_ref, out_ref, *, top):
    tp, seq, _ = parts_ref.shape
    past = pieces_ref.shape[1] - 8
    residual = jnp.concatenate([pieces_ref[k, :seq, :] for k in range(tp)], axis=1)
    residual = residual.astype(jnp.float32)
    for k in range(tp):
        residual = residual + parts_ref[k].astype(jnp.float32)
    ends = [pieces_ref[k, past:, :].astype(jnp.float32) for k in range(tp)]
    lean = jnp.concatenate([end[0:1] + end[1:2] for end in ends], axis=1)
    total = residual.shape[1]
    width = total // tp
    inverse = lax.rsqrt(jnp.sum(residual * residual, axis=1, keepdims=True) / total + EPSILON)
    logit = jnp.sum(residual * lean, axis=1, keepdims=True) * inverse
    branch = jax.nn.sigmoid(logit)
    upper = branch.astype(jnp.bfloat16).astype(jnp.float32)
    own = jnp.zeros((residual.shape[0], width), jnp.float32)
    for k in range(tp):
        own = own + jnp.where(tp_ref[0] == k, residual[:, k * width : (k + 1) * width], 0.0)
    res_ref[...] = own
    mix = (own * inverse * gain_ref[...]).astype(jnp.bfloat16)
    routes = routes_ref[...]
    lane = lax.broadcasted_iota(jnp.int32, routes.shape, 1)
    routes = jnp.where(lane == 3 * top, upper, routes)
    routes = jnp.where(lane == 3 * top + 1, branch - upper, routes)
    notes = routes.astype(jnp.bfloat16)
    for k in range(out_ref.shape[0]):
        out_ref[k, :, :width] = mix
        out_ref[k, :, width:] = notes


def slot_hits(notes, first, line, plane, top):
    total = notes.shape[0]
    slots = plane * line * CAP
    row = lax.broadcasted_iota(jnp.int32, (total, slots), 0)
    col = lax.broadcasted_iota(jnp.int32, (total, slots), 1)
    code = (first + col // (line * CAP)) * CAP + col % CAP
    here = row // (total // line) == (col // CAP) % line
    code = jnp.where(here, code, -1).astype(jnp.float32)
    return [notes[:, k : k + 1] == code for k in range(top)]


def outward_kernel(first_ref, seen_ref, out_ref, *, top):
    line, seq, wide = seen_ref.shape
    width = wide - LANES
    plane, tp, items, _ = out_ref.shape
    slots = line * CAP
    notes = seen_ref[:, :, width:].reshape(line * seq, LANES).astype(jnp.float32)
    rows = seen_ref[:, :, :width].reshape(line * seq, width)
    hits = slot_hits(notes, first_ref[0], line, plane, top)
    select = sum(jnp.where(h, 1.0, 0.0) for h in hits).astype(jnp.bfloat16)
    placed = lax.dot_general(select, rows, TURNED, preferred_element_type=jnp.float32)
    placed = placed.astype(jnp.bfloat16).reshape(plane, slots, width)
    for k in range(tp):
        out_ref[:, k, :slots, :] = placed
    dealt = rows.astype(jnp.float32).reshape(plane, tp, items - slots, width)
    out_ref[:, :, slots:, :] = dealt.astype(jnp.bfloat16)


def weights_kernel(first_ref, seen_ref, upper_ref, lower_ref, *, top, plane):
    line, seq, wide = seen_ref.shape
    width = wide - LANES
    notes = seen_ref[:, :, width:].reshape(line * seq, LANES).astype(jnp.float32)
    hits = slot_hits(notes, first_ref[0], line, plane, top)
    upper_ref[...] = sum(
        jnp.where(h, notes[:, top + k : top + k + 1], 0.0) for k, h in enumerate(hits)
    ).astype(jnp.bfloat16)
    lower_ref[...] = sum(
        jnp.where(h, notes[:, 2 * top + k : 2 * top + k + 1], 0.0) for k, h in enumerate(hits)
    ).astype(jnp.bfloat16)


def expert_kernel(
    seen_ref, gate_ref, up_ref, down_hbm, own_hbm, other_hbm, out_ref, down_ref, dense_ref, sems, *, slots
):
    fetches = [
        pltpu.make_async_copy(own_hbm, dense_ref.at[0], sems.at[0]),
        pltpu.make_async_copy(other_hbm, dense_ref.at[1], sems.at[1]),
        pltpu.make_async_copy(down_hbm, down_ref, sems.at[2]),
    ]
    for fetch in fetches:
        fetch.start()
    plane, tp, items, width = seen_ref.shape
    gate_pre = up_pre = 0.0
    for k in range(tp):
        rows = seen_ref[:, k, :slots, :].reshape(plane * slots, width)
        gate_pre = gate_pre + mm(rows, gate_ref[0, k * width : (k + 1) * width, :])
        up_pre = up_pre + mm(rows, up_ref[0, k * width : (k + 1) * width, :])
    act = clamped_unit(gate_pre, up_pre).astype(jnp.bfloat16)
    _, columns, _, rows_each, _ = dense_ref.shape
    units = rows_each // 3
    every = 2 * columns * units
    dealt = items - slots
    fetches[0].wait()
    fetches[1].wait()
    gate_pre = up_pre = 0.0
    for k in range(tp):
        rows = seen_ref[:, k, slots:, :].astype(jnp.float32).reshape(plane * dealt, width)
        rows = rows.astype(jnp.bfloat16)
        gate = dense_ref[:, :, k, :units, :].reshape(every, width)
        up = dense_ref[:, :, k, units : 2 * units, :].reshape(every, width)
        gate_pre = gate_pre + lax.dot_general(
            rows, gate, ACROSS, preferred_element_type=jnp.float32
        )
        up_pre = up_pre + lax.dot_general(rows, up, ACROSS, preferred_element_type=jnp.float32)
    dense_act = (gate_pre / (1.0 + jnp.exp(-gate_pre)) * up_pre).astype(jnp.bfloat16)
    for k in range(tp):
        down = dense_ref[:, :, k, 2 * units :, :].reshape(every, width)
        part = mm(dense_act, down).reshape(plane, dealt, width)
        out_ref[:, k, slots:, :] = part.astype(jnp.bfloat16)
    fetches[2].wait()
    for k in range(tp):
        part = mm(act, down_ref[0, :, k * width : (k + 1) * width]).astype(jnp.bfloat16)
        out_ref[:, k, :slots, :] = part.reshape(plane, slots, width)


def inward_kernel(seen_ref, line_ref, upper_ref, lower_ref, out_ref, *, top):
    line, seq, width = out_ref.shape
    plane, tp, _, _ = seen_ref.shape
    slots = line * CAP
    whole = jnp.zeros((plane, slots, width), jnp.float32)
    for k in range(tp):
        whole = whole + seen_ref[:, k, :slots, :].astype(jnp.float32)
    whole = whole.astype(jnp.bfloat16).reshape(plane * slots, width)
    routed = mm(upper_ref[...], whole) + mm(lower_ref[...], whole)
    dense = seen_ref[:, :, slots:, :].astype(jnp.float32).reshape(line * seq, width)
    notes = line_ref[:, :, width:].reshape(line * seq, LANES).astype(jnp.float32)
    branch = notes[:, 3 * top : 3 * top + 1] + notes[:, 3 * top + 1 : 3 * top + 2]
    back = (routed + branch * dense).astype(jnp.bfloat16)
    out_ref[...] = back.reshape(line, seq, width)


def doubled(held, step):
    columns = lax.axis_size("ep_1")
    other = lax.ppermute(held, "ep_1", [(i, i ^ step) for i in range(columns)])
    return jnp.concatenate([held, other], axis=0)


def shaped(shape, dtype):
    return jax.ShapeDtypeStruct(shape, dtype)


def body(
    hidden_in,
    norm_gain_attn,
    query_weight,
    key_weight,
    value_weight,
    query_gain,
    key_gain,
    lambda_head,
    sub_gain,
    out_weight,
    cache_key,
    cache_value,
    lengths,
    norm_gain_mix,
    route_ids,
    route_logits,
    expert_gate,
    expert_up,
    expert_down,
    dense_gate,
    dense_up,
    dense_down,
    branch_gate,
):
    seq, top = route_ids.shape
    width = hidden_in.shape[1]
    units = dense_down.shape[0]
    line = lax.axis_size("ep_0")
    plane = lax.axis_size("ep_1") * lax.axis_size("ep_2")
    tp = lax.axis_size("tp")
    slots = line * CAP
    dealt = line * seq // (plane * tp)
    past = seq + 3 * units
    mine = pl.pallas_call(
        opening_kernel, out_shape=shaped((tp, past + 8, width), jnp.bfloat16), name="opening", compiler_params=LIMIT
    )(
        *map(
            far,
            (
                hidden_in,
                dense_gate.T,
                dense_up.T,
                dense_down,
                norm_gain_mix[None, :],
                branch_gate[None, :],
            ),
        )
    )
    pieces = lax.all_to_all(mine, "tp", 0, 0, tiled=True)
    full_rows = jnp.concatenate([pieces[k, :seq] for k in range(tp)], axis=1).astype(jnp.float32)
    routes = pl.pallas_call(
        routes_kernel, out_shape=shaped((seq, LANES), jnp.float32), name="routes", compiler_params=LIMIT
    )(route_ids, route_ids.T, route_logits)
    normed = rms_scale(full_rows, norm_gain_attn).astype(jnp.bfloat16)
    head_out, key_rows, value_rows = attend(
        normed,
        query_weight,
        key_weight,
        value_weight,
        query_gain,
        key_gain,
        lambda_head,
        sub_gain,
        cache_key,
        cache_value,
        lengths,
    )
    head_terms = jnp.dot(head_out, out_weight, preferred_element_type=jnp.float32)
    parts = from_everyone(head_terms.astype(jnp.bfloat16), "tp")
    columns = lax.axis_size("ep_1")
    steps = [1 << k for k in reversed(range(columns.bit_length() - 1))]
    own_dense = pieces[None, :, seq:past]
    for step in steps[:1]:
        own_dense = doubled(own_dense, step)
    residual, message = pl.pallas_call(
        lambda *refs: mix_kernel(*refs, top=top),
        out_shape=(
            shaped((seq, width), jnp.float32),
            shaped((line, seq, width + LANES), jnp.bfloat16),
        ),
        in_specs=[SCALARS] + [WHOLE] * 4,
        name="mix",
        compiler_params=LIMIT,
    )(
        lax.axis_index("tp").reshape(1),
        near(parts),
        near(pieces),
        norm_gain_mix[None, :],
        near(routes),
    )
    seen = lax.all_to_all(message, "ep_0", 0, 0, tiled=True)
    for step in steps[1:]:
        own_dense = doubled(own_dense, step)
    own_dense, seen = lax.optimization_barrier((own_dense, seen))
    seen = near(seen)
    other_dense = lax.ppermute(own_dense, "ep_2", [(0, 1), (1, 0)])
    first = (lax.axis_index("ep_0") * plane).reshape(1)
    outward = pl.pallas_call(
        lambda *refs: outward_kernel(*refs, top=top),
        out_shape=shaped((plane, tp, slots + dealt, width), jnp.bfloat16),
        in_specs=[SCALARS, WHOLE],
        name="outward",
        compiler_params=LIMIT,
    )(first, seen)
    arrived = lax.all_to_all(
        outward.reshape(plane * tp, slots + dealt, width), BLOCK, 0, 0, tiled=True
    ).reshape(plane, tp, slots + dealt, width)
    upper, lower = pl.pallas_call(
        lambda *refs: weights_kernel(*refs, top=top, plane=plane),
        out_shape=(
            shaped((line * seq, plane * slots), jnp.bfloat16),
            shaped((line * seq, plane * slots), jnp.bfloat16),
        ),
        in_specs=[SCALARS, WHOLE],
        name="weights",
        compiler_params=LIMIT,
    )(first, seen)
    sent = pl.pallas_call(
        lambda *refs: expert_kernel(*refs, slots=slots),
        out_shape=shaped((plane, tp, slots + dealt, width), jnp.bfloat16),
        in_specs=[WHOLE] * 3 + [pl.BlockSpec(memory_space=pl.ANY)] * 3,
        scratch_shapes=[
            pltpu.VMEM(expert_down.shape, expert_down.dtype),
            pltpu.VMEM((2, *own_dense.shape), own_dense.dtype),
            pltpu.SemaphoreType.DMA((3,)),
        ],
        name="experts",
        compiler_params=LIMIT,
    )(
        near(arrived),
        near(expert_gate),
        near(expert_up),
        far(expert_down),
        far(own_dense),
        far(other_dense),
    )
    returned = lax.all_to_all(
        sent.reshape(plane * tp, slots + dealt, width), BLOCK, 0, 0, tiled=True
    ).reshape(plane, tp, slots + dealt, width)
    back = pl.pallas_call(
        lambda *refs: inward_kernel(*refs, top=top),
        out_shape=shaped((line, seq, width), jnp.bfloat16),
        name="inward",
        compiler_params=LIMIT,
    )(near(returned), seen, near(upper), near(lower))
    home = lax.all_to_all(back, "ep_0", 0, 0, tiled=True)
    layer_out = (residual + jnp.sum(home.astype(jnp.float32), axis=0)).astype(jnp.bfloat16)
    return (layer_out, key_rows, value_rows)


def solution(mesh):
    split = Mesh(mesh.devices.reshape(16, 4, 2, mesh.shape["tp"]), ("ep_0", "ep_1", "ep_2", "tp"))
    in_specs = (
        P(EP, "tp"),
        P(),
        P(None, "tp"),
        P(None, "tp"),
        P(None, "tp"),
        P(),
        P(),
        P("tp"),
        P(),
        P("tp", None),
        P(EP, None, "tp"),
        P(EP, None, "tp"),
        P(EP),
        P("tp"),
        P(EP, None),
        P(EP, None),
        P(EP, None, "tp"),
        P(EP, None, "tp"),
        P(EP, "tp", None),
        P("tp", EP),
        P("tp", EP),
        P(EP, "tp"),
        P("tp"),
    )
    out_specs = (P(EP, "tp"), P(EP, "tp"), P(EP, "tp"))
    return jax.shard_map(body, mesh=split, in_specs=in_specs, out_specs=out_specs, check_vma=False)
```

```python
import math

import jax
import jax.numpy as jnp
from jax import lax
from jax.experimental import pallas as pl
from jax.experimental.pallas import tpu as pltpu

from jax.sharding import Mesh
from jax.sharding import PartitionSpec as P


EP = ("ep_0", "ep_1", "ep_2")
BLOCK = ("ep_1", "ep_2", "tp")
CAP = 2


EPSILON = 1e-06
CLAMP_LIMIT = 7.0
SWISH_ALPHA = 1.702
OUT_SCALE = 0.2 + 0.6 * math.exp(-0.6)


def clamped_unit(gate_pre, up_pre):
    gate_cut = jnp.minimum(gate_pre, CLAMP_LIMIT)
    up_cut = jnp.clip(up_pre, -CLAMP_LIMIT, CLAMP_LIMIT)
    return (up_cut + 1.0) * gate_cut * jax.nn.sigmoid(SWISH_ALPHA * gate_cut)


LANES = 128
TURNED = (((0,), (0,)), ((), ()))
ACROSS = (((1,), (1,)), ((), ()))
SCALARS = pl.BlockSpec(memory_space=pltpu.SMEM)
LIMIT = pltpu.CompilerParams(vmem_limit_bytes=12 * 2**20)
WHOLE = pl.BlockSpec(memory_space=pltpu.VMEM)


def mm(a, b):
    return jnp.dot(a, b, preferred_element_type=jnp.float32)


def kept(x):
    return pltpu.VMEM(x.shape, x.dtype)


def far(x):
    return pltpu.with_memory_space_constraint(x, pltpu.HBM)


def near(x):
    return pltpu.with_memory_space_constraint(x, pltpu.VMEM)


def opening_kernel(hidden_ref, gate_ref, up_ref, down_ref, gain_ref, branch_ref, out_ref):
    lean = gain_ref[...] * branch_ref[...]
    high = lean.astype(jnp.bfloat16).astype(jnp.float32)
    row = lax.broadcasted_iota(jnp.int32, (8, lean.shape[1]), 0)
    extra = jnp.where(row == 0, high, jnp.where(row == 1, lean - high, 0.0))
    extra = extra.astype(jnp.bfloat16)
    seq, units = hidden_ref.shape[0], down_ref.shape[0]
    past = seq + 3 * units
    for k in range(out_ref.shape[0]):
        out_ref[k, :seq, :] = hidden_ref[...]
        out_ref[k, seq : seq + units, :] = gate_ref[...]
        out_ref[k, seq + units : seq + 2 * units, :] = up_ref[...]
        out_ref[k, seq + 2 * units : past, :] = down_ref[...]
        out_ref[k, past:, :] = extra


def routes_kernel(ids_ref, turned_ref, logits_ref, out_ref):
    ids = ids_ref[...]
    turned = turned_ref[...]
    count, top = ids.shape
    logits = logits_ref[...]
    grown = jnp.exp(logits - jnp.max(logits, axis=1, keepdims=True))
    weight = grown / jnp.sum(grown, axis=1, keepdims=True)
    upper = weight.astype(jnp.bfloat16).astype(jnp.float32)
    lower = weight - upper
    row = lax.broadcasted_iota(jnp.int32, (count, count), 0)
    col = lax.broadcasted_iota(jnp.int32, (count, count), 1)
    lane = lax.broadcasted_iota(jnp.int32, (count, LANES), 1)
    packed = jnp.zeros((count, LANES), jnp.float32)
    for k in range(top):
        mine = ids[:, k : k + 1]
        same = jnp.zeros((count, count), jnp.float32)
        for other in range(top):
            same = same + jnp.where(mine == turned[other : other + 1, :], 1.0, 0.0)
        rank = jnp.sum(jnp.where(col < row, same, 0.0), axis=1, keepdims=True)
        code = mine.astype(jnp.float32) * CAP + rank
        packed = jnp.where(lane == k, code, packed)
        packed = jnp.where(lane == top + k, upper[:, k : k + 1], packed)
        packed = jnp.where(lane == 2 * top + k, lower[:, k : k + 1], packed)
    out_ref[...] = packed


def stage_kernel(*refs):
    count = len(refs) // 2
    sems = refs[-1]
    moves = [
        pltpu.make_async_copy(refs[k], refs[count + k], sems.at[k]) for k in range(count)
    ]
    for move in moves:
        move.start()
    for move in moves:
        move.wait()


def attend_kernel(
    lambda_ref,
    pieces_ref,
    gain_ref,
    query_ref,
    key_ref,
    value_ref,
    query_gain_ref,
    key_gain_ref,
    sub_ref,
    out_weight_ref,
    past_key_ref,
    past_value_ref,
    lengths_ref,
    out_ref,
    key_rows_ref,
    value_rows_ref,
):
    seq, past, size = past_key_ref.shape
    tp = pieces_ref.shape[0]
    half = size // 2
    full = jnp.concatenate([pieces_ref[k, :seq, :] for k in range(tp)], axis=1)
    full = full.astype(jnp.float32)
    square = jnp.sum(full * full, axis=1, keepdims=True) / full.shape[1]
    normed = (full * lax.rsqrt(square + EPSILON) * gain_ref[...]).astype(jnp.bfloat16)
    first = lax.broadcasted_iota(jnp.int32, (seq, size), 1) < half

    def halves(x):
        return (
            jnp.sum(jnp.where(first, x, 0.0), axis=1, keepdims=True),
            jnp.sum(jnp.where(first, 0.0, x), axis=1, keepdims=True),
        )

    def scaled(x, gain):
        low, high = halves(x * x)
        inverse = jnp.where(
            first, lax.rsqrt(low / half + EPSILON), lax.rsqrt(high / half + EPSILON)
        )
        return (x * inverse * gain).astype(jnp.bfloat16)

    query = scaled(mm(normed, query_ref[...]), query_gain_ref[...])
    key = scaled(mm(normed, key_ref[...]), key_gain_ref[...])
    value = mm(normed, value_ref[...]).astype(jnp.bfloat16)
    key_rows_ref[...] = key
    value_rows_ref[...] = value
    query = query.astype(jnp.float32)
    both = jnp.concatenate(
        [jnp.where(first, query, 0.0), jnp.where(first, 0.0, query)], axis=0
    )
    row = lax.broadcasted_iota(jnp.int32, (2 * seq, size), 0) % seq
    score = jnp.zeros((2 * seq, past), jnp.float32)
    for k in range(seq):
        mine = jnp.where(row == k, both, 0.0).astype(jnp.bfloat16)
        score = score + lax.dot_general(
            mine, past_key_ref[k], ACROSS, preferred_element_type=jnp.float32
        )
    scale = half**-0.5
    valid = lax.broadcasted_iota(jnp.int32, (seq, past), 1) < lengths_ref[...]
    own = [jnp.exp(o * scale) for o in halves(query * key.astype(jnp.float32))]
    grown = [
        jnp.where(valid, jnp.exp(score[m * seq : (m + 1) * seq] * scale), 0.0) for m in range(2)
    ]
    total = [jnp.sum(g, axis=1, keepdims=True) + o for g, o in zip(grown, own)]
    share = lambda_ref[0]
    weight = (grown[0] / total[0] - share * (grown[1] / total[1])).astype(jnp.bfloat16)
    weight_own = (own[0] / total[0] - share * (own[1] / total[1])).astype(jnp.bfloat16)
    weight = weight.astype(jnp.float32)
    row = lax.broadcasted_iota(jnp.int32, (seq, past), 0)
    mixed = weight_own.astype(jnp.float32) * value.astype(jnp.float32)
    for k in range(seq):
        mine = jnp.where(row == k, weight, 0.0).astype(jnp.bfloat16)
        mixed = mixed + mm(mine, past_value_ref[k])
    square = jnp.sum(mixed * mixed, axis=1, keepdims=True) / size
    head = mixed * lax.rsqrt(square + EPSILON) * sub_ref[...] * OUT_SCALE
    part = mm(head.astype(jnp.bfloat16), out_weight_ref[...]).astype(jnp.bfloat16)
    for k in range(tp):
        out_ref[k] = part


def mix_kernel(tp_ref, parts_ref, pieces_ref, gain_ref, routes_ref, res_ref, out_ref, *, top):
    tp, seq, _ = parts_ref.shape
    past = pieces_ref.shape[1] - 8
    residual = jnp.concatenate([pieces_ref[k, :seq, :] for k in range(tp)], axis=1)
    residual = residual.astype(jnp.float32)
    for k in range(tp):
        residual = residual + parts_ref[k].astype(jnp.float32)
    ends = [pieces_ref[k, past:, :].astype(jnp.float32) for k in range(tp)]
    lean = jnp.concatenate([end[0:1] + end[1:2] for end in ends], axis=1)
    total = residual.shape[1]
    width = total // tp
    inverse = lax.rsqrt(jnp.sum(residual * residual, axis=1, keepdims=True) / total + EPSILON)
    logit = jnp.sum(residual * lean, axis=1, keepdims=True) * inverse
    branch = jax.nn.sigmoid(logit)
    upper = branch.astype(jnp.bfloat16).astype(jnp.float32)
    own = jnp.zeros((residual.shape[0], width), jnp.float32)
    for k in range(tp):
        own = own + jnp.where(tp_ref[0] == k, residual[:, k * width : (k + 1) * width], 0.0)
    res_ref[...] = own
    mix = (own * inverse * gain_ref[...]).astype(jnp.bfloat16)
    routes = routes_ref[...]
    lane = lax.broadcasted_iota(jnp.int32, routes.shape, 1)
    routes = jnp.where(lane == 3 * top, upper, routes)
    routes = jnp.where(lane == 3 * top + 1, branch - upper, routes)
    notes = routes.astype(jnp.bfloat16)
    for k in range(out_ref.shape[0]):
        out_ref[k, :, :width] = mix
        out_ref[k, :, width:] = notes


def slot_hits(notes, first, line, plane, top):
    total = notes.shape[0]
    slots = plane * line * CAP
    row = lax.broadcasted_iota(jnp.int32, (total, slots), 0)
    col = lax.broadcasted_iota(jnp.int32, (total, slots), 1)
    code = (first + col // (line * CAP)) * CAP + col % CAP
    here = row // (total // line) == (col // CAP) % line
    code = jnp.where(here, code, -1).astype(jnp.float32)
    return [notes[:, k : k + 1] == code for k in range(top)]


def outward_kernel(first_ref, seen_ref, out_ref, *, top):
    line, seq, wide = seen_ref.shape
    width = wide - LANES
    plane, tp, items, _ = out_ref.shape
    slots = line * CAP
    notes = seen_ref[:, :, width:].reshape(line * seq, LANES).astype(jnp.float32)
    rows = seen_ref[:, :, :width].reshape(line * seq, width)
    hits = slot_hits(notes, first_ref[0], line, plane, top)
    select = sum(jnp.where(h, 1.0, 0.0) for h in hits).astype(jnp.bfloat16)
    placed = lax.dot_general(select, rows, TURNED, preferred_element_type=jnp.float32)
    placed = placed.astype(jnp.bfloat16).reshape(plane, slots, width)
    for k in range(tp):
        out_ref[:, k, :slots, :] = placed
    dealt = rows.astype(jnp.float32).reshape(plane, tp, items - slots, width)
    out_ref[:, :, slots:, :] = dealt.astype(jnp.bfloat16)


def weights_kernel(first_ref, seen_ref, upper_ref, lower_ref, *, top, plane):
    line, seq, wide = seen_ref.shape
    width = wide - LANES
    notes = seen_ref[:, :, width:].reshape(line * seq, LANES).astype(jnp.float32)
    hits = slot_hits(notes, first_ref[0], line, plane, top)
    upper_ref[...] = sum(
        jnp.where(h, notes[:, top + k : top + k + 1], 0.0) for k, h in enumerate(hits)
    ).astype(jnp.bfloat16)
    lower_ref[...] = sum(
        jnp.where(h, notes[:, 2 * top + k : 2 * top + k + 1], 0.0) for k, h in enumerate(hits)
    ).astype(jnp.bfloat16)


def expert_kernel(
    seen_ref, gate_ref, up_ref, down_hbm, own_hbm, other_hbm, out_ref, down_ref, dense_ref, sems, *, slots
):
    fetches = [
        pltpu.make_async_copy(own_hbm, dense_ref.at[0], sems.at[0]),
        pltpu.make_async_copy(other_hbm, dense_ref.at[1], sems.at[1]),
        pltpu.make_async_copy(down_hbm, down_ref, sems.at[2]),
    ]
    for fetch in fetches:
        fetch.start()
    plane, tp, items, width = seen_ref.shape
    gate_pre = up_pre = 0.0
    for k in range(tp):
        rows = seen_ref[:, k, :slots, :].reshape(plane * slots, width)
        gate_pre = gate_pre + mm(rows, gate_ref[0, k * width : (k + 1) * width, :])
        up_pre = up_pre + mm(rows, up_ref[0, k * width : (k + 1) * width, :])
    act = clamped_unit(gate_pre, up_pre).astype(jnp.bfloat16)
    _, columns, _, rows_each, _ = dense_ref.shape
    units = rows_each // 3
    every = 2 * columns * units
    dealt = items - slots
    fetches[0].wait()
    fetches[1].wait()
    gate_pre = up_pre = 0.0
    for k in range(tp):
        rows = seen_ref[:, k, slots:, :].astype(jnp.float32).reshape(plane * dealt, width)
        rows = rows.astype(jnp.bfloat16)
        gate = dense_ref[:, :, k, :units, :].reshape(every, width)
        up = dense_ref[:, :, k, units : 2 * units, :].reshape(every, width)
        gate_pre = gate_pre + lax.dot_general(
            rows, gate, ACROSS, preferred_element_type=jnp.float32
        )
        up_pre = up_pre + lax.dot_general(rows, up, ACROSS, preferred_element_type=jnp.float32)
    dense_act = (gate_pre / (1.0 + jnp.exp(-gate_pre)) * up_pre).astype(jnp.bfloat16)
    for k in range(tp):
        down = dense_ref[:, :, k, 2 * units :, :].reshape(every, width)
        part = mm(dense_act, down).reshape(plane, dealt, width)
        out_ref[:, k, slots:, :] = part.astype(jnp.bfloat16)
    fetches[2].wait()
    for k in range(tp):
        part = mm(act, down_ref[0, :, k * width : (k + 1) * width]).astype(jnp.bfloat16)
        out_ref[:, k, :slots, :] = part.reshape(plane, slots, width)


def inward_kernel(seen_ref, line_ref, upper_ref, lower_ref, out_ref, *, top):
    line, seq, width = out_ref.shape
    plane, tp, _, _ = seen_ref.shape
    slots = line * CAP
    whole = jnp.zeros((plane, slots, width), jnp.float32)
    for k in range(tp):
        whole = whole + seen_ref[:, k, :slots, :].astype(jnp.float32)
    whole = whole.astype(jnp.bfloat16).reshape(plane * slots, width)
    routed = mm(upper_ref[...], whole) + mm(lower_ref[...], whole)
    dense = seen_ref[:, :, slots:, :].astype(jnp.float32).reshape(line * seq, width)
    notes = line_ref[:, :, width:].reshape(line * seq, LANES).astype(jnp.float32)
    branch = notes[:, 3 * top : 3 * top + 1] + notes[:, 3 * top + 1 : 3 * top + 2]
    back = (routed + branch * dense).astype(jnp.bfloat16)
    out_ref[...] = back.reshape(line, seq, width)


def doubled(held, step):
    columns = lax.axis_size("ep_1")
    other = lax.ppermute(held, "ep_1", [(i, i ^ step) for i in range(columns)])
    return jnp.concatenate([held, other], axis=0)


def shaped(shape, dtype):
    return jax.ShapeDtypeStruct(shape, dtype)


def body(
    hidden_in,
    norm_gain_attn,
    query_weight,
    key_weight,
    value_weight,
    query_gain,
    key_gain,
    lambda_head,
    sub_gain,
    out_weight,
    cache_key,
    cache_value,
    lengths,
    norm_gain_mix,
    route_ids,
    route_logits,
    expert_gate,
    expert_up,
    expert_down,
    dense_gate,
    dense_up,
    dense_down,
    branch_gate,
):
    seq, top = route_ids.shape
    width = hidden_in.shape[1]
    units = dense_down.shape[0]
    line = lax.axis_size("ep_0")
    plane = lax.axis_size("ep_1") * lax.axis_size("ep_2")
    tp = lax.axis_size("tp")
    slots = line * CAP
    dealt = line * seq // (plane * tp)
    past = seq + 3 * units
    mine = pl.pallas_call(
        opening_kernel, out_shape=shaped((tp, past + 8, width), jnp.bfloat16), name="opening", compiler_params=LIMIT
    )(
        *map(
            far,
            (
                hidden_in,
                dense_gate.T,
                dense_up.T,
                dense_down,
                norm_gain_mix[None, :],
                branch_gate[None, :],
            ),
        )
    )
    pieces = lax.all_to_all(mine, "tp", 0, 0, tiled=True)
    needed = (
        norm_gain_attn[None, :],
        query_weight,
        key_weight,
        value_weight,
        query_gain[None, :],
        key_gain[None, :],
        sub_gain[None, :],
        out_weight,
        cache_key,
        cache_value,
        norm_gain_mix[None, :],
    )
    *staged, gain_here = pl.pallas_call(
        stage_kernel,
        out_shape=tuple(map(kept, needed)),
        in_specs=[pl.BlockSpec(memory_space=pl.ANY)] * len(needed),
        out_specs=(WHOLE,) * len(needed),
        scratch_shapes=[pltpu.SemaphoreType.DMA((len(needed),))],
        name="stage",
        compiler_params=LIMIT,
    )(*map(far, needed))
    routes = pl.pallas_call(
        routes_kernel, out_shape=shaped((seq, LANES), jnp.float32), name="routes", compiler_params=LIMIT
    )(route_ids, route_ids.T, route_logits)
    size = value_weight.shape[1]
    parts, key_rows, value_rows = pl.pallas_call(
        attend_kernel,
        out_shape=(
            shaped((tp, seq, out_weight.shape[1]), jnp.bfloat16),
            shaped((seq, size), jnp.bfloat16),
            shaped((seq, size), jnp.bfloat16),
        ),
        in_specs=[SCALARS] + [WHOLE] * 12,
        name="attend",
        compiler_params=LIMIT,
    )(
        lambda_head,
        near(pieces),
        *map(near, staged),
        near(lengths[:, None]),
    )
    parts = lax.all_to_all(parts, "tp", 0, 0, tiled=True)
    columns = lax.axis_size("ep_1")
    steps = [1 << k for k in reversed(range(columns.bit_length() - 1))]
    own_dense = pieces[None, :, seq:past]
    for step in steps[:1]:
        own_dense = doubled(own_dense, step)
    residual, message = pl.pallas_call(
        lambda *refs: mix_kernel(*refs, top=top),
        out_shape=(
            shaped((seq, width), jnp.float32),
            shaped((line, seq, width + LANES), jnp.bfloat16),
        ),
        in_specs=[SCALARS] + [WHOLE] * 4,
        name="mix",
        compiler_params=LIMIT,
    )(
        lax.axis_index("tp").reshape(1),
        near(parts),
        near(pieces),
        near(gain_here),
        near(routes),
    )
    seen = lax.all_to_all(message, "ep_0", 0, 0, tiled=True)
    for step in steps[1:]:
        own_dense = doubled(own_dense, step)
    own_dense, seen = lax.optimization_barrier((own_dense, seen))
    seen = near(seen)
    other_dense = lax.ppermute(own_dense, "ep_2", [(0, 1), (1, 0)])
    first = (lax.axis_index("ep_0") * plane).reshape(1)
    outward = pl.pallas_call(
        lambda *refs: outward_kernel(*refs, top=top),
        out_shape=shaped((plane, tp, slots + dealt, width), jnp.bfloat16),
        in_specs=[SCALARS, WHOLE],
        name="outward",
        compiler_params=LIMIT,
    )(first, seen)
    arrived = lax.all_to_all(
        outward.reshape(plane * tp, slots + dealt, width), BLOCK, 0, 0, tiled=True
    ).reshape(plane, tp, slots + dealt, width)
    upper, lower = pl.pallas_call(
        lambda *refs: weights_kernel(*refs, top=top, plane=plane),
        out_shape=(
            shaped((line * seq, plane * slots), jnp.bfloat16),
            shaped((line * seq, plane * slots), jnp.bfloat16),
        ),
        in_specs=[SCALARS, WHOLE],
        name="weights",
        compiler_params=LIMIT,
    )(first, seen)
    sent = pl.pallas_call(
        lambda *refs: expert_kernel(*refs, slots=slots),
        out_shape=shaped((plane, tp, slots + dealt, width), jnp.bfloat16),
        in_specs=[WHOLE] * 3 + [pl.BlockSpec(memory_space=pl.ANY)] * 3,
        scratch_shapes=[
            pltpu.VMEM(expert_down.shape, expert_down.dtype),
            pltpu.VMEM((2, *own_dense.shape), own_dense.dtype),
            pltpu.SemaphoreType.DMA((3,)),
        ],
        name="experts",
        compiler_params=LIMIT,
    )(
        near(arrived),
        near(expert_gate),
        near(expert_up),
        far(expert_down),
        far(own_dense),
        far(other_dense),
    )
    returned = lax.all_to_all(
        sent.reshape(plane * tp, slots + dealt, width), BLOCK, 0, 0, tiled=True
    ).reshape(plane, tp, slots + dealt, width)
    back = pl.pallas_call(
        lambda *refs: inward_kernel(*refs, top=top),
        out_shape=shaped((line, seq, width), jnp.bfloat16),
        name="inward",
        compiler_params=LIMIT,
    )(near(returned), seen, near(upper), near(lower))
    home = lax.all_to_all(back, "ep_0", 0, 0, tiled=True)
    layer_out = (residual + jnp.sum(home.astype(jnp.float32), axis=0)).astype(jnp.bfloat16)
    return (layer_out, key_rows, value_rows)


def solution(mesh):
    split = Mesh(mesh.devices.reshape(16, 4, 2, mesh.shape["tp"]), ("ep_0", "ep_1", "ep_2", "tp"))
    in_specs = (
        P(EP, "tp"),
        P(),
        P(None, "tp"),
        P(None, "tp"),
        P(None, "tp"),
        P(),
        P(),
        P("tp"),
        P(),
        P("tp", None),
        P(EP, None, "tp"),
        P(EP, None, "tp"),
        P(EP),
        P("tp"),
        P(EP, None),
        P(EP, None),
        P(EP, None, "tp"),
        P(EP, None, "tp"),
        P(EP, "tp", None),
        P("tp", EP),
        P("tp", EP),
        P(EP, "tp"),
        P("tp"),
    )
    out_specs = (P(EP, "tp"), P(EP, "tp"), P(EP, "tp"))
    return jax.shard_map(body, mesh=split, in_specs=in_specs, out_specs=out_specs, check_vma=False)
```

```python
import math

import jax
import jax.numpy as jnp
from jax import lax
from jax.experimental import pallas as pl
from jax.experimental.pallas import tpu as pltpu

from jax.sharding import Mesh
from jax.sharding import PartitionSpec as P


EP = ("ep_0", "ep_1", "ep_2")
BLOCK = ("ep_1", "ep_2", "tp")
CAP = 2


EPSILON = 1e-06
CLAMP_LIMIT = 7.0
SWISH_ALPHA = 1.702
OUT_SCALE = 0.2 + 0.6 * math.exp(-0.6)


def clamped_unit(gate_pre, up_pre):
    gate_cut = jnp.minimum(gate_pre, CLAMP_LIMIT)
    up_cut = jnp.clip(up_pre, -CLAMP_LIMIT, CLAMP_LIMIT)
    return (up_cut + 1.0) * gate_cut * jax.nn.sigmoid(SWISH_ALPHA * gate_cut)


LANES = 128
TURNED = (((0,), (0,)), ((), ()))
ACROSS = (((1,), (1,)), ((), ()))
SCALARS = pl.BlockSpec(memory_space=pltpu.SMEM)
LIMIT = pltpu.CompilerParams(vmem_limit_bytes=12 * 2**20)
WHOLE = pl.BlockSpec(memory_space=pltpu.VMEM)


def mm(a, b):
    return jnp.dot(a, b, preferred_element_type=jnp.float32)


def sent_to_hbm(shape, dtype):
    return pltpu.HBM(shape, dtype)


def kept(x):
    return pltpu.VMEM(x.shape, x.dtype)


def far(x):
    return pltpu.with_memory_space_constraint(x, pltpu.HBM)


def near(x):
    return pltpu.with_memory_space_constraint(x, pltpu.VMEM)


def opening_kernel(hidden_ref, gate_ref, up_ref, down_ref, gain_ref, branch_ref, out_ref):
    lean = gain_ref[...] * branch_ref[...]
    high = lean.astype(jnp.bfloat16).astype(jnp.float32)
    row = lax.broadcasted_iota(jnp.int32, (8, lean.shape[1]), 0)
    extra = jnp.where(row == 0, high, jnp.where(row == 1, lean - high, 0.0))
    extra = extra.astype(jnp.bfloat16)
    seq, units = hidden_ref.shape[0], down_ref.shape[0]
    past = seq + 3 * units
    for k in range(out_ref.shape[0]):
        out_ref[k, :seq, :] = hidden_ref[...]
        out_ref[k, seq : seq + units, :] = gate_ref[...]
        out_ref[k, seq + units : seq + 2 * units, :] = up_ref[...]
        out_ref[k, seq + 2 * units : past, :] = down_ref[...]
        out_ref[k, past:, :] = extra


def routes_kernel(ids_ref, turned_ref, logits_ref, out_ref):
    ids = ids_ref[...]
    turned = turned_ref[...]
    count, top = ids.shape
    logits = logits_ref[...]
    grown = jnp.exp(logits - jnp.max(logits, axis=1, keepdims=True))
    weight = grown / jnp.sum(grown, axis=1, keepdims=True)
    upper = weight.astype(jnp.bfloat16).astype(jnp.float32)
    lower = weight - upper
    row = lax.broadcasted_iota(jnp.int32, (count, count), 0)
    col = lax.broadcasted_iota(jnp.int32, (count, count), 1)
    lane = lax.broadcasted_iota(jnp.int32, (count, LANES), 1)
    packed = jnp.zeros((count, LANES), jnp.float32)
    for k in range(top):
        mine = ids[:, k : k + 1]
        same = jnp.zeros((count, count), jnp.float32)
        for other in range(top):
            same = same + jnp.where(mine == turned[other : other + 1, :], 1.0, 0.0)
        rank = jnp.sum(jnp.where(col < row, same, 0.0), axis=1, keepdims=True)
        code = mine.astype(jnp.float32) * CAP + rank
        packed = jnp.where(lane == k, code, packed)
        packed = jnp.where(lane == top + k, upper[:, k : k + 1], packed)
        packed = jnp.where(lane == 2 * top + k, lower[:, k : k + 1], packed)
    out_ref[...] = packed


def stage_kernel(*refs):
    count = len(refs) // 2
    sems = refs[-1]
    moves = [
        pltpu.make_async_copy(refs[k], refs[count + k], sems.at[k]) for k in range(count)
    ]
    for move in moves:
        move.start()
    for move in moves:
        move.wait()


def attend_kernel(
    lambda_ref,
    pieces_ref,
    gain_ref,
    query_ref,
    key_ref,
    value_ref,
    query_gain_ref,
    key_gain_ref,
    sub_ref,
    out_weight_ref,
    past_key_ref,
    past_value_ref,
    lengths_ref,
    out_ref,
    key_rows_ref,
    value_rows_ref,
):
    seq, past, size = past_key_ref.shape
    tp = pieces_ref.shape[0]
    half = size // 2
    full = jnp.concatenate([pieces_ref[k, :seq, :] for k in range(tp)], axis=1)
    full = full.astype(jnp.float32)
    square = jnp.sum(full * full, axis=1, keepdims=True) / full.shape[1]
    normed = (full * lax.rsqrt(square + EPSILON) * gain_ref[...]).astype(jnp.bfloat16)
    first = lax.broadcasted_iota(jnp.int32, (seq, size), 1) < half

    def halves(x):
        return (
            jnp.sum(jnp.where(first, x, 0.0), axis=1, keepdims=True),
            jnp.sum(jnp.where(first, 0.0, x), axis=1, keepdims=True),
        )

    def scaled(x, gain):
        low, high = halves(x * x)
        inverse = jnp.where(
            first, lax.rsqrt(low / half + EPSILON), lax.rsqrt(high / half + EPSILON)
        )
        return (x * inverse * gain).astype(jnp.bfloat16)

    query = scaled(mm(normed, query_ref[...]), query_gain_ref[...])
    key = scaled(mm(normed, key_ref[...]), key_gain_ref[...])
    value = mm(normed, value_ref[...]).astype(jnp.bfloat16)
    key_rows_ref[...] = key
    value_rows_ref[...] = value
    query = query.astype(jnp.float32)
    both = jnp.concatenate(
        [jnp.where(first, query, 0.0), jnp.where(first, 0.0, query)], axis=0
    )
    row = lax.broadcasted_iota(jnp.int32, (2 * seq, size), 0) % seq
    score = jnp.zeros((2 * seq, past), jnp.float32)
    for k in range(seq):
        mine = jnp.where(row == k, both, 0.0).astype(jnp.bfloat16)
        score = score + lax.dot_general(
            mine, past_key_ref[k], ACROSS, preferred_element_type=jnp.float32
        )
    scale = half**-0.5
    valid = lax.broadcasted_iota(jnp.int32, (seq, past), 1) < lengths_ref[...]
    own = [jnp.exp(o * scale) for o in halves(query * key.astype(jnp.float32))]
    grown = [
        jnp.where(valid, jnp.exp(score[m * seq : (m + 1) * seq] * scale), 0.0) for m in range(2)
    ]
    total = [jnp.sum(g, axis=1, keepdims=True) + o for g, o in zip(grown, own)]
    share = lambda_ref[0]
    weight = (grown[0] / total[0] - share * (grown[1] / total[1])).astype(jnp.bfloat16)
    weight_own = (own[0] / total[0] - share * (own[1] / total[1])).astype(jnp.bfloat16)
    weight = weight.astype(jnp.float32)
    row = lax.broadcasted_iota(jnp.int32, (seq, past), 0)
    mixed = weight_own.astype(jnp.float32) * value.astype(jnp.float32)
    for k in range(seq):
        mine = jnp.where(row == k, weight, 0.0).astype(jnp.bfloat16)
        mixed = mixed + mm(mine, past_value_ref[k])
    square = jnp.sum(mixed * mixed, axis=1, keepdims=True) / size
    head = mixed * lax.rsqrt(square + EPSILON) * sub_ref[...] * OUT_SCALE
    part = mm(head.astype(jnp.bfloat16), out_weight_ref[...]).astype(jnp.bfloat16)
    for k in range(tp):
        out_ref[k] = part


def mix_kernel(tp_ref, parts_ref, pieces_ref, gain_ref, routes_ref, res_ref, out_ref, *, top):
    tp, seq, _ = parts_ref.shape
    past = pieces_ref.shape[1] - 8
    residual = jnp.concatenate([pieces_ref[k, :seq, :] for k in range(tp)], axis=1)
    residual = residual.astype(jnp.float32)
    for k in range(tp):
        residual = residual + parts_ref[k].astype(jnp.float32)
    ends = [pieces_ref[k, past:, :].astype(jnp.float32) for k in range(tp)]
    lean = jnp.concatenate([end[0:1] + end[1:2] for end in ends], axis=1)
    total = residual.shape[1]
    width = total // tp
    inverse = lax.rsqrt(jnp.sum(residual * residual, axis=1, keepdims=True) / total + EPSILON)
    logit = jnp.sum(residual * lean, axis=1, keepdims=True) * inverse
    branch = jax.nn.sigmoid(logit)
    upper = branch.astype(jnp.bfloat16).astype(jnp.float32)
    own = jnp.zeros((residual.shape[0], width), jnp.float32)
    for k in range(tp):
        own = own + jnp.where(tp_ref[0] == k, residual[:, k * width : (k + 1) * width], 0.0)
    res_ref[...] = own
    mix = (own * inverse * gain_ref[...]).astype(jnp.bfloat16)
    routes = routes_ref[...]
    lane = lax.broadcasted_iota(jnp.int32, routes.shape, 1)
    routes = jnp.where(lane == 3 * top, upper, routes)
    routes = jnp.where(lane == 3 * top + 1, branch - upper, routes)
    rows = out_ref.shape[1] - width // LANES * seq
    stride = LANES * rows // seq
    notes = routes[:rows]
    for g in range(1, seq // rows):
        notes = notes + pltpu.roll(routes[g * rows : (g + 1) * rows], stride * g, axis=1)
    notes = notes.astype(jnp.bfloat16)
    for k in range(out_ref.shape[0]):
        for h in range(width // LANES):
            out_ref[k, h * seq : (h + 1) * seq, :] = mix[:, h * LANES : (h + 1) * LANES]
        out_ref[k, width // LANES * seq :, :] = notes


def notes_of(seen_ref, seq):
    line = seen_ref.shape[0]
    rows = seen_ref.shape[1] % seq
    packed = seen_ref[:, seen_ref.shape[1] - rows :, :].astype(jnp.float32)
    stride = LANES * rows // seq
    turned = [packed]
    for g in range(1, seq // rows):
        turned.append(pltpu.roll(packed, LANES - stride * g, axis=2))
    return jnp.concatenate(turned, axis=1).reshape(line * seq, LANES)


def slot_hits(notes, first, line, plane, top):
    total = notes.shape[0]
    slots = plane * line * CAP
    row = lax.broadcasted_iota(jnp.int32, (total, slots), 0)
    col = lax.broadcasted_iota(jnp.int32, (total, slots), 1)
    code = (first + col // (line * CAP)) * CAP + col % CAP
    here = row // (total // line) == (col // CAP) % line
    code = jnp.where(here, code, -1).astype(jnp.float32)
    return [notes[:, k : k + 1] == code for k in range(top)]


def outward_kernel(first_ref, seen_ref, out_hbm, placed_ref, dealt_ref, sems, *, top, seq):
    line = seen_ref.shape[0]
    plane, tp, items, width = out_hbm.shape
    slots = line * CAP
    rows = jnp.concatenate(
        [
            seen_ref[:, h * seq : (h + 1) * seq, :].reshape(line * seq, LANES)
            for h in range(width // LANES)
        ],
        axis=1,
    )
    dealt = rows.astype(jnp.float32).reshape(plane, tp, items - slots, width)
    dealt_ref[...] = dealt.astype(jnp.bfloat16)
    moves = [
        pltpu.make_async_copy(dealt_ref, out_hbm.at[:, :, pl.ds(slots, items - slots)], sems.at[tp])
    ]
    moves[0].start()
    hits = slot_hits(notes_of(seen_ref, seq), first_ref[0], line, plane, top)
    select = sum(jnp.where(h, 1.0, 0.0) for h in hits).astype(jnp.bfloat16)
    placed = lax.dot_general(select, rows, TURNED, preferred_element_type=jnp.float32)
    placed_ref[...] = placed.astype(jnp.bfloat16).reshape(plane, slots, width)
    for k in range(tp):
        moves.append(
            pltpu.make_async_copy(placed_ref, out_hbm.at[:, k, pl.ds(0, slots)], sems.at[k])
        )
        moves[-1].start()
    for move in moves:
        move.wait()


def weights_kernel(first_ref, seen_ref, upper_ref, lower_ref, branch_ref, *, top, plane, seq):
    line = seen_ref.shape[0]
    notes = notes_of(seen_ref, seq)
    hits = slot_hits(notes, first_ref[0], line, plane, top)
    upper_ref[...] = sum(
        jnp.where(h, notes[:, top + k : top + k + 1], 0.0) for k, h in enumerate(hits)
    ).astype(jnp.bfloat16)
    lower_ref[...] = sum(
        jnp.where(h, notes[:, 2 * top + k : 2 * top + k + 1], 0.0) for k, h in enumerate(hits)
    ).astype(jnp.bfloat16)
    branch = notes[:, 3 * top : 3 * top + 1] + notes[:, 3 * top + 1 : 3 * top + 2]
    branch_ref[...] = jnp.broadcast_to(branch, branch_ref.shape)


def expert_kernel(
    seen_ref, gate_ref, up_ref, down_hbm, own_hbm, other_hbm, out_hbm, down_ref, dense_ref, out_ref, sems, *, slots
):
    fetches = [
        pltpu.make_async_copy(own_hbm, dense_ref.at[0], sems.at[0]),
        pltpu.make_async_copy(other_hbm, dense_ref.at[1], sems.at[1]),
        pltpu.make_async_copy(down_hbm, down_ref, sems.at[2]),
    ]
    for fetch in fetches:
        fetch.start()
    plane, tp, items, width = seen_ref.shape
    gate_pre = up_pre = 0.0
    for k in range(tp):
        rows = seen_ref[:, k, :slots, :].reshape(plane * slots, width)
        gate_pre = gate_pre + mm(rows, gate_ref[0, k * width : (k + 1) * width, :])
        up_pre = up_pre + mm(rows, up_ref[0, k * width : (k + 1) * width, :])
    act = clamped_unit(gate_pre, up_pre).astype(jnp.bfloat16)
    _, columns, _, rows_each, _ = dense_ref.shape
    units = rows_each // 3
    every = 2 * columns * units
    dealt = items - slots
    fetches[0].wait()
    fetches[1].wait()
    gate_pre = up_pre = 0.0
    for k in range(tp):
        rows = seen_ref[:, k, slots:, :].astype(jnp.float32).reshape(plane * dealt, width)
        rows = rows.astype(jnp.bfloat16)
        gate = dense_ref[:, :, k, :units, :].reshape(every, width)
        up = dense_ref[:, :, k, units : 2 * units, :].reshape(every, width)
        gate_pre = gate_pre + lax.dot_general(
            rows, gate, ACROSS, preferred_element_type=jnp.float32
        )
        up_pre = up_pre + lax.dot_general(rows, up, ACROSS, preferred_element_type=jnp.float32)
    dense_act = (gate_pre / (1.0 + jnp.exp(-gate_pre)) * up_pre).astype(jnp.bfloat16)
    fetches[2].wait()
    moves = []
    for k in range(tp):
        part = mm(act, down_ref[0, :, k * width : (k + 1) * width]).astype(jnp.bfloat16)
        out_ref[k, :, :slots, :] = part.reshape(plane, slots, width)
        down = dense_ref[:, :, k, 2 * units :, :].reshape(every, width)
        part = mm(dense_act, down).reshape(plane, dealt, width)
        out_ref[k, :, slots:, :] = part.astype(jnp.bfloat16)
        moves.append(pltpu.make_async_copy(out_ref.at[k], out_hbm.at[:, k], sems.at[3 + k]))
        moves[-1].start()
    for move in moves:
        move.wait()


def inward_kernel(seen_ref, upper_ref, lower_ref, branch_ref, out_ref):
    line, seq, width = out_ref.shape
    plane, tp, _, _ = seen_ref.shape
    slots = line * CAP
    whole = jnp.zeros((plane, slots, width), jnp.float32)
    for k in range(tp):
        whole = whole + seen_ref[:, k, :slots, :].astype(jnp.float32)
    whole = whole.astype(jnp.bfloat16).reshape(plane * slots, width)
    routed = mm(upper_ref[...], whole) + mm(lower_ref[...], whole)
    dense = seen_ref[:, :, slots:, :].astype(jnp.float32).reshape(line * seq, width)
    back = (routed + branch_ref[...] * dense).astype(jnp.bfloat16)
    out_ref[...] = back.reshape(line, seq, width)


def doubled(held, step):
    columns = lax.axis_size("ep_1")
    other = lax.ppermute(held, "ep_1", [(i, i ^ step) for i in range(columns)])
    return jnp.concatenate([held, other], axis=0)


def shaped(shape, dtype):
    return jax.ShapeDtypeStruct(shape, dtype)


def body(
    hidden_in,
    norm_gain_attn,
    query_weight,
    key_weight,
    value_weight,
    query_gain,
    key_gain,
    lambda_head,
    sub_gain,
    out_weight,
    cache_key,
    cache_value,
    lengths,
    norm_gain_mix,
    route_ids,
    route_logits,
    expert_gate,
    expert_up,
    expert_down,
    dense_gate,
    dense_up,
    dense_down,
    branch_gate,
):
    seq, top = route_ids.shape
    width = hidden_in.shape[1]
    units = dense_down.shape[0]
    line = lax.axis_size("ep_0")
    plane = lax.axis_size("ep_1") * lax.axis_size("ep_2")
    tp = lax.axis_size("tp")
    slots = line * CAP
    dealt = line * seq // (plane * tp)
    past = seq + 3 * units
    mine = pl.pallas_call(
        opening_kernel, out_shape=shaped((tp, past + 8, width), jnp.bfloat16), name="opening", compiler_params=LIMIT
    )(
        *map(
            far,
            (
                hidden_in,
                dense_gate.T,
                dense_up.T,
                dense_down,
                norm_gain_mix[None, :],
                branch_gate[None, :],
            ),
        )
    )
    pieces = lax.all_to_all(mine, "tp", 0, 0, tiled=True)
    needed = (
        norm_gain_attn[None, :],
        query_weight,
        key_weight,
        value_weight,
        query_gain[None, :],
        key_gain[None, :],
        sub_gain[None, :],
        out_weight,
        cache_key,
        cache_value,
        norm_gain_mix[None, :],
    )
    *staged, gain_here = pl.pallas_call(
        stage_kernel,
        out_shape=tuple(map(kept, needed)),
        in_specs=[pl.BlockSpec(memory_space=pl.ANY)] * len(needed),
        out_specs=(WHOLE,) * len(needed),
        scratch_shapes=[pltpu.SemaphoreType.DMA((len(needed),))],
        name="stage",
        compiler_params=LIMIT,
    )(*map(far, needed))
    routes = pl.pallas_call(
        routes_kernel, out_shape=shaped((seq, LANES), jnp.float32), name="routes", compiler_params=LIMIT
    )(route_ids, route_ids.T, route_logits)
    size = value_weight.shape[1]
    parts, key_rows, value_rows = pl.pallas_call(
        attend_kernel,
        out_shape=(
            shaped((tp, seq, out_weight.shape[1]), jnp.bfloat16),
            shaped((seq, size), jnp.bfloat16),
            shaped((seq, size), jnp.bfloat16),
        ),
        in_specs=[SCALARS] + [WHOLE] * 12,
        name="attend",
        compiler_params=LIMIT,
    )(
        lambda_head,
        near(pieces),
        *map(near, staged),
        near(lengths[:, None]),
    )
    parts = lax.all_to_all(parts, "tp", 0, 0, tiled=True)
    columns = lax.axis_size("ep_1")
    steps = [1 << k for k in reversed(range(columns.bit_length() - 1))]
    own_dense = pieces[None, :, seq:past]
    for step in steps[:1]:
        own_dense = doubled(own_dense, step)
    residual, message = pl.pallas_call(
        lambda *refs: mix_kernel(*refs, top=top),
        out_shape=(
            shaped((seq, width), jnp.float32),
            shaped((line, width // LANES * seq + 8, LANES), jnp.bfloat16),
        ),
        in_specs=[SCALARS] + [WHOLE] * 4,
        name="mix",
        compiler_params=LIMIT,
    )(
        lax.axis_index("tp").reshape(1),
        near(parts),
        near(pieces),
        near(gain_here),
        near(routes),
    )
    seen = lax.all_to_all(message, "ep_0", 0, 0, tiled=True)
    for step in steps[1:]:
        own_dense = doubled(own_dense, step)
    own_dense, seen = lax.optimization_barrier((own_dense, seen))
    seen = near(seen)
    other_dense = lax.ppermute(own_dense, "ep_2", [(0, 1), (1, 0)])
    first = (lax.axis_index("ep_0") * plane).reshape(1)
    outward = pl.pallas_call(
        lambda *refs: outward_kernel(*refs, top=top, seq=seq),
        out_shape=sent_to_hbm((plane, tp, slots + dealt, width), jnp.bfloat16),
        in_specs=[SCALARS, WHOLE],
        out_specs=pl.BlockSpec(memory_space=pl.ANY),
        scratch_shapes=[
            pltpu.VMEM((plane, slots, width), jnp.bfloat16),
            pltpu.VMEM((plane, tp, dealt, width), jnp.bfloat16),
            pltpu.SemaphoreType.DMA((tp + 1,)),
        ],
        name="outward",
        compiler_params=LIMIT,
    )(first, seen)
    arrived = lax.all_to_all(
        outward.reshape(plane * tp, slots + dealt, width), BLOCK, 0, 0, tiled=True
    ).reshape(plane, tp, slots + dealt, width)
    upper, lower, branch = pl.pallas_call(
        lambda *refs: weights_kernel(*refs, top=top, plane=plane, seq=seq),
        out_shape=(
            shaped((line * seq, plane * slots), jnp.bfloat16),
            shaped((line * seq, plane * slots), jnp.bfloat16),
            shaped((line * seq, width), jnp.float32),
        ),
        in_specs=[SCALARS, WHOLE],
        name="weights",
        compiler_params=LIMIT,
    )(first, seen)
    sent = pl.pallas_call(
        lambda *refs: expert_kernel(*refs, slots=slots),
        out_shape=sent_to_hbm((plane, tp, slots + dealt, width), jnp.bfloat16),
        in_specs=[WHOLE] * 3 + [pl.BlockSpec(memory_space=pl.ANY)] * 3,
        out_specs=pl.BlockSpec(memory_space=pl.ANY),
        scratch_shapes=[
            pltpu.VMEM(expert_down.shape, expert_down.dtype),
            pltpu.VMEM((2, *own_dense.shape), own_dense.dtype),
            pltpu.VMEM((tp, plane, slots + dealt, width), jnp.bfloat16),
            pltpu.SemaphoreType.DMA((3 + tp,)),
        ],
        name="experts",
        compiler_params=LIMIT,
    )(
        near(arrived),
        near(expert_gate),
        near(expert_up),
        far(expert_down),
        far(own_dense),
        far(other_dense),
    )
    returned = lax.all_to_all(
        sent.reshape(plane * tp, slots + dealt, width), BLOCK, 0, 0, tiled=True
    ).reshape(plane, tp, slots + dealt, width)
    back = pl.pallas_call(
        inward_kernel,
        out_shape=shaped((line, seq, width), jnp.bfloat16),
        name="inward",
        compiler_params=LIMIT,
    )(near(returned), near(upper), near(lower), near(branch))
    home = lax.all_to_all(back, "ep_0", 0, 0, tiled=True)
    layer_out = (residual + jnp.sum(home.astype(jnp.float32), axis=0)).astype(jnp.bfloat16)
    return (layer_out, key_rows, value_rows)


def solution(mesh):
    split = Mesh(mesh.devices.reshape(16, 4, 2, mesh.shape["tp"]), ("ep_0", "ep_1", "ep_2", "tp"))
    in_specs = (
        P(EP, "tp"),
        P(),
        P(None, "tp"),
        P(None, "tp"),
        P(None, "tp"),
        P(),
        P(),
        P("tp"),
        P(),
        P("tp", None),
        P(EP, None, "tp"),
        P(EP, None, "tp"),
        P(EP),
        P("tp"),
        P(EP, None),
        P(EP, None),
        P(EP, None, "tp"),
        P(EP, None, "tp"),
        P(EP, "tp", None),
        P("tp", EP),
        P("tp", EP),
        P(EP, "tp"),
        P("tp"),
    )
    out_specs = (P(EP, "tp"), P(EP, "tp"), P(EP, "tp"))
    return jax.shard_map(body, mesh=split, in_specs=in_specs, out_specs=out_specs, check_vma=False)
```

```python
import math

import jax
import jax.numpy as jnp
from jax import lax
from jax.experimental import pallas as pl
from jax.experimental.pallas import tpu as pltpu

from jax.sharding import Mesh
from jax.sharding import PartitionSpec as P


EP = ("ep_0", "ep_1", "ep_2")
BLOCK = ("ep_1", "ep_2", "tp")
CAP = 2


EPSILON = 1e-06
CLAMP_LIMIT = 7.0
SWISH_ALPHA = 1.702
OUT_SCALE = 0.2 + 0.6 * math.exp(-0.6)


def clamped_unit(gate_pre, up_pre):
    gate_cut = jnp.minimum(gate_pre, CLAMP_LIMIT)
    up_cut = jnp.clip(up_pre, -CLAMP_LIMIT, CLAMP_LIMIT)
    return (up_cut + 1.0) * gate_cut * jax.nn.sigmoid(SWISH_ALPHA * gate_cut)


LANES = 128
TURNED = (((0,), (0,)), ((), ()))
ACROSS = (((1,), (1,)), ((), ()))
SCALARS = pl.BlockSpec(memory_space=pltpu.SMEM)
LIMIT = pltpu.CompilerParams(vmem_limit_bytes=12 * 2**20)
WHOLE = pl.BlockSpec(memory_space=pltpu.VMEM)


def mm(a, b):
    return jnp.dot(a, b, preferred_element_type=jnp.float32)


def sent_to_hbm(shape, dtype):
    return pltpu.HBM(shape, dtype)


def kept(x):
    return pltpu.VMEM(x.shape, x.dtype)


def far(x):
    return pltpu.with_memory_space_constraint(x, pltpu.HBM)


def near(x):
    return pltpu.with_memory_space_constraint(x, pltpu.VMEM)


def opening_kernel(hidden_ref, gate_ref, up_ref, down_ref, gain_ref, branch_ref, out_ref):
    lean = gain_ref[...] * branch_ref[...]
    high = lean.astype(jnp.bfloat16).astype(jnp.float32)
    row = lax.broadcasted_iota(jnp.int32, (8, lean.shape[1]), 0)
    extra = jnp.where(row == 0, high, jnp.where(row == 1, lean - high, 0.0))
    extra = extra.astype(jnp.bfloat16)
    seq, units = hidden_ref.shape[0], down_ref.shape[0]
    past = seq + 3 * units
    for k in range(out_ref.shape[0]):
        out_ref[k, :seq, :] = hidden_ref[...]
        out_ref[k, seq : seq + units, :] = gate_ref[...]
        out_ref[k, seq + units : seq + 2 * units, :] = up_ref[...]
        out_ref[k, seq + 2 * units : past, :] = down_ref[...]
        out_ref[k, past:, :] = extra


def routes_kernel(ids_ref, turned_ref, logits_ref, out_ref):
    ids = ids_ref[...]
    turned = turned_ref[...]
    count, top = ids.shape
    logits = logits_ref[...]
    grown = jnp.exp(logits - jnp.max(logits, axis=1, keepdims=True))
    weight = grown / jnp.sum(grown, axis=1, keepdims=True)
    upper = weight.astype(jnp.bfloat16).astype(jnp.float32)
    lower = weight - upper
    row = lax.broadcasted_iota(jnp.int32, (count, count), 0)
    col = lax.broadcasted_iota(jnp.int32, (count, count), 1)
    lane = lax.broadcasted_iota(jnp.int32, (count, LANES), 1)
    packed = jnp.zeros((count, LANES), jnp.float32)
    for k in range(top):
        mine = ids[:, k : k + 1]
        same = jnp.zeros((count, count), jnp.float32)
        for other in range(top):
            same = same + jnp.where(mine == turned[other : other + 1, :], 1.0, 0.0)
        rank = jnp.sum(jnp.where(col < row, same, 0.0), axis=1, keepdims=True)
        code = mine.astype(jnp.float32) * CAP + rank
        packed = jnp.where(lane == k, code, packed)
        packed = jnp.where(lane == top + k, upper[:, k : k + 1], packed)
        packed = jnp.where(lane == 2 * top + k, lower[:, k : k + 1], packed)
    out_ref[...] = packed


def stage_kernel(*refs):
    count = len(refs) // 2
    sems = refs[-1]
    moves = [
        pltpu.make_async_copy(refs[k], refs[count + k], sems.at[k]) for k in range(count)
    ]
    for move in moves:
        move.start()
    for move in moves:
        move.wait()


def brought(arrays):
    return pl.pallas_call(
        stage_kernel,
        out_shape=tuple(map(kept, arrays)),
        in_specs=[pl.BlockSpec(memory_space=pl.ANY)] * len(arrays),
        out_specs=(WHOLE,) * len(arrays),
        scratch_shapes=[pltpu.SemaphoreType.DMA((len(arrays),))],
        name="stage",
        compiler_params=LIMIT,
    )(*map(far, arrays))


def attend_kernel(
    lambda_ref,
    pieces_ref,
    gain_ref,
    query_ref,
    key_ref,
    value_ref,
    query_gain_ref,
    key_gain_ref,
    sub_ref,
    out_weight_ref,
    past_key_ref,
    past_value_ref,
    lengths_ref,
    out_ref,
    key_rows_ref,
    value_rows_ref,
):
    seq, past, size = past_key_ref.shape
    tp = pieces_ref.shape[0]
    half = size // 2
    full = jnp.concatenate([pieces_ref[k, :seq, :] for k in range(tp)], axis=1)
    full = full.astype(jnp.float32)
    square = jnp.sum(full * full, axis=1, keepdims=True) / full.shape[1]
    normed = (full * lax.rsqrt(square + EPSILON) * gain_ref[...]).astype(jnp.bfloat16)
    first = lax.broadcasted_iota(jnp.int32, (seq, size), 1) < half

    def halves(x):
        return (
            jnp.sum(jnp.where(first, x, 0.0), axis=1, keepdims=True),
            jnp.sum(jnp.where(first, 0.0, x), axis=1, keepdims=True),
        )

    def scaled(x, gain):
        low, high = halves(x * x)
        inverse = jnp.where(
            first, lax.rsqrt(low / half + EPSILON), lax.rsqrt(high / half + EPSILON)
        )
        return (x * inverse * gain).astype(jnp.bfloat16)

    query = scaled(mm(normed, query_ref[...]), query_gain_ref[...])
    key = scaled(mm(normed, key_ref[...]), key_gain_ref[...])
    value = mm(normed, value_ref[...]).astype(jnp.bfloat16)
    key_rows_ref[...] = key
    value_rows_ref[...] = value
    query = query.astype(jnp.float32)
    both = jnp.concatenate(
        [jnp.where(first, query, 0.0), jnp.where(first, 0.0, query)], axis=0
    )
    row = lax.broadcasted_iota(jnp.int32, (2 * seq, size), 0) % seq
    score = jnp.zeros((2 * seq, past), jnp.float32)
    for k in range(seq):
        mine = jnp.where(row == k, both, 0.0).astype(jnp.bfloat16)
        score = score + lax.dot_general(
            mine, past_key_ref[k], ACROSS, preferred_element_type=jnp.float32
        )
    scale = half**-0.5
    valid = lax.broadcasted_iota(jnp.int32, (seq, past), 1) < lengths_ref[...]
    own = [jnp.exp(o * scale) for o in halves(query * key.astype(jnp.float32))]
    grown = [
        jnp.where(valid, jnp.exp(score[m * seq : (m + 1) * seq] * scale), 0.0) for m in range(2)
    ]
    total = [jnp.sum(g, axis=1, keepdims=True) + o for g, o in zip(grown, own)]
    share = lambda_ref[0]
    weight = (grown[0] / total[0] - share * (grown[1] / total[1])).astype(jnp.bfloat16)
    weight_own = (own[0] / total[0] - share * (own[1] / total[1])).astype(jnp.bfloat16)
    weight = weight.astype(jnp.float32)
    row = lax.broadcasted_iota(jnp.int32, (seq, past), 0)
    mixed = weight_own.astype(jnp.float32) * value.astype(jnp.float32)
    for k in range(seq):
        mine = jnp.where(row == k, weight, 0.0).astype(jnp.bfloat16)
        mixed = mixed + mm(mine, past_value_ref[k])
    square = jnp.sum(mixed * mixed, axis=1, keepdims=True) / size
    head = mixed * lax.rsqrt(square + EPSILON) * sub_ref[...] * OUT_SCALE
    part = mm(head.astype(jnp.bfloat16), out_weight_ref[...]).astype(jnp.bfloat16)
    for k in range(tp):
        out_ref[k] = part


def mix_kernel(tp_ref, parts_ref, pieces_ref, gain_ref, routes_ref, res_ref, out_ref, *, top):
    tp, seq, _ = parts_ref.shape
    past = pieces_ref.shape[1] - 8
    residual = jnp.concatenate([pieces_ref[k, :seq, :] for k in range(tp)], axis=1)
    residual = residual.astype(jnp.float32)
    for k in range(tp):
        residual = residual + parts_ref[k].astype(jnp.float32)
    ends = [pieces_ref[k, past:, :].astype(jnp.float32) for k in range(tp)]
    lean = jnp.concatenate([end[0:1] + end[1:2] for end in ends], axis=1)
    total = residual.shape[1]
    width = total // tp
    inverse = lax.rsqrt(jnp.sum(residual * residual, axis=1, keepdims=True) / total + EPSILON)
    logit = jnp.sum(residual * lean, axis=1, keepdims=True) * inverse
    branch = jax.nn.sigmoid(logit)
    upper = branch.astype(jnp.bfloat16).astype(jnp.float32)
    own = jnp.zeros((residual.shape[0], width), jnp.float32)
    for k in range(tp):
        own = own + jnp.where(tp_ref[0] == k, residual[:, k * width : (k + 1) * width], 0.0)
    res_ref[...] = own
    mix = (own * inverse * gain_ref[...]).astype(jnp.bfloat16)
    routes = routes_ref[...]
    lane = lax.broadcasted_iota(jnp.int32, routes.shape, 1)
    routes = jnp.where(lane == 3 * top, upper, routes)
    routes = jnp.where(lane == 3 * top + 1, branch - upper, routes)
    rows = out_ref.shape[1] - width // LANES * seq
    stride = LANES * rows // seq
    notes = routes[:rows]
    for g in range(1, seq // rows):
        notes = notes + pltpu.roll(routes[g * rows : (g + 1) * rows], stride * g, axis=1)
    notes = notes.astype(jnp.bfloat16)
    for k in range(out_ref.shape[0]):
        for h in range(width // LANES):
            out_ref[k, h * seq : (h + 1) * seq, :] = mix[:, h * LANES : (h + 1) * LANES]
        out_ref[k, width // LANES * seq :, :] = notes


def notes_of(seen_ref, seq):
    line = seen_ref.shape[0]
    rows = seen_ref.shape[1] % seq
    packed = seen_ref[:, seen_ref.shape[1] - rows :, :].astype(jnp.float32)
    stride = LANES * rows // seq
    turned = [packed]
    for g in range(1, seq // rows):
        turned.append(pltpu.roll(packed, LANES - stride * g, axis=2))
    return jnp.concatenate(turned, axis=1).reshape(line * seq, LANES)


def slot_hits(notes, first, line, plane, top):
    total = notes.shape[0]
    slots = plane * line * CAP
    row = lax.broadcasted_iota(jnp.int32, (total, slots), 0)
    col = lax.broadcasted_iota(jnp.int32, (total, slots), 1)
    code = (first + col // (line * CAP)) * CAP + col % CAP
    here = row // (total // line) == (col // CAP) % line
    code = jnp.where(here, code, -1).astype(jnp.float32)
    return [notes[:, k : k + 1] == code for k in range(top)]


def outward_kernel(first_ref, seen_ref, out_hbm, placed_ref, dealt_ref, sems, *, top, seq):
    line = seen_ref.shape[0]
    plane, tp, items, width = out_hbm.shape
    slots = line * CAP
    rows = jnp.concatenate(
        [
            seen_ref[:, h * seq : (h + 1) * seq, :].reshape(line * seq, LANES)
            for h in range(width // LANES)
        ],
        axis=1,
    )
    dealt = rows.astype(jnp.float32).reshape(plane, tp, items - slots, width)
    dealt_ref[...] = dealt.astype(jnp.bfloat16)
    moves = [
        pltpu.make_async_copy(dealt_ref, out_hbm.at[:, :, pl.ds(slots, items - slots)], sems.at[tp])
    ]
    moves[0].start()
    hits = slot_hits(notes_of(seen_ref, seq), first_ref[0], line, plane, top)
    select = sum(jnp.where(h, 1.0, 0.0) for h in hits).astype(jnp.bfloat16)
    placed = lax.dot_general(select, rows, TURNED, preferred_element_type=jnp.float32)
    placed_ref[...] = placed.astype(jnp.bfloat16).reshape(plane, slots, width)
    for k in range(tp):
        moves.append(
            pltpu.make_async_copy(placed_ref, out_hbm.at[:, k, pl.ds(0, slots)], sems.at[k])
        )
        moves[-1].start()
    for move in moves:
        move.wait()


def weights_kernel(first_ref, seen_ref, upper_ref, lower_ref, branch_ref, *, top, plane, seq):
    line = seen_ref.shape[0]
    notes = notes_of(seen_ref, seq)
    hits = slot_hits(notes, first_ref[0], line, plane, top)
    upper_ref[...] = sum(
        jnp.where(h, notes[:, top + k : top + k + 1], 0.0) for k, h in enumerate(hits)
    ).astype(jnp.bfloat16)
    lower_ref[...] = sum(
        jnp.where(h, notes[:, 2 * top + k : 2 * top + k + 1], 0.0) for k, h in enumerate(hits)
    ).astype(jnp.bfloat16)
    branch = notes[:, 3 * top : 3 * top + 1] + notes[:, 3 * top + 1 : 3 * top + 2]
    branch_ref[...] = jnp.broadcast_to(branch, branch_ref.shape)


def expert_kernel(
    seen_ref, gate_ref, up_ref, down_ref, own_ref, other_ref, out_hbm, out_ref, sems, *, slots
):
    plane, tp, items, width = seen_ref.shape
    rows = jnp.concatenate(
        [seen_ref[:, k, :slots, :].reshape(plane * slots, width) for k in range(tp)], axis=1
    )
    gate_pre = mm(rows, gate_ref[0])
    up_pre = mm(rows, up_ref[0])
    act = clamped_unit(gate_pre, up_pre).astype(jnp.bfloat16)
    columns, _, rows_each, _ = own_ref.shape
    units = rows_each // 3
    dealt = items - slots

    def units_at(k, lo):
        return jnp.concatenate(
            [
                ref[:, k, lo : lo + units, :].reshape(columns * units, width)
                for ref in (own_ref, other_ref)
            ],
            axis=0,
        )

    rows = jnp.concatenate(
        [
            seen_ref[:, k, slots:, :].astype(jnp.float32).reshape(plane * dealt, width)
            for k in range(tp)
        ],
        axis=1,
    ).astype(jnp.bfloat16)

    def units_of(lo):
        return jnp.concatenate(
            [units_at(k, lo) for k in range(tp)],
            axis=1,
        )

    gate_pre = lax.dot_general(rows, units_of(0), ACROSS, preferred_element_type=jnp.float32)
    up_pre = lax.dot_general(rows, units_of(units), ACROSS, preferred_element_type=jnp.float32)
    dense_act = (gate_pre / (1.0 + jnp.exp(-gate_pre)) * up_pre).astype(jnp.bfloat16)
    moves = []
    for k in range(tp):
        part = mm(act, down_ref[0, :, k * width : (k + 1) * width]).astype(jnp.bfloat16)
        out_ref[k, :, :slots, :] = part.reshape(plane, slots, width)
        part = mm(dense_act, units_at(k, 2 * units)).reshape(plane, dealt, width)
        out_ref[k, :, slots:, :] = part.astype(jnp.bfloat16)
        moves.append(pltpu.make_async_copy(out_ref.at[k], out_hbm.at[:, k], sems.at[k]))
        moves[-1].start()
    for move in moves:
        move.wait()


def inward_kernel(seen_ref, upper_ref, lower_ref, branch_ref, out_ref):
    line, seq, width = out_ref.shape
    plane, tp, _, _ = seen_ref.shape
    slots = line * CAP
    whole = jnp.zeros((plane, slots, width), jnp.float32)
    for k in range(tp):
        whole = whole + seen_ref[:, k, :slots, :].astype(jnp.float32)
    whole = whole.astype(jnp.bfloat16).reshape(plane * slots, width)
    routed = mm(upper_ref[...], whole) + mm(lower_ref[...], whole)
    dense = seen_ref[:, :, slots:, :].astype(jnp.float32).reshape(line * seq, width)
    back = (routed + branch_ref[...] * dense).astype(jnp.bfloat16)
    out_ref[...] = back.reshape(line, seq, width)


def doubled(held, step):
    columns = lax.axis_size("ep_1")
    other = lax.ppermute(held, "ep_1", [(i, i ^ step) for i in range(columns)])
    return jnp.concatenate([held, other], axis=0)


def shaped(shape, dtype):
    return jax.ShapeDtypeStruct(shape, dtype)


def body(
    hidden_in,
    norm_gain_attn,
    query_weight,
    key_weight,
    value_weight,
    query_gain,
    key_gain,
    lambda_head,
    sub_gain,
    out_weight,
    cache_key,
    cache_value,
    lengths,
    norm_gain_mix,
    route_ids,
    route_logits,
    expert_gate,
    expert_up,
    expert_down,
    dense_gate,
    dense_up,
    dense_down,
    branch_gate,
):
    seq, top = route_ids.shape
    width = hidden_in.shape[1]
    units = dense_down.shape[0]
    line = lax.axis_size("ep_0")
    plane = lax.axis_size("ep_1") * lax.axis_size("ep_2")
    tp = lax.axis_size("tp")
    slots = line * CAP
    dealt = line * seq // (plane * tp)
    past = seq + 3 * units
    mine = pl.pallas_call(
        opening_kernel, out_shape=shaped((tp, past + 8, width), jnp.bfloat16), name="opening", compiler_params=LIMIT
    )(
        *map(
            far,
            (
                hidden_in,
                dense_gate.T,
                dense_up.T,
                dense_down,
                norm_gain_mix[None, :],
                branch_gate[None, :],
            ),
        )
    )
    pieces = lax.all_to_all(mine, "tp", 0, 0, tiled=True)
    needed = (
        norm_gain_attn[None, :],
        query_weight,
        key_weight,
        value_weight,
        query_gain[None, :],
        key_gain[None, :],
        sub_gain[None, :],
        out_weight,
        cache_key,
        cache_value,
        norm_gain_mix[None, :],
    )
    *staged, gain_here = brought(needed)
    routes = pl.pallas_call(
        routes_kernel, out_shape=shaped((seq, LANES), jnp.float32), name="routes", compiler_params=LIMIT
    )(route_ids, route_ids.T, route_logits)
    size = value_weight.shape[1]
    parts, key_rows, value_rows = pl.pallas_call(
        attend_kernel,
        out_shape=(
            shaped((tp, seq, out_weight.shape[1]), jnp.bfloat16),
            shaped((seq, size), jnp.bfloat16),
            shaped((seq, size), jnp.bfloat16),
        ),
        in_specs=[SCALARS] + [WHOLE] * 12,
        name="attend",
        compiler_params=LIMIT,
    )(
        lambda_head,
        near(pieces),
        *map(near, staged),
        near(lengths[:, None]),
    )
    parts = lax.all_to_all(parts, "tp", 0, 0, tiled=True)
    columns = lax.axis_size("ep_1")
    steps = [1 << k for k in reversed(range(columns.bit_length() - 1))]
    own_dense = pieces[None, :, seq:past]
    for step in steps[:1]:
        own_dense = doubled(own_dense, step)
    residual, message = pl.pallas_call(
        lambda *refs: mix_kernel(*refs, top=top),
        out_shape=(
            shaped((seq, width), jnp.float32),
            shaped((line, width // LANES * seq + 8, LANES), jnp.bfloat16),
        ),
        in_specs=[SCALARS] + [WHOLE] * 4,
        name="mix",
        compiler_params=LIMIT,
    )(
        lax.axis_index("tp").reshape(1),
        near(parts),
        near(pieces),
        near(gain_here),
        near(routes),
    )
    seen = lax.all_to_all(message, "ep_0", 0, 0, tiled=True)
    for step in steps[1:]:
        own_dense = doubled(own_dense, step)
    own_dense, seen = lax.optimization_barrier((own_dense, seen))
    seen = near(seen)
    other_dense = lax.ppermute(own_dense, "ep_2", [(0, 1), (1, 0)])
    first = (lax.axis_index("ep_0") * plane).reshape(1)
    outward = pl.pallas_call(
        lambda *refs: outward_kernel(*refs, top=top, seq=seq),
        out_shape=sent_to_hbm((plane, tp, slots + dealt, width), jnp.bfloat16),
        in_specs=[SCALARS, WHOLE],
        out_specs=pl.BlockSpec(memory_space=pl.ANY),
        scratch_shapes=[
            pltpu.VMEM((plane, slots, width), jnp.bfloat16),
            pltpu.VMEM((plane, tp, dealt, width), jnp.bfloat16),
            pltpu.SemaphoreType.DMA((tp + 1,)),
        ],
        name="outward",
        compiler_params=LIMIT,
    )(first, seen)
    arrived = lax.all_to_all(
        outward.reshape(plane * tp, slots + dealt, width), BLOCK, 0, 0, tiled=True
    ).reshape(plane, tp, slots + dealt, width)
    upper, lower, branch = pl.pallas_call(
        lambda *refs: weights_kernel(*refs, top=top, plane=plane, seq=seq),
        out_shape=(
            shaped((line * seq, plane * slots), jnp.bfloat16),
            shaped((line * seq, plane * slots), jnp.bfloat16),
            shaped((line * seq, width), jnp.float32),
        ),
        in_specs=[SCALARS, WHOLE],
        name="weights",
        compiler_params=LIMIT,
    )(first, seen)
    tools = brought((expert_gate, expert_up, expert_down, own_dense, other_dense))
    sent = pl.pallas_call(
        lambda *refs: expert_kernel(*refs, slots=slots),
        out_shape=sent_to_hbm((plane, tp, slots + dealt, width), jnp.bfloat16),
        in_specs=[WHOLE] * 6,
        out_specs=pl.BlockSpec(memory_space=pl.ANY),
        scratch_shapes=[
            pltpu.VMEM((tp, plane, slots + dealt, width), jnp.bfloat16),
            pltpu.SemaphoreType.DMA((tp,)),
        ],
        name="experts",
        compiler_params=LIMIT,
    )(
        near(arrived),
        *map(near, tools),
    )
    returned = lax.all_to_all(
        sent.reshape(plane * tp, slots + dealt, width), BLOCK, 0, 0, tiled=True
    ).reshape(plane, tp, slots + dealt, width)
    back = pl.pallas_call(
        inward_kernel,
        out_shape=shaped((line, seq, width), jnp.bfloat16),
        name="inward",
        compiler_params=LIMIT,
    )(near(returned), near(upper), near(lower), near(branch))
    home = lax.all_to_all(back, "ep_0", 0, 0, tiled=True)
    layer_out = (residual + jnp.sum(home.astype(jnp.float32), axis=0)).astype(jnp.bfloat16)
    return (layer_out, key_rows, value_rows)


def solution(mesh):
    split = Mesh(mesh.devices.reshape(16, 4, 2, mesh.shape["tp"]), ("ep_0", "ep_1", "ep_2", "tp"))
    in_specs = (
        P(EP, "tp"),
        P(),
        P(None, "tp"),
        P(None, "tp"),
        P(None, "tp"),
        P(),
        P(),
        P("tp"),
        P(),
        P("tp", None),
        P(EP, None, "tp"),
        P(EP, None, "tp"),
        P(EP),
        P("tp"),
        P(EP, None),
        P(EP, None),
        P(EP, None, "tp"),
        P(EP, None, "tp"),
        P(EP, "tp", None),
        P("tp", EP),
        P("tp", EP),
        P(EP, "tp"),
        P("tp"),
    )
    out_specs = (P(EP, "tp"), P(EP, "tp"), P(EP, "tp"))
    return jax.shard_map(body, mesh=split, in_specs=in_specs, out_specs=out_specs, check_vma=False)
```

```python
import math

import jax
import jax.numpy as jnp
from jax import lax
from jax.experimental import pallas as pl
from jax.experimental.pallas import tpu as pltpu

from jax.sharding import Mesh
from jax.sharding import PartitionSpec as P


EP = ("ep_0", "ep_1", "ep_2")
PLANE = ("ep_1", "ep_2")
BLOCK = ("ep_1", "ep_2", "tp")
CAP = 2


EPSILON = 1e-06
CLAMP_LIMIT = 7.0
SWISH_ALPHA = 1.702
OUT_SCALE = 0.2 + 0.6 * math.exp(-0.6)


def clamped_unit(gate_pre, up_pre):
    gate_cut = jnp.minimum(gate_pre, CLAMP_LIMIT)
    up_cut = jnp.clip(up_pre, -CLAMP_LIMIT, CLAMP_LIMIT)
    return (up_cut + 1.0) * gate_cut * jax.nn.sigmoid(SWISH_ALPHA * gate_cut)


LANES = 128
TURNED = (((0,), (0,)), ((), ()))
ACROSS = (((1,), (1,)), ((), ()))
SCALARS = pl.BlockSpec(memory_space=pltpu.SMEM)
LIMIT = pltpu.CompilerParams(vmem_limit_bytes=12 * 2**20)
WHOLE = pl.BlockSpec(memory_space=pltpu.VMEM)


def mm(a, b):
    return jnp.dot(a, b, preferred_element_type=jnp.float32)


def sent_to_hbm(shape, dtype):
    return pltpu.HBM(shape, dtype)


def kept(x):
    return pltpu.VMEM(x.shape, x.dtype)


def far(x):
    return pltpu.with_memory_space_constraint(x, pltpu.HBM)


def near(x):
    return pltpu.with_memory_space_constraint(x, pltpu.VMEM)


def opening_kernel(hidden_ref, gate_ref, up_ref, down_ref, gain_ref, branch_ref, out_ref):
    lean = gain_ref[...] * branch_ref[...]
    high = lean.astype(jnp.bfloat16).astype(jnp.float32)
    row = lax.broadcasted_iota(jnp.int32, (8, lean.shape[1]), 0)
    extra = jnp.where(row == 0, high, jnp.where(row == 1, lean - high, 0.0))
    extra = extra.astype(jnp.bfloat16)
    seq, units = hidden_ref.shape[0], down_ref.shape[0]
    past = seq + 3 * units
    for k in range(out_ref.shape[0]):
        out_ref[k, :seq, :] = hidden_ref[...]
        out_ref[k, seq : seq + units, :] = gate_ref[...]
        out_ref[k, seq + units : seq + 2 * units, :] = up_ref[...]
        out_ref[k, seq + 2 * units : past, :] = down_ref[...]
        out_ref[k, past:, :] = extra


def routes_kernel(ids_ref, turned_ref, logits_ref, out_ref):
    ids = ids_ref[...]
    turned = turned_ref[...]
    count, top = ids.shape
    logits = logits_ref[...]
    grown = jnp.exp(logits - jnp.max(logits, axis=1, keepdims=True))
    weight = grown / jnp.sum(grown, axis=1, keepdims=True)
    upper = weight.astype(jnp.bfloat16).astype(jnp.float32)
    lower = weight - upper
    row = lax.broadcasted_iota(jnp.int32, (count, count), 0)
    col = lax.broadcasted_iota(jnp.int32, (count, count), 1)
    lane = lax.broadcasted_iota(jnp.int32, (count, LANES), 1)
    packed = jnp.zeros((count, LANES), jnp.float32)
    for k in range(top):
        mine = ids[:, k : k + 1]
        same = jnp.zeros((count, count), jnp.float32)
        for other in range(top):
            same = same + jnp.where(mine == turned[other : other + 1, :], 1.0, 0.0)
        rank = jnp.sum(jnp.where(col < row, same, 0.0), axis=1, keepdims=True)
        code = mine.astype(jnp.float32) * CAP + rank
        packed = jnp.where(lane == k, code, packed)
        packed = jnp.where(lane == top + k, upper[:, k : k + 1], packed)
        packed = jnp.where(lane == 2 * top + k, lower[:, k : k + 1], packed)
    out_ref[...] = packed


def stage_kernel(*refs):
    count = len(refs) // 2
    sems = refs[-1]
    moves = [
        pltpu.make_async_copy(refs[k], refs[count + k], sems.at[k]) for k in range(count)
    ]
    for move in moves:
        move.start()
    for move in moves:
        move.wait()


def brought(arrays):
    return pl.pallas_call(
        stage_kernel,
        out_shape=tuple(map(kept, arrays)),
        in_specs=[pl.BlockSpec(memory_space=pl.ANY)] * len(arrays),
        out_specs=(WHOLE,) * len(arrays),
        scratch_shapes=[pltpu.SemaphoreType.DMA((len(arrays),))],
        name="stage",
        compiler_params=LIMIT,
    )(*map(far, arrays))


def attend_kernel(
    lambda_ref,
    pieces_ref,
    gain_ref,
    query_ref,
    key_ref,
    value_ref,
    query_gain_ref,
    key_gain_ref,
    sub_ref,
    out_weight_ref,
    past_key_ref,
    past_value_ref,
    lengths_ref,
    out_ref,
    key_rows_ref,
    value_rows_ref,
):
    seq, past, size = past_key_ref.shape
    tp = pieces_ref.shape[0]
    half = size // 2
    full = jnp.concatenate([pieces_ref[k, :seq, :] for k in range(tp)], axis=1)
    full = full.astype(jnp.float32)
    square = jnp.sum(full * full, axis=1, keepdims=True) / full.shape[1]
    normed = (full * lax.rsqrt(square + EPSILON) * gain_ref[...]).astype(jnp.bfloat16)
    first = lax.broadcasted_iota(jnp.int32, (seq, size), 1) < half

    def halves(x):
        return (
            jnp.sum(jnp.where(first, x, 0.0), axis=1, keepdims=True),
            jnp.sum(jnp.where(first, 0.0, x), axis=1, keepdims=True),
        )

    def scaled(x, gain):
        low, high = halves(x * x)
        inverse = jnp.where(
            first, lax.rsqrt(low / half + EPSILON), lax.rsqrt(high / half + EPSILON)
        )
        return (x * inverse * gain).astype(jnp.bfloat16)

    query = scaled(mm(normed, query_ref[...]), query_gain_ref[...])
    key = scaled(mm(normed, key_ref[...]), key_gain_ref[...])
    value = mm(normed, value_ref[...]).astype(jnp.bfloat16)
    key_rows_ref[...] = key
    value_rows_ref[...] = value
    query = query.astype(jnp.float32)
    both = jnp.concatenate(
        [jnp.where(first, query, 0.0), jnp.where(first, 0.0, query)], axis=0
    )
    row = lax.broadcasted_iota(jnp.int32, (2 * seq, size), 0) % seq
    score = jnp.zeros((2 * seq, past), jnp.float32)
    for k in range(seq):
        mine = jnp.where(row == k, both, 0.0).astype(jnp.bfloat16)
        score = score + lax.dot_general(
            mine, past_key_ref[k], ACROSS, preferred_element_type=jnp.float32
        )
    scale = half**-0.5
    valid = lax.broadcasted_iota(jnp.int32, (seq, past), 1) < lengths_ref[...]
    own = [jnp.exp(o * scale) for o in halves(query * key.astype(jnp.float32))]
    grown = [
        jnp.where(valid, jnp.exp(score[m * seq : (m + 1) * seq] * scale), 0.0) for m in range(2)
    ]
    total = [jnp.sum(g, axis=1, keepdims=True) + o for g, o in zip(grown, own)]
    share = lambda_ref[0]
    weight = (grown[0] / total[0] - share * (grown[1] / total[1])).astype(jnp.bfloat16)
    weight_own = (own[0] / total[0] - share * (own[1] / total[1])).astype(jnp.bfloat16)
    weight = weight.astype(jnp.float32)
    row = lax.broadcasted_iota(jnp.int32, (seq, past), 0)
    mixed = weight_own.astype(jnp.float32) * value.astype(jnp.float32)
    for k in range(seq):
        mine = jnp.where(row == k, weight, 0.0).astype(jnp.bfloat16)
        mixed = mixed + mm(mine, past_value_ref[k])
    square = jnp.sum(mixed * mixed, axis=1, keepdims=True) / size
    head = mixed * lax.rsqrt(square + EPSILON) * sub_ref[...] * OUT_SCALE
    part = mm(head.astype(jnp.bfloat16), out_weight_ref[...]).astype(jnp.bfloat16)
    for k in range(tp):
        out_ref[k] = part


def mix_kernel(tp_ref, parts_ref, pieces_ref, gain_ref, routes_ref, res_ref, out_ref, *, top):
    tp, seq, _ = parts_ref.shape
    past = pieces_ref.shape[1] - 8
    residual = jnp.concatenate([pieces_ref[k, :seq, :] for k in range(tp)], axis=1)
    residual = residual.astype(jnp.float32)
    for k in range(tp):
        residual = residual + parts_ref[k].astype(jnp.float32)
    ends = [pieces_ref[k, past:, :].astype(jnp.float32) for k in range(tp)]
    lean = jnp.concatenate([end[0:1] + end[1:2] for end in ends], axis=1)
    total = residual.shape[1]
    width = total // tp
    inverse = lax.rsqrt(jnp.sum(residual * residual, axis=1, keepdims=True) / total + EPSILON)
    logit = jnp.sum(residual * lean, axis=1, keepdims=True) * inverse
    branch = jax.nn.sigmoid(logit)
    upper = branch.astype(jnp.bfloat16).astype(jnp.float32)
    own = jnp.zeros((residual.shape[0], width), jnp.float32)
    for k in range(tp):
        own = own + jnp.where(tp_ref[0] == k, residual[:, k * width : (k + 1) * width], 0.0)
    res_ref[...] = own
    mix = (own * inverse * gain_ref[...]).astype(jnp.bfloat16)
    routes = routes_ref[...]
    lane = lax.broadcasted_iota(jnp.int32, routes.shape, 1)
    routes = jnp.where(lane == 3 * top, upper, routes)
    routes = jnp.where(lane == 3 * top + 1, branch - upper, routes)
    rows = out_ref.shape[1] - width // LANES * seq
    stride = LANES * rows // seq
    notes = routes[:rows]
    for g in range(1, seq // rows):
        notes = notes + pltpu.roll(routes[g * rows : (g + 1) * rows], stride * g, axis=1)
    notes = notes.astype(jnp.bfloat16)
    for k in range(out_ref.shape[0]):
        for h in range(width // LANES):
            out_ref[k, h * seq : (h + 1) * seq, :] = mix[:, h * LANES : (h + 1) * LANES]
        out_ref[k, width // LANES * seq :, :] = notes


def notes_of(seen_ref, seq):
    line = seen_ref.shape[0]
    rows = seen_ref.shape[1] % seq
    packed = seen_ref[:, seen_ref.shape[1] - rows :, :].astype(jnp.float32)
    stride = LANES * rows // seq
    turned = [packed]
    for g in range(1, seq // rows):
        turned.append(pltpu.roll(packed, LANES - stride * g, axis=2))
    return jnp.concatenate(turned, axis=1).reshape(line * seq, LANES)


def slot_hits(notes, first, line, plane, top):
    total = notes.shape[0]
    slots = plane * line * CAP
    row = lax.broadcasted_iota(jnp.int32, (total, slots), 0)
    col = lax.broadcasted_iota(jnp.int32, (total, slots), 1)
    code = (first + col // (line * CAP)) * CAP + col % CAP
    here = row // (total // line) == (col // CAP) % line
    code = jnp.where(here, code, -1).astype(jnp.float32)
    return [notes[:, k : k + 1] == code for k in range(top)]


def outward_kernel(first_ref, seen_ref, out_hbm, placed_ref, dealt_ref, sems, *, top, seq):
    line = seen_ref.shape[0]
    plane, tp, items, width = out_hbm.shape
    slots = line * CAP
    rows = jnp.concatenate(
        [
            seen_ref[:, h * seq : (h + 1) * seq, :].reshape(line * seq, LANES)
            for h in range(width // LANES)
        ],
        axis=1,
    )
    dealt = rows.astype(jnp.float32).reshape(plane, tp, items - slots, width)
    dealt_ref[...] = dealt.astype(jnp.bfloat16)
    moves = [
        pltpu.make_async_copy(dealt_ref, out_hbm.at[:, :, pl.ds(slots, items - slots)], sems.at[tp])
    ]
    moves[0].start()
    hits = slot_hits(notes_of(seen_ref, seq), first_ref[0], line, plane, top)
    select = sum(jnp.where(h, 1.0, 0.0) for h in hits).astype(jnp.bfloat16)
    placed = lax.dot_general(select, rows, TURNED, preferred_element_type=jnp.float32)
    placed_ref[...] = placed.astype(jnp.bfloat16).reshape(plane, slots, width)
    for k in range(tp):
        moves.append(
            pltpu.make_async_copy(placed_ref, out_hbm.at[:, k, pl.ds(0, slots)], sems.at[k])
        )
        moves[-1].start()
    for move in moves:
        move.wait()


def weights_kernel(first_ref, seen_ref, upper_ref, lower_ref, branch_ref, *, top, plane, seq):
    line = seen_ref.shape[0]
    notes = notes_of(seen_ref, seq)
    hits = slot_hits(notes, first_ref[0], line, plane, top)
    upper_ref[...] = sum(
        jnp.where(h, notes[:, top + k : top + k + 1], 0.0) for k, h in enumerate(hits)
    ).astype(jnp.bfloat16)
    lower_ref[...] = sum(
        jnp.where(h, notes[:, 2 * top + k : 2 * top + k + 1], 0.0) for k, h in enumerate(hits)
    ).astype(jnp.bfloat16)
    branch = notes[:, 3 * top : 3 * top + 1] + notes[:, 3 * top + 1 : 3 * top + 2]
    branch_ref[...] = jnp.broadcast_to(branch, branch_ref.shape)


def expert_kernel(
    seen_ref, gate_ref, up_ref, down_ref, own_ref, other_ref, out_hbm, out_ref, sems, *, slots
):
    plane, tp, items, width = seen_ref.shape
    rows = jnp.concatenate(
        [seen_ref[:, k, :slots, :].reshape(plane * slots, width) for k in range(tp)], axis=1
    )
    gate_pre = mm(rows, gate_ref[0])
    up_pre = mm(rows, up_ref[0])
    act = clamped_unit(gate_pre, up_pre).astype(jnp.bfloat16)
    columns, _, rows_each, _ = own_ref.shape
    units = rows_each // 3
    dealt = items - slots

    def units_at(k, lo):
        return jnp.concatenate(
            [
                ref[:, k, lo : lo + units, :].reshape(columns * units, width)
                for ref in (own_ref, other_ref)
            ],
            axis=0,
        )

    rows = jnp.concatenate(
        [
            seen_ref[:, k, slots:, :].astype(jnp.float32).reshape(plane * dealt, width)
            for k in range(tp)
        ],
        axis=1,
    ).astype(jnp.bfloat16)

    def units_of(lo):
        return jnp.concatenate(
            [units_at(k, lo) for k in range(tp)],
            axis=1,
        )

    gate_pre = lax.dot_general(rows, units_of(0), ACROSS, preferred_element_type=jnp.float32)
    up_pre = lax.dot_general(rows, units_of(units), ACROSS, preferred_element_type=jnp.float32)
    dense_act = (gate_pre / (1.0 + jnp.exp(-gate_pre)) * up_pre).astype(jnp.bfloat16)
    moves = []
    for k in range(tp):
        part = mm(act, down_ref[0, :, k * width : (k + 1) * width]).astype(jnp.bfloat16)
        out_ref[k, :, :slots, :] = part.reshape(plane, slots, width)
        part = mm(dense_act, units_at(k, 2 * units)).reshape(plane, dealt, width)
        out_ref[k, :, slots:, :] = part.astype(jnp.bfloat16)
        moves.append(pltpu.make_async_copy(out_ref.at[k], out_hbm.at[:, k], sems.at[k]))
        moves[-1].start()
    for move in moves:
        move.wait()


def inward_kernel(seen_ref, upper_ref, lower_ref, branch_ref, out_ref):
    line, seq, width = out_ref.shape
    plane, tp, _, _ = seen_ref.shape
    slots = line * CAP
    whole = jnp.zeros((plane, slots, width), jnp.float32)
    for k in range(tp):
        whole = whole + seen_ref[:, k, :slots, :].astype(jnp.float32)
    whole = whole.astype(jnp.bfloat16).reshape(plane * slots, width)
    routed = mm(upper_ref[...], whole) + mm(lower_ref[...], whole)
    dense = seen_ref[:, :, slots:, :].astype(jnp.float32).reshape(line * seq, width)
    back = (routed + branch_ref[...] * dense).astype(jnp.bfloat16)
    out_ref[...] = back.reshape(line, seq, width)


def doubled(held, step):
    columns, cores = lax.axis_size("ep_1"), lax.axis_size("ep_2")
    flips = [step, step | 2 * step if 2 * step < columns else step]
    pairs = [
        (i * cores + c, (i ^ flips[c % 2]) * cores + c) for i in range(columns) for c in range(cores)
    ]
    other = lax.ppermute(held, PLANE, pairs)
    return jnp.concatenate([held, other], axis=0)


def shaped(shape, dtype):
    return jax.ShapeDtypeStruct(shape, dtype)


def body(
    hidden_in,
    norm_gain_attn,
    query_weight,
    key_weight,
    value_weight,
    query_gain,
    key_gain,
    lambda_head,
    sub_gain,
    out_weight,
    cache_key,
    cache_value,
    lengths,
    norm_gain_mix,
    route_ids,
    route_logits,
    expert_gate,
    expert_up,
    expert_down,
    dense_gate,
    dense_up,
    dense_down,
    branch_gate,
):
    seq, top = route_ids.shape
    width = hidden_in.shape[1]
    units = dense_down.shape[0]
    line = lax.axis_size("ep_0")
    plane = lax.axis_size("ep_1") * lax.axis_size("ep_2")
    tp = lax.axis_size("tp")
    slots = line * CAP
    dealt = line * seq // (plane * tp)
    past = seq + 3 * units
    mine = pl.pallas_call(
        opening_kernel, out_shape=shaped((tp, past + 8, width), jnp.bfloat16), name="opening", compiler_params=LIMIT
    )(
        *map(
            far,
            (
                hidden_in,
                dense_gate.T,
                dense_up.T,
                dense_down,
                norm_gain_mix[None, :],
                branch_gate[None, :],
            ),
        )
    )
    pieces = lax.all_to_all(mine, "tp", 0, 0, tiled=True)
    needed = (
        norm_gain_attn[None, :],
        query_weight,
        key_weight,
        value_weight,
        query_gain[None, :],
        key_gain[None, :],
        sub_gain[None, :],
        out_weight,
        cache_key,
        cache_value,
        norm_gain_mix[None, :],
    )
    *staged, gain_here = brought(needed)
    routes = pl.pallas_call(
        routes_kernel, out_shape=shaped((seq, LANES), jnp.float32), name="routes", compiler_params=LIMIT
    )(route_ids, route_ids.T, route_logits)
    size = value_weight.shape[1]
    parts, key_rows, value_rows = pl.pallas_call(
        attend_kernel,
        out_shape=(
            shaped((tp, seq, out_weight.shape[1]), jnp.bfloat16),
            shaped((seq, size), jnp.bfloat16),
            shaped((seq, size), jnp.bfloat16),
        ),
        in_specs=[SCALARS] + [WHOLE] * 12,
        name="attend",
        compiler_params=LIMIT,
    )(
        lambda_head,
        near(pieces),
        *map(near, staged),
        near(lengths[:, None]),
    )
    parts = lax.all_to_all(parts, "tp", 0, 0, tiled=True)
    columns = lax.axis_size("ep_1")
    steps = [1 << k for k in reversed(range(columns.bit_length() - 1))]
    own_dense = pieces[None, :, seq:past]
    for step in steps[:1]:
        own_dense = doubled(own_dense, step)
    residual, message = pl.pallas_call(
        lambda *refs: mix_kernel(*refs, top=top),
        out_shape=(
            shaped((seq, width), jnp.float32),
            shaped((line, width // LANES * seq + 8, LANES), jnp.bfloat16),
        ),
        in_specs=[SCALARS] + [WHOLE] * 4,
        name="mix",
        compiler_params=LIMIT,
    )(
        lax.axis_index("tp").reshape(1),
        near(parts),
        near(pieces),
        near(gain_here),
        near(routes),
    )
    seen = lax.all_to_all(message, "ep_0", 0, 0, tiled=True)
    for step in steps[1:]:
        own_dense = doubled(own_dense, step)
    own_dense, seen = lax.optimization_barrier((own_dense, seen))
    seen = near(seen)
    other_dense = lax.ppermute(own_dense, "ep_2", [(0, 1), (1, 0)])
    first = (lax.axis_index("ep_0") * plane).reshape(1)
    outward = pl.pallas_call(
        lambda *refs: outward_kernel(*refs, top=top, seq=seq),
        out_shape=sent_to_hbm((plane, tp, slots + dealt, width), jnp.bfloat16),
        in_specs=[SCALARS, WHOLE],
        out_specs=pl.BlockSpec(memory_space=pl.ANY),
        scratch_shapes=[
            pltpu.VMEM((plane, slots, width), jnp.bfloat16),
            pltpu.VMEM((plane, tp, dealt, width), jnp.bfloat16),
            pltpu.SemaphoreType.DMA((tp + 1,)),
        ],
        name="outward",
        compiler_params=LIMIT,
    )(first, seen)
    arrived = lax.all_to_all(
        outward.reshape(plane * tp, slots + dealt, width), BLOCK, 0, 0, tiled=True
    ).reshape(plane, tp, slots + dealt, width)
    upper, lower, branch = pl.pallas_call(
        lambda *refs: weights_kernel(*refs, top=top, plane=plane, seq=seq),
        out_shape=(
            shaped((line * seq, plane * slots), jnp.bfloat16),
            shaped((line * seq, plane * slots), jnp.bfloat16),
            shaped((line * seq, width), jnp.float32),
        ),
        in_specs=[SCALARS, WHOLE],
        name="weights",
        compiler_params=LIMIT,
    )(first, seen)
    tools = brought((expert_gate, expert_up, expert_down, own_dense, other_dense))
    sent = pl.pallas_call(
        lambda *refs: expert_kernel(*refs, slots=slots),
        out_shape=sent_to_hbm((plane, tp, slots + dealt, width), jnp.bfloat16),
        in_specs=[WHOLE] * 6,
        out_specs=pl.BlockSpec(memory_space=pl.ANY),
        scratch_shapes=[
            pltpu.VMEM((tp, plane, slots + dealt, width), jnp.bfloat16),
            pltpu.SemaphoreType.DMA((tp,)),
        ],
        name="experts",
        compiler_params=LIMIT,
    )(
        near(arrived),
        *map(near, tools),
    )
    returned = lax.all_to_all(
        sent.reshape(plane * tp, slots + dealt, width), BLOCK, 0, 0, tiled=True
    ).reshape(plane, tp, slots + dealt, width)
    back = pl.pallas_call(
        inward_kernel,
        out_shape=shaped((line, seq, width), jnp.bfloat16),
        name="inward",
        compiler_params=LIMIT,
    )(near(returned), near(upper), near(lower), near(branch))
    home = lax.all_to_all(back, "ep_0", 0, 0, tiled=True)
    layer_out = (residual + jnp.sum(home.astype(jnp.float32), axis=0)).astype(jnp.bfloat16)
    return (layer_out, key_rows, value_rows)


def solution(mesh):
    split = Mesh(mesh.devices.reshape(16, 4, 2, mesh.shape["tp"]), ("ep_0", "ep_1", "ep_2", "tp"))
    in_specs = (
        P(EP, "tp"),
        P(),
        P(None, "tp"),
        P(None, "tp"),
        P(None, "tp"),
        P(),
        P(),
        P("tp"),
        P(),
        P("tp", None),
        P(EP, None, "tp"),
        P(EP, None, "tp"),
        P(EP),
        P("tp"),
        P(EP, None),
        P(EP, None),
        P(EP, None, "tp"),
        P(EP, None, "tp"),
        P(EP, "tp", None),
        P("tp", EP),
        P("tp", EP),
        P(EP, "tp"),
        P("tp"),
    )
    out_specs = (P(EP, "tp"), P(EP, "tp"), P(EP, "tp"))
    return jax.shard_map(body, mesh=split, in_specs=in_specs, out_specs=out_specs, check_vma=False)
```

```python
import math

import jax
import jax.numpy as jnp
from jax import lax
from jax.experimental import pallas as pl
from jax.experimental.pallas import tpu as pltpu

from jax.sharding import Mesh
from jax.sharding import PartitionSpec as P


EP = ("ep_0", "ep_1", "ep_2")
BLOCK = ("ep_1", "ep_2", "tp")
CAP = 2


EPSILON = 1e-06
CLAMP_LIMIT = 7.0
SWISH_ALPHA = 1.702
OUT_SCALE = 0.2 + 0.6 * math.exp(-0.6)


def clamped_unit(gate_pre, up_pre):
    gate_cut = jnp.minimum(gate_pre, CLAMP_LIMIT)
    up_cut = jnp.clip(up_pre, -CLAMP_LIMIT, CLAMP_LIMIT)
    return (up_cut + 1.0) * gate_cut * jax.nn.sigmoid(SWISH_ALPHA * gate_cut)


LANES = 128
TURNED = (((0,), (0,)), ((), ()))
ACROSS = (((1,), (1,)), ((), ()))
SCALARS = pl.BlockSpec(memory_space=pltpu.SMEM)
LIMIT = pltpu.CompilerParams(vmem_limit_bytes=12 * 2**20)
WHOLE = pl.BlockSpec(memory_space=pltpu.VMEM)


def mm(a, b):
    return jnp.dot(a, b, preferred_element_type=jnp.float32)


def sent_to_hbm(shape, dtype):
    return pltpu.HBM(shape, dtype)


def kept(x):
    return pltpu.VMEM(x.shape, x.dtype)


def far(x):
    return pltpu.with_memory_space_constraint(x, pltpu.HBM)


def near(x):
    return pltpu.with_memory_space_constraint(x, pltpu.VMEM)


def opening_kernel(hidden_ref, gate_ref, up_ref, down_ref, gain_ref, branch_ref, out_ref):
    lean = gain_ref[...] * branch_ref[...]
    high = lean.astype(jnp.bfloat16).astype(jnp.float32)
    row = lax.broadcasted_iota(jnp.int32, (8, lean.shape[1]), 0)
    extra = jnp.where(row == 0, high, jnp.where(row == 1, lean - high, 0.0))
    extra = extra.astype(jnp.bfloat16)
    seq, units = hidden_ref.shape[0], down_ref.shape[0]
    past = seq + 3 * units
    for k in range(out_ref.shape[0]):
        out_ref[k, :seq, :] = hidden_ref[...]
        out_ref[k, seq : seq + units, :] = gate_ref[...]
        out_ref[k, seq + units : seq + 2 * units, :] = up_ref[...]
        out_ref[k, seq + 2 * units : past, :] = down_ref[...]
        out_ref[k, past:, :] = extra


def routes_kernel(ids_ref, turned_ref, logits_ref, out_ref):
    ids = ids_ref[...]
    turned = turned_ref[...]
    count, top = ids.shape
    logits = logits_ref[...]
    grown = jnp.exp(logits - jnp.max(logits, axis=1, keepdims=True))
    weight = grown / jnp.sum(grown, axis=1, keepdims=True)
    upper = weight.astype(jnp.bfloat16).astype(jnp.float32)
    lower = weight - upper
    row = lax.broadcasted_iota(jnp.int32, (count, count), 0)
    col = lax.broadcasted_iota(jnp.int32, (count, count), 1)
    lane = lax.broadcasted_iota(jnp.int32, (count, LANES), 1)
    packed = jnp.zeros((count, LANES), jnp.float32)
    for k in range(top):
        mine = ids[:, k : k + 1]
        same = jnp.zeros((count, count), jnp.float32)
        for other in range(top):
            same = same + jnp.where(mine == turned[other : other + 1, :], 1.0, 0.0)
        rank = jnp.sum(jnp.where(col < row, same, 0.0), axis=1, keepdims=True)
        code = mine.astype(jnp.float32) * CAP + rank
        packed = jnp.where(lane == k, code, packed)
        packed = jnp.where(lane == top + k, upper[:, k : k + 1], packed)
        packed = jnp.where(lane == 2 * top + k, lower[:, k : k + 1], packed)
    out_ref[...] = packed


def stage_kernel(*refs):
    count = len(refs) // 2
    sems = refs[-1]
    moves = [
        pltpu.make_async_copy(refs[k], refs[count + k], sems.at[k]) for k in range(count)
    ]
    for move in moves:
        move.start()
    for move in moves:
        move.wait()


def brought(arrays):
    return pl.pallas_call(
        stage_kernel,
        out_shape=tuple(map(kept, arrays)),
        in_specs=[pl.BlockSpec(memory_space=pl.ANY)] * len(arrays),
        out_specs=(WHOLE,) * len(arrays),
        scratch_shapes=[pltpu.SemaphoreType.DMA((len(arrays),))],
        name="stage",
        compiler_params=LIMIT,
    )(*map(far, arrays))


def spread(message_ref, out_hbm, sems):
    moves = [
        pltpu.make_async_copy(message_ref, out_hbm.at[k], sems.at[k])
        for k in range(out_hbm.shape[0])
    ]
    for move in moves:
        move.start()
    for move in moves:
        move.wait()


def attend_kernel(
    lambda_ref,
    pieces_ref,
    gain_ref,
    query_ref,
    key_ref,
    value_ref,
    query_gain_ref,
    key_gain_ref,
    sub_ref,
    out_weight_ref,
    past_key_ref,
    past_value_ref,
    lengths_ref,
    out_hbm,
    key_rows_ref,
    value_rows_ref,
    part_ref,
    sems,
):
    seq, past, size = past_key_ref.shape
    tp = pieces_ref.shape[0]
    half = size // 2
    full = jnp.concatenate([pieces_ref[k, :seq, :] for k in range(tp)], axis=1)
    full = full.astype(jnp.float32)
    square = jnp.sum(full * full, axis=1, keepdims=True) / full.shape[1]
    normed = (full * lax.rsqrt(square + EPSILON) * gain_ref[...]).astype(jnp.bfloat16)
    first = lax.broadcasted_iota(jnp.int32, (seq, size), 1) < half

    def halves(x):
        return (
            jnp.sum(jnp.where(first, x, 0.0), axis=1, keepdims=True),
            jnp.sum(jnp.where(first, 0.0, x), axis=1, keepdims=True),
        )

    def scaled(x, gain):
        low, high = halves(x * x)
        inverse = jnp.where(
            first, lax.rsqrt(low / half + EPSILON), lax.rsqrt(high / half + EPSILON)
        )
        return (x * inverse * gain).astype(jnp.bfloat16)

    query = scaled(mm(normed, query_ref[...]), query_gain_ref[...])
    key = scaled(mm(normed, key_ref[...]), key_gain_ref[...])
    value = mm(normed, value_ref[...]).astype(jnp.bfloat16)
    key_rows_ref[...] = key
    value_rows_ref[...] = value
    query = query.astype(jnp.float32)
    both = jnp.concatenate(
        [jnp.where(first, query, 0.0), jnp.where(first, 0.0, query)], axis=0
    )
    row = lax.broadcasted_iota(jnp.int32, (2 * seq, size), 0) % seq
    score = jnp.zeros((2 * seq, past), jnp.float32)
    for k in range(seq):
        mine = jnp.where(row == k, both, 0.0).astype(jnp.bfloat16)
        score = score + lax.dot_general(
            mine, past_key_ref[k], ACROSS, preferred_element_type=jnp.float32
        )
    scale = half**-0.5
    valid = lax.broadcasted_iota(jnp.int32, (seq, past), 1) < lengths_ref[...]
    own = [jnp.exp(o * scale) for o in halves(query * key.astype(jnp.float32))]
    grown = [
        jnp.where(valid, jnp.exp(score[m * seq : (m + 1) * seq] * scale), 0.0) for m in range(2)
    ]
    total = [jnp.sum(g, axis=1, keepdims=True) + o for g, o in zip(grown, own)]
    share = lambda_ref[0]
    weight = (grown[0] / total[0] - share * (grown[1] / total[1])).astype(jnp.bfloat16)
    weight_own = (own[0] / total[0] - share * (own[1] / total[1])).astype(jnp.bfloat16)
    weight = weight.astype(jnp.float32)
    row = lax.broadcasted_iota(jnp.int32, (seq, past), 0)
    mixed = weight_own.astype(jnp.float32) * value.astype(jnp.float32)
    for k in range(seq):
        mine = jnp.where(row == k, weight, 0.0).astype(jnp.bfloat16)
        mixed = mixed + mm(mine, past_value_ref[k])
    square = jnp.sum(mixed * mixed, axis=1, keepdims=True) / size
    head = mixed * lax.rsqrt(square + EPSILON) * sub_ref[...] * OUT_SCALE
    part_ref[...] = mm(head.astype(jnp.bfloat16), out_weight_ref[...]).astype(jnp.bfloat16)
    spread(part_ref, out_hbm, sems)


def mix_kernel(tp_ref, parts_ref, pieces_ref, gain_ref, routes_ref, res_ref, out_hbm, message_ref, sems, *, top):
    tp, seq, _ = parts_ref.shape
    past = pieces_ref.shape[1] - 8
    residual = jnp.concatenate([pieces_ref[k, :seq, :] for k in range(tp)], axis=1)
    residual = residual.astype(jnp.float32)
    for k in range(tp):
        residual = residual + parts_ref[k].astype(jnp.float32)
    ends = [pieces_ref[k, past:, :].astype(jnp.float32) for k in range(tp)]
    lean = jnp.concatenate([end[0:1] + end[1:2] for end in ends], axis=1)
    total = residual.shape[1]
    width = total // tp
    inverse = lax.rsqrt(jnp.sum(residual * residual, axis=1, keepdims=True) / total + EPSILON)
    logit = jnp.sum(residual * lean, axis=1, keepdims=True) * inverse
    branch = jax.nn.sigmoid(logit)
    upper = branch.astype(jnp.bfloat16).astype(jnp.float32)
    own = jnp.zeros((residual.shape[0], width), jnp.float32)
    for k in range(tp):
        own = own + jnp.where(tp_ref[0] == k, residual[:, k * width : (k + 1) * width], 0.0)
    res_ref[...] = own
    mix = (own * inverse * gain_ref[...]).astype(jnp.bfloat16)
    routes = routes_ref[...]
    lane = lax.broadcasted_iota(jnp.int32, routes.shape, 1)
    routes = jnp.where(lane == 3 * top, upper, routes)
    routes = jnp.where(lane == 3 * top + 1, branch - upper, routes)
    rows = message_ref.shape[0] - width // LANES * seq
    stride = LANES * rows // seq
    notes = routes[:rows]
    for g in range(1, seq // rows):
        notes = notes + pltpu.roll(routes[g * rows : (g + 1) * rows], stride * g, axis=1)
    notes = notes.astype(jnp.bfloat16)
    for h in range(width // LANES):
        message_ref[h * seq : (h + 1) * seq, :] = mix[:, h * LANES : (h + 1) * LANES]
    message_ref[width // LANES * seq :, :] = notes
    spread(message_ref, out_hbm, sems)


def notes_of(seen_ref, seq):
    line = seen_ref.shape[0]
    rows = seen_ref.shape[1] % seq
    packed = seen_ref[:, seen_ref.shape[1] - rows :, :].astype(jnp.float32)
    stride = LANES * rows // seq
    turned = [packed]
    for g in range(1, seq // rows):
        turned.append(pltpu.roll(packed, LANES - stride * g, axis=2))
    return jnp.concatenate(turned, axis=1).reshape(line * seq, LANES)


def slot_hits(notes, first, line, plane, top):
    total = notes.shape[0]
    slots = plane * line * CAP
    row = lax.broadcasted_iota(jnp.int32, (total, slots), 0)
    col = lax.broadcasted_iota(jnp.int32, (total, slots), 1)
    code = (first + col // (line * CAP)) * CAP + col % CAP
    here = row // (total // line) == (col // CAP) % line
    code = jnp.where(here, code, -1).astype(jnp.float32)
    return [notes[:, k : k + 1] == code for k in range(top)]


def outward_kernel(first_ref, seen_ref, out_hbm, placed_ref, dealt_ref, sems, *, top, seq):
    line = seen_ref.shape[0]
    plane, tp, items, width = out_hbm.shape
    slots = line * CAP
    rows = jnp.concatenate(
        [
            seen_ref[:, h * seq : (h + 1) * seq, :].reshape(line * seq, LANES)
            for h in range(width // LANES)
        ],
        axis=1,
    )
    dealt = rows.astype(jnp.float32).reshape(plane, tp, items - slots, width)
    dealt_ref[...] = dealt.astype(jnp.bfloat16)
    moves = [
        pltpu.make_async_copy(dealt_ref, out_hbm.at[:, :, pl.ds(slots, items - slots)], sems.at[tp])
    ]
    moves[0].start()
    hits = slot_hits(notes_of(seen_ref, seq), first_ref[0], line, plane, top)
    select = sum(jnp.where(h, 1.0, 0.0) for h in hits).astype(jnp.bfloat16)
    placed = lax.dot_general(select, rows, TURNED, preferred_element_type=jnp.float32)
    placed_ref[...] = placed.astype(jnp.bfloat16).reshape(plane, slots, width)
    for k in range(tp):
        moves.append(
            pltpu.make_async_copy(placed_ref, out_hbm.at[:, k, pl.ds(0, slots)], sems.at[k])
        )
        moves[-1].start()
    for move in moves:
        move.wait()


def weights_kernel(first_ref, seen_ref, upper_ref, lower_ref, branch_ref, *, top, plane, seq):
    line = seen_ref.shape[0]
    notes = notes_of(seen_ref, seq)
    hits = slot_hits(notes, first_ref[0], line, plane, top)
    upper_ref[...] = sum(
        jnp.where(h, notes[:, top + k : top + k + 1], 0.0) for k, h in enumerate(hits)
    ).astype(jnp.bfloat16)
    lower_ref[...] = sum(
        jnp.where(h, notes[:, 2 * top + k : 2 * top + k + 1], 0.0) for k, h in enumerate(hits)
    ).astype(jnp.bfloat16)
    branch = notes[:, 3 * top : 3 * top + 1] + notes[:, 3 * top + 1 : 3 * top + 2]
    branch_ref[...] = jnp.broadcast_to(branch, branch_ref.shape)


def expert_kernel(
    seen_ref, gate_ref, up_ref, down_ref, own_ref, other_ref, out_hbm, out_ref, sems, *, slots
):
    plane, tp, items, width = seen_ref.shape
    rows = jnp.concatenate(
        [seen_ref[:, k, :slots, :].reshape(plane * slots, width) for k in range(tp)], axis=1
    )
    gate_pre = mm(rows, gate_ref[0])
    up_pre = mm(rows, up_ref[0])
    act = clamped_unit(gate_pre, up_pre).astype(jnp.bfloat16)
    columns, _, rows_each, _ = own_ref.shape
    units = rows_each // 3
    dealt = items - slots

    def units_at(k, lo):
        return jnp.concatenate(
            [
                ref[:, k, lo : lo + units, :].reshape(columns * units, width)
                for ref in (own_ref, other_ref)
            ],
            axis=0,
        )

    rows = jnp.concatenate(
        [
            seen_ref[:, k, slots:, :].astype(jnp.float32).reshape(plane * dealt, width)
            for k in range(tp)
        ],
        axis=1,
    ).astype(jnp.bfloat16)

    def units_of(lo):
        return jnp.concatenate(
            [units_at(k, lo) for k in range(tp)],
            axis=1,
        )

    gate_pre = lax.dot_general(rows, units_of(0), ACROSS, preferred_element_type=jnp.float32)
    up_pre = lax.dot_general(rows, units_of(units), ACROSS, preferred_element_type=jnp.float32)
    dense_act = (gate_pre / (1.0 + jnp.exp(-gate_pre)) * up_pre).astype(jnp.bfloat16)
    moves = []
    for k in range(tp):
        part = mm(act, down_ref[0, :, k * width : (k + 1) * width]).astype(jnp.bfloat16)
        out_ref[k, :, :slots, :] = part.reshape(plane, slots, width)
        part = mm(dense_act, units_at(k, 2 * units)).reshape(plane, dealt, width)
        out_ref[k, :, slots:, :] = part.astype(jnp.bfloat16)
        moves.append(pltpu.make_async_copy(out_ref.at[k], out_hbm.at[:, k], sems.at[k]))
        moves[-1].start()
    for move in moves:
        move.wait()


def inward_kernel(seen_ref, upper_ref, lower_ref, branch_ref, out_ref):
    line, seq, width = out_ref.shape
    plane, tp, _, _ = seen_ref.shape
    slots = line * CAP
    whole = jnp.zeros((plane, slots, width), jnp.float32)
    for k in range(tp):
        whole = whole + seen_ref[:, k, :slots, :].astype(jnp.float32)
    whole = whole.astype(jnp.bfloat16).reshape(plane * slots, width)
    routed = mm(upper_ref[...], whole) + mm(lower_ref[...], whole)
    dense = seen_ref[:, :, slots:, :].astype(jnp.float32).reshape(line * seq, width)
    back = (routed + branch_ref[...] * dense).astype(jnp.bfloat16)
    out_ref[...] = back.reshape(line, seq, width)


def doubled(held, step):
    columns = lax.axis_size("ep_1")
    other = lax.ppermute(held, "ep_1", [(i, i ^ step) for i in range(columns)])
    return jnp.concatenate([held, other], axis=0)


def shaped(shape, dtype):
    return jax.ShapeDtypeStruct(shape, dtype)


def body(
    hidden_in,
    norm_gain_attn,
    query_weight,
    key_weight,
    value_weight,
    query_gain,
    key_gain,
    lambda_head,
    sub_gain,
    out_weight,
    cache_key,
    cache_value,
    lengths,
    norm_gain_mix,
    route_ids,
    route_logits,
    expert_gate,
    expert_up,
    expert_down,
    dense_gate,
    dense_up,
    dense_down,
    branch_gate,
):
    seq, top = route_ids.shape
    width = hidden_in.shape[1]
    units = dense_down.shape[0]
    line = lax.axis_size("ep_0")
    plane = lax.axis_size("ep_1") * lax.axis_size("ep_2")
    tp = lax.axis_size("tp")
    slots = line * CAP
    dealt = line * seq // (plane * tp)
    past = seq + 3 * units
    mine = pl.pallas_call(
        opening_kernel, out_shape=shaped((tp, past + 8, width), jnp.bfloat16), name="opening", compiler_params=LIMIT
    )(
        *map(
            far,
            (
                hidden_in,
                dense_gate.T,
                dense_up.T,
                dense_down,
                norm_gain_mix[None, :],
                branch_gate[None, :],
            ),
        )
    )
    pieces = lax.all_to_all(mine, "tp", 0, 0, tiled=True)
    needed = (
        norm_gain_attn[None, :],
        query_weight,
        key_weight,
        value_weight,
        query_gain[None, :],
        key_gain[None, :],
        sub_gain[None, :],
        out_weight,
        cache_key,
        cache_value,
        norm_gain_mix[None, :],
    )
    *staged, gain_here = brought(needed)
    routes = pl.pallas_call(
        routes_kernel, out_shape=shaped((seq, LANES), jnp.float32), name="routes", compiler_params=LIMIT
    )(route_ids, route_ids.T, route_logits)
    size = value_weight.shape[1]
    parts, key_rows, value_rows = pl.pallas_call(
        attend_kernel,
        out_shape=(
            sent_to_hbm((tp, seq, out_weight.shape[1]), jnp.bfloat16),
            shaped((seq, size), jnp.bfloat16),
            shaped((seq, size), jnp.bfloat16),
        ),
        in_specs=[SCALARS] + [WHOLE] * 12,
        out_specs=(pl.BlockSpec(memory_space=pl.ANY), WHOLE, WHOLE),
        scratch_shapes=[
            pltpu.VMEM((seq, out_weight.shape[1]), jnp.bfloat16),
            pltpu.SemaphoreType.DMA((tp,)),
        ],
        name="attend",
        compiler_params=LIMIT,
    )(
        lambda_head,
        near(pieces),
        *map(near, staged),
        near(lengths[:, None]),
    )
    parts = lax.all_to_all(parts, "tp", 0, 0, tiled=True)
    columns = lax.axis_size("ep_1")
    steps = [1 << k for k in reversed(range(columns.bit_length() - 1))]
    own_dense = pieces[None, :, seq:past]
    for step in steps[:1]:
        own_dense = doubled(own_dense, step)
    residual, message = pl.pallas_call(
        lambda *refs: mix_kernel(*refs, top=top),
        out_shape=(
            shaped((seq, width), jnp.float32),
            sent_to_hbm((line, width // LANES * seq + 8, LANES), jnp.bfloat16),
        ),
        in_specs=[SCALARS] + [WHOLE] * 4,
        out_specs=(WHOLE, pl.BlockSpec(memory_space=pl.ANY)),
        scratch_shapes=[
            pltpu.VMEM((width // LANES * seq + 8, LANES), jnp.bfloat16),
            pltpu.SemaphoreType.DMA((line,)),
        ],
        name="mix",
        compiler_params=LIMIT,
    )(
        lax.axis_index("tp").reshape(1),
        near(parts),
        near(pieces),
        near(gain_here),
        near(routes),
    )
    seen = lax.all_to_all(message, "ep_0", 0, 0, tiled=True)
    for step in steps[1:]:
        own_dense = doubled(own_dense, step)
    own_dense, seen = lax.optimization_barrier((own_dense, seen))
    seen = near(seen)
    other_dense = lax.ppermute(own_dense, "ep_2", [(0, 1), (1, 0)])
    first = (lax.axis_index("ep_0") * plane).reshape(1)
    outward = pl.pallas_call(
        lambda *refs: outward_kernel(*refs, top=top, seq=seq),
        out_shape=sent_to_hbm((plane, tp, slots + dealt, width), jnp.bfloat16),
        in_specs=[SCALARS, WHOLE],
        out_specs=pl.BlockSpec(memory_space=pl.ANY),
        scratch_shapes=[
            pltpu.VMEM((plane, slots, width), jnp.bfloat16),
            pltpu.VMEM((plane, tp, dealt, width), jnp.bfloat16),
            pltpu.SemaphoreType.DMA((tp + 1,)),
        ],
        name="outward",
        compiler_params=LIMIT,
    )(first, seen)
    arrived = lax.all_to_all(
        outward.reshape(plane * tp, slots + dealt, width), BLOCK, 0, 0, tiled=True
    ).reshape(plane, tp, slots + dealt, width)
    upper, lower, branch = pl.pallas_call(
        lambda *refs: weights_kernel(*refs, top=top, plane=plane, seq=seq),
        out_shape=(
            shaped((line * seq, plane * slots), jnp.bfloat16),
            shaped((line * seq, plane * slots), jnp.bfloat16),
            shaped((line * seq, width), jnp.float32),
        ),
        in_specs=[SCALARS, WHOLE],
        name="weights",
        compiler_params=LIMIT,
    )(first, seen)
    tools = brought((expert_gate, expert_up, expert_down, own_dense, other_dense))
    sent = pl.pallas_call(
        lambda *refs: expert_kernel(*refs, slots=slots),
        out_shape=sent_to_hbm((plane, tp, slots + dealt, width), jnp.bfloat16),
        in_specs=[WHOLE] * 6,
        out_specs=pl.BlockSpec(memory_space=pl.ANY),
        scratch_shapes=[
            pltpu.VMEM((tp, plane, slots + dealt, width), jnp.bfloat16),
            pltpu.SemaphoreType.DMA((tp,)),
        ],
        name="experts",
        compiler_params=LIMIT,
    )(
        near(arrived),
        *map(near, tools),
    )
    returned = lax.all_to_all(
        sent.reshape(plane * tp, slots + dealt, width), BLOCK, 0, 0, tiled=True
    ).reshape(plane, tp, slots + dealt, width)
    back = pl.pallas_call(
        inward_kernel,
        out_shape=shaped((line, seq, width), jnp.bfloat16),
        name="inward",
        compiler_params=LIMIT,
    )(near(returned), near(upper), near(lower), near(branch))
    home = lax.all_to_all(back, "ep_0", 0, 0, tiled=True)
    layer_out = (residual + jnp.sum(home.astype(jnp.float32), axis=0)).astype(jnp.bfloat16)
    return (layer_out, key_rows, value_rows)


def solution(mesh):
    split = Mesh(mesh.devices.reshape(16, 4, 2, mesh.shape["tp"]), ("ep_0", "ep_1", "ep_2", "tp"))
    in_specs = (
        P(EP, "tp"),
        P(),
        P(None, "tp"),
        P(None, "tp"),
        P(None, "tp"),
        P(),
        P(),
        P("tp"),
        P(),
        P("tp", None),
        P(EP, None, "tp"),
        P(EP, None, "tp"),
        P(EP),
        P("tp"),
        P(EP, None),
        P(EP, None),
        P(EP, None, "tp"),
        P(EP, None, "tp"),
        P(EP, "tp", None),
        P("tp", EP),
        P("tp", EP),
        P(EP, "tp"),
        P("tp"),
    )
    out_specs = (P(EP, "tp"), P(EP, "tp"), P(EP, "tp"))
    return jax.shard_map(body, mesh=split, in_specs=in_specs, out_specs=out_specs, check_vma=False)
```
